512 devices in a mesh: sp: 64 (over z, y), tp: 8 (over x, core).
Axes of the slice: x: 4, y: 4, z: 16, core: 2. Of those that a mesh axis runs over, the one named last changes fastest.
Arguments:
- tokens: bfloat16 [16384, 2048], P('sp', 'tp'), may hold values from -64 to 64
- input_norm_gain: float32 [2048], replicated, may hold values from 0.1 to 1.9
- attention_query_weight: bfloat16 [2048, 512], P(None, 'tp'), may hold values from -0.21875 to 0.21875
- attention_key_weight: bfloat16 [2048, 512], P(None, 'tp'), may hold values from -0.21875 to 0.21875
- attention_value_weight: bfloat16 [2048, 512], P(None, 'tp'), may hold values from -0.125 to 0.125
- attention_score_bias: float32 [8], P('tp'), may hold values from -18 to -7
- recurrence_query_weight: bfloat16 [2048, 1024], P(None, 'tp'), may hold values from -0.125 to 0.125
- forget_weight: bfloat16 [2048, 1024], P(None, 'tp'), may hold values from -0.125 to 0.125
- input_weight: bfloat16 [2048, 512], P(None, 'tp'), may hold values from -0.125 to 0.125
- output_gate_weight: bfloat16 [2048, 512], P(None, 'tp'), may hold values from -0.125 to 0.125
- forget_minimum: float32 [8, 128], P('tp'), may hold values from 0.9 to 1
- decay_spikes: float32 [16384, 8], P('sp', 'tp'), may hold values from -2.2 to 0
- head_norm_gain: float32 [64], replicated, may hold values from 0.1 to 1.9
- attention_output_weight: bfloat16 [512, 2048], P('tp'), may hold values from -0.25 to 0.25
- recurrence_output_weight: bfloat16 [512, 2048], P('tp'), may hold values from -0.25 to 0.25
Outputs:
- mixed: bfloat16 [16384, 2048], P('sp', 'tp')
The draws below stay inside these ranges and needn't reach their ends.
All inputs are finite; a program needn't handle non-finite values.
Results may differ from the reference program's by a relative error of at most 0.018.
Values may be sent and summed in bfloat16 or wider, within the bound.
A program may use at most 64 MiB of HBM per device.

```python
import jax
import jax.numpy as jnp
from jax import lax

D = 2048
SB_HEADS = 8
HEAD = 64
REC_HEADS = 8
REC_KEY = 128
REC_VAL = 64
TOK_DEV = 256
REC_SPAN = 64
TOKENS = 16384


def draw_tokens(key, part):
    streams = jax.random.split(jax.random.fold_in(key, 11), 3)
    column_rise = jnp.exp(jnp.log(4.0) * jnp.arange(D, dtype=jnp.float32) / D)
    column_rough = jnp.exp(jax.random.uniform(streams[0], (D,), jnp.float32, -0.35, 0.35))
    row_scale = jnp.exp(jax.random.uniform(streams[1], (TOKENS, 1), jnp.float32, -0.7, 0.7))
    noise_field = jnp.clip(jax.random.normal(streams[2], (TOKENS, D), jnp.float32), -5.0, 5.0)
    return (noise_field * row_scale * column_rise[None, :] * column_rough[None, :]).astype(jnp.bfloat16)


def draw_attention_score_bias(key, part):
    spread = jax.random.uniform(jax.random.fold_in(key, 23), (SB_HEADS,), jnp.float32, jnp.log(0.3), jnp.log(3.0))
    return spread - jnp.log(90.0 * TOKENS)


def draw_forget_minimum(key, part):
    streams = jax.random.split(jax.random.fold_in(key, 31), 3)
    ranking = jax.random.permutation(streams[0], REC_HEADS)
    slow_count = REC_HEADS // 2
    is_slow = (ranking < slow_count)[:, None]
    slow_gap = jnp.exp(jax.random.uniform(streams[1], (REC_HEADS, REC_KEY), jnp.float32, jnp.log(0.2), jnp.log(1.2))) / TOKENS
    fast_gap = jnp.exp(jax.random.uniform(streams[2], (REC_HEADS, REC_KEY), jnp.float32, jnp.log(0.04), jnp.log(0.1)))
    return 1.0 - jnp.where(is_slow, slow_gap, fast_gap)


def draw_decay_spikes(key, part):
    streams = jax.random.split(jax.random.fold_in(key, 47), 3)
    block_count = TOKENS // TOK_DEV
    block_rate = jnp.exp(jax.random.uniform(streams[0], (block_count, 1, REC_HEADS), jnp.float32, jnp.log(0.15), jnp.log(0.6))) / TOKENS
    steady = -jnp.broadcast_to(block_rate, (block_count, TOK_DEV, REC_HEADS)).reshape(TOKENS, REC_HEADS)
    places = jax.random.randint(streams[1], (3, REC_HEADS), 0, TOKENS)
    struck = jnp.arange(TOKENS, dtype=jnp.int32)[:, None, None] == places[None]
    depth = jnp.log(jax.random.uniform(streams[2], (3, REC_HEADS), jnp.float32, 0.5, 0.8))
    return steady + jnp.sum(jnp.where(struck, depth[None], 0.0), axis=1)


def steps_of(rng, shape, cuts, low, top_value):
    def one(dim, blocks):
        heights = jax.random.uniform(jax.random.fold_in(jax.random.fold_in(rng, 6), dim), (blocks,), jnp.float32, low / len(cuts), top_value / len(cuts))
        return jnp.repeat(jnp.exp(heights), shape[dim] // blocks).reshape((-1,) + (1,) * (len(shape) - dim - 1))

    gain = one(*cuts[0])
    for cut in cuts[1:]:
        gain = gain * one(*cut)
    return gain


def normal_values(rng, extent, scale, reach, cuts=(), kind=jnp.bfloat16):
    entries = jax.random.normal(rng, extent, jnp.float32) * scale
    if len(cuts) > 0:
        entries = steps_of(rng, extent, cuts, -0.22, 0.18) * entries
    return jnp.clip(entries, min=-reach, max=reach).astype(kind)


def setup_inputs(seed: int = 0) -> dict:
    arg_keys = jax.random.split(jax.random.key(seed), 16)
    return {
        "tokens": draw_tokens(jax.random.fold_in(arg_keys[15], 71), 0),
        "input_norm_gain": jnp.clip(1.0 + 0.18 * jax.random.normal(arg_keys[1], (D,), jnp.float32), 0.1, 1.9),
        "attention_query_weight": normal_values(arg_keys[2], (D, SB_HEADS * HEAD), (D // 3) ** -0.5, 0.21875, ((1, 8),)),
        "attention_key_weight": normal_values(arg_keys[3], (D, SB_HEADS * HEAD), (D // 3) ** -0.5, 0.21875, ((1, 8),)),
        "attention_value_weight": normal_values(arg_keys[4], (D, SB_HEADS * HEAD), D ** -0.5, 0.125, ((1, 8),)),
        "attention_score_bias": draw_attention_score_bias(jax.random.fold_in(arg_keys[15], 71), 0),
        "recurrence_query_weight": normal_values(arg_keys[6], (D, REC_HEADS * REC_KEY), D ** -0.5, 0.125, ((1, 8),)),
        "forget_weight": normal_values(arg_keys[7], (D, REC_HEADS * REC_KEY), D ** -0.5, 0.125, ((1, 8),)),
        "input_weight": normal_values(arg_keys[8], (D, REC_HEADS * REC_VAL), D ** -0.5, 0.125, ((1, 8),)),
        "output_gate_weight": normal_values(arg_keys[9], (D, REC_HEADS * REC_VAL), D ** -0.5, 0.125, ((1, 8),)),
        "forget_minimum": draw_forget_minimum(jax.random.fold_in(arg_keys[15], 71), 0),
        "decay_spikes": draw_decay_spikes(jax.random.fold_in(arg_keys[15], 71), 0),
        "head_norm_gain": jnp.clip(1.0 + 0.18 * jax.random.normal(arg_keys[12], (REC_VAL,), jnp.float32), 0.1, 1.9),
        "attention_output_weight": normal_values(arg_keys[13], (SB_HEADS * HEAD, D), (SB_HEADS * HEAD) ** -0.5, 0.25, ((0, 8),)),
        "recurrence_output_weight": normal_values(arg_keys[14], (REC_HEADS * REC_VAL, D), (REC_HEADS * REC_VAL) ** -0.5, 0.25, ((0, 8),)),
    }


epsilon = 1e-06

def project(scaled, inverse, weight):
    return (jnp.dot(scaled, weight, preferred_element_type=jnp.float32) * inverse).astype(jnp.bfloat16)

def stick_breaking(query_stick, key_stick, value_stick, attention_score_bias):
    block_count = TOKENS // TOK_DEV
    query_blocks = query_stick.reshape(block_count, TOK_DEV, SB_HEADS, HEAD)
    key_heads = key_stick.reshape(TOKENS, SB_HEADS, HEAD).astype(jnp.float32)
    value_heads = value_stick.reshape(TOKENS, SB_HEADS, HEAD).astype(jnp.float32)
    key_pos = jnp.arange(TOKENS, dtype=jnp.int32)

    def one_block(inputs):
        query_block, number = inputs
        query_pos = number * TOK_DEV + jnp.arange(TOK_DEV, dtype=jnp.int32)
        scores = jnp.einsum('qhd,khd->hqk', query_block.astype(jnp.float32), key_heads) * HEAD ** (-0.5)
        scores = scores + attention_score_bias[:, None, None]
        before = (key_pos[None, :] < query_pos[:, None])[None]
        log_rest = jnp.where(before, jax.nn.log_sigmoid(-scores), 0.0)
        later_sum = lax.cumsum(log_rest, axis=2, reverse=True) - log_rest
        weights = jnp.where(before, jnp.exp(jax.nn.log_sigmoid(scores) + later_sum), 0.0).astype(jnp.bfloat16)
        final_output = jnp.einsum('hqk,khd->qhd', weights.astype(jnp.float32), value_heads)
        return final_output.reshape(TOK_DEV, SB_HEADS * HEAD).astype(jnp.bfloat16)
    blocks = lax.map(one_block, (query_blocks, jnp.arange(block_count, dtype=jnp.int32)))
    return blocks.reshape(TOKENS, SB_HEADS * HEAD)

def linear_recurrence(query_rows, forget_rows, input_rows, gate_rows, forget_minimum, decay_spikes, head_norm_gain):
    peak_value = lax.Precision.HIGHEST
    raised_values = jax.nn.silu(query_rows.astype(jnp.float32)).reshape(TOKENS, REC_HEADS, REC_KEY)
    admitted_input = (1.0 - forget_minimum)[None] * jax.nn.sigmoid(-forget_rows.astype(jnp.float32).reshape(TOKENS, REC_HEADS, REC_KEY))
    forget_logarithm = jnp.log1p(-admitted_input) + decay_spikes[:, :, None]
    inputs = input_rows.astype(jnp.float32).reshape(TOKENS, REC_HEADS, REC_VAL)
    span_count = TOKENS // REC_SPAN
    causal = jnp.tril(jnp.ones((REC_SPAN, REC_SPAN), jnp.bool_))[:, :, None, None]

    def to_spans(array):
        return array.reshape(span_count, REC_SPAN, REC_HEADS, array.shape[-1])

    def advance(recurrent_memory, pieces):
        window_query, window_admitted, window_input, span_log = pieces
        running_total = jnp.cumsum(span_log, axis=0)
        log_gaps = running_total[:, None] - running_total[None, :]
        decay_table = jnp.where(causal, jnp.exp(jnp.where(causal, log_gaps, 0.0)), 0.0)
        inner_scores = jnp.einsum('thk,shk,tshk->hts', window_query, window_admitted, decay_table, precision=peak_value)
        final_output = jnp.einsum('hts,shv->thv', inner_scores, window_input, precision=peak_value)
        final_output = final_output + jnp.einsum('zbg,bgp->zbp', window_query * jnp.exp(running_total), recurrent_memory, precision=peak_value)
        window_total = running_total[-1]
        recurrent_memory = recurrent_memory * jnp.exp(window_total)[:, :, None] + jnp.einsum('rof,roi->ofi', window_admitted * jnp.exp(window_total[None] - running_total), window_input, precision=peak_value)
        return (recurrent_memory, final_output)
    start_memory = jnp.zeros((REC_HEADS, REC_KEY, REC_VAL), jnp.float32)
    memory_end, outputs = lax.scan(advance, start_memory, (to_spans(raised_values), to_spans(admitted_input), to_spans(inputs), to_spans(forget_logarithm)))
    outputs = outputs.reshape(TOKENS, REC_HEADS, REC_VAL)
    normed = outputs * lax.rsqrt(lax.optimization_barrier(jnp.mean(outputs * outputs, axis=2, keepdims=True)) + epsilon) * head_norm_gain
    gated_out = normed * jax.nn.silu(gate_rows.astype(jnp.float32).reshape(TOKENS, REC_HEADS, REC_VAL))
    return gated_out.reshape(TOKENS, REC_HEADS * REC_VAL).astype(jnp.bfloat16)

def reference(tokens, input_norm_gain, attention_query_weight, attention_key_weight, attention_value_weight, attention_score_bias, recurrence_query_weight, forget_weight, input_weight, output_gate_weight, forget_minimum, decay_spikes, head_norm_gain, attention_output_weight, recurrence_output_weight):
    values = tokens.astype(jnp.float32)
    scaled = (values * input_norm_gain[None, :]).astype(jnp.bfloat16)
    inverse = lax.rsqrt(lax.optimization_barrier(jnp.mean(values * values, axis=1, keepdims=True)) + epsilon)
    query_stick = project(scaled, inverse, attention_query_weight)
    key_stick = project(scaled, inverse, attention_key_weight)
    value_stick = project(scaled, inverse, attention_value_weight)
    query_rows = project(scaled, inverse, recurrence_query_weight)
    forget_rows = project(scaled, inverse, forget_weight)
    input_rows = project(scaled, inverse, input_weight)
    gate_rows = project(scaled, inverse, output_gate_weight)
    stick_heads = stick_breaking(query_stick, key_stick, value_stick, attention_score_bias)
    recurrence_heads = linear_recurrence(query_rows, forget_rows, input_rows, gate_rows, forget_minimum, decay_spikes, head_norm_gain)
    mixed_out = jnp.dot(stick_heads, attention_output_weight, preferred_element_type=jnp.float32)
    mixed_out = mixed_out + jnp.dot(recurrence_heads, recurrence_output_weight, preferred_element_type=jnp.float32)
    return mixed_out.astype(jnp.bfloat16)
```

```python
import functools

import jax
import jax.numpy as jnp
from jax import lax
from jax.experimental import pallas as pl
from jax.experimental.pallas import tpu as pltpu
from jax.sharding import Mesh
from jax.sharding import PartitionSpec as P

LOG2E = 1.4426950408889634
KB = 256

D = 2048
HEAD = 64
REC_KEY = 128
REC_VAL = 64
REC_SPAN = 64
SP = ("sp_0", "sp_1")


epsilon = 1e-06


def copy_for_each(array, axis):
    copies = jnp.broadcast_to(array, (lax.axis_size(axis), *array.shape))
    return lax.all_to_all(copies, axis, split_axis=0, concat_axis=0, tiled=True)


def laid_out(pieces, dim):
    lengths = list(pieces.shape[1:])
    lengths[dim] *= pieces.shape[0]
    return jnp.moveaxis(pieces, 0, dim).reshape(lengths)


def gathered_copies(array, axis, dim):
    pieces = copy_for_each(array, axis)
    return laid_out(pieces, dim)


def side_by_side(arrays, axis, dim, along):
    ends, at = ([], 0)
    for a in arrays[:-1]:
        at += a.shape[along]
        ends.append(at)
    both = jnp.concatenate(arrays, axis=along)
    return tuple(jnp.split(lax.all_gather(both, axis, axis=dim, tiled=True), ends, axis=along))


def neutral_like(array, identity):
    return jax.tree.map(
        lambda a, e: jnp.broadcast_to(jnp.asarray(e, a.dtype), a.shape), array, identity
    )


def entering(array, axes, combine, identity):
    before = start = neutral_like(array, identity)
    running = array
    for axis in reversed(axes):
        size, here = (lax.axis_size(axis), lax.axis_index(axis))
        pieces = jax.tree.map(lambda part: lax.all_gather(part, axis), running)
        inside, running = (start, start)
        for k in range(size):
            passed = k < here
            running = combine(running, jax.tree.map(lambda part: part[k], pieces))
            inside = jax.tree.map(lambda new, old: jnp.where(passed, new, old), running, inside)
        before = combine(inside, before)
    return before


def cut_along(array, dim, size):
    lengths = array.shape
    pieces = array.reshape(*lengths[:dim], size, lengths[dim] // size, *lengths[dim + 1 :])
    return jnp.moveaxis(pieces, dim, 0)


def summed_on_arrival(array, axis, dim):
    pieces = cut_along(array, dim, lax.axis_size(axis))
    arrived = lax.all_to_all(pieces, axis, split_axis=0, concat_axis=0, tiled=True)
    return arrived.astype(jnp.float32).sum(axis=0)


def dot(a, b, ta=False, tb=False):
    dims = (((0 if ta else 1,), (1 if tb else 0,)), ((), ()))
    return lax.dot_general(a, b, dims, preferred_element_type=jnp.float32)


def stick_tile(q, kv, tri, bias2, carry, keep=None):
    z = dot(q, kv, tb=True) * (LOG2E / 8.0) + bias2
    soft = jnp.maximum(z, jnp.log(1.0 + jnp.exp2(jnp.minimum(z, 30.0))) * LOG2E)
    if keep is not None:
        soft = jnp.where(keep, soft, 0.0)
    later = dot(soft.astype(jnp.bfloat16), tri)
    weight = jnp.exp2((z - soft) + (later + carry))
    if keep is not None:
        weight = jnp.where(keep, weight, 0.0)
    part = dot(weight.astype(jnp.bfloat16), kv)
    return part, carry + (later[:, 0:1] - soft[:, 0:1])


def stick_kernel(pos_ref, bias_ref, q_ref, kv_ref, out_ref, tri_ref, acc_ref, carry_ref):
    pos = pos_ref[0]
    bias2 = bias_ref[0] * LOG2E
    rows = lax.broadcasted_iota(jnp.int32, (KB, KB), 0)
    cols = lax.broadcasted_iota(jnp.int32, (KB, KB), 1)
    tri_ref[...] = jnp.where(rows > cols, -1.0, 0.0).astype(jnp.bfloat16)
    q = q_ref[...]
    zero = jnp.zeros((KB, 1), jnp.float32)
    part, carry = stick_tile(
        q, kv_ref[pl.ds(pl.multiple_of(pos * KB, KB), KB), :], tri_ref[...], bias2, zero, cols < rows
    )
    acc_ref[...] = part
    carry_ref[...] = jnp.broadcast_to(carry, carry_ref.shape)

    def block(i, _):
        at = pl.multiple_of((pos - 1 - i) * KB, KB)
        part, carry = stick_tile(
            q, kv_ref[pl.ds(at, KB), :], tri_ref[...], bias2, carry_ref[:, 0:1]
        )
        acc_ref[...] += part
        carry_ref[...] = jnp.broadcast_to(carry, carry_ref.shape)
        return 0

    lax.fori_loop(0, pos, block, 0)
    out_ref[...] = acc_ref[...].astype(jnp.bfloat16)


def stick(pos, bias, q, kv):
    return pl.pallas_call(
        stick_kernel,
        out_shape=jax.ShapeDtypeStruct((KB, 2 * HEAD), jnp.bfloat16),
        in_specs=[
            pl.BlockSpec(memory_space=pltpu.SMEM),
            pl.BlockSpec(memory_space=pltpu.SMEM),
            pl.BlockSpec(memory_space=pltpu.VMEM),
            pl.BlockSpec(memory_space=pltpu.VMEM),
        ],
        out_specs=pl.BlockSpec(memory_space=pltpu.VMEM),
        scratch_shapes=[
            pltpu.VMEM((KB, KB), jnp.bfloat16),
            pltpu.VMEM((KB, 2 * HEAD), jnp.float32),
            pltpu.VMEM((KB, 128), jnp.float32),
        ],
        name="stick",
    )(pos, bias, q, kv)


def scan_kernel(query_ref, forget_ref, input_ref, low_ref, spike_ref, out_ref, lift_ref, state_ref, total_ref):
    span = REC_SPAN
    rows = lax.broadcasted_iota(jnp.int32, (span, span), 0)
    cols = lax.broadcasted_iota(jnp.int32, (span, span), 1)
    causal = cols <= rows
    ones = jnp.where(causal, 1.0, 0.0)
    state = jnp.zeros((REC_VAL, REC_KEY), jnp.float32)
    offset = jnp.zeros((1, REC_KEY), jnp.float32)
    for n in range(query_ref.shape[0] // span):
        at = slice(n * span, (n + 1) * span)
        query = query_ref[at, :].astype(jnp.float32)
        lifted = query * jax.nn.sigmoid(query)
        intake = (1.0 - low_ref[...]) * jax.nn.sigmoid(-forget_ref[at, :].astype(jnp.float32))
        log_forget = jnp.log1p(-intake) + spike_ref[at, :]
        running = lax.dot_general(
            ones, log_forget, (((1,), (0,)), ((), ())),
            precision=lax.Precision.HIGHEST, preferred_element_type=jnp.float32,
        )
        total = running[span - 1 : span, :]
        middle = running[span // 2 - 1 : span // 2, :]
        value = input_ref[at, :]
        grown = (lifted * jnp.exp(running - middle)).astype(jnp.bfloat16)
        shrunk = (intake * jnp.exp(middle - running)).astype(jnp.bfloat16)
        inner = jnp.where(causal, dot(grown, shrunk, tb=True), 0.0)
        faded = (lifted * jnp.exp(running)).astype(jnp.bfloat16)
        out = dot(inner.astype(jnp.bfloat16), value) + dot(faded, state.astype(jnp.bfloat16), tb=True)
        out_ref[at, :] = out
        lift_ref[at, :] = (lifted * jnp.exp(running + offset)).astype(jnp.bfloat16)
        kept = (intake * jnp.exp(total - running)).astype(jnp.bfloat16)
        state = state * jnp.exp(total) + dot(value, kept, ta=True)
        offset = offset + total
    state_ref[...] = state
    total_ref[...] = offset


def local_scan(query, forget, inputs, low, spikes):
    n = query.shape[0]
    f32, bf16 = jnp.float32, jnp.bfloat16
    vmem = pl.BlockSpec(memory_space=pltpu.VMEM)
    return pl.pallas_call(
        scan_kernel,
        out_shape=(
            jax.ShapeDtypeStruct((n, REC_VAL), f32),
            jax.ShapeDtypeStruct((n, REC_KEY), bf16),
            jax.ShapeDtypeStruct((REC_VAL, REC_KEY), f32),
            jax.ShapeDtypeStruct((1, REC_KEY), f32),
        ),
        in_specs=[vmem] * 5,
        out_specs=(vmem,) * 4,
        name="local_scan",
    )(query, forget, inputs, low, spikes)


def shards(
    tokens,
    input_norm_gain,
    attention_query_weight,
    attention_key_weight,
    attention_value_weight,
    attention_score_bias,
    recurrence_query_weight,
    forget_weight,
    input_weight,
    output_gate_weight,
    forget_minimum,
    decay_spikes,
    head_norm_gain,
    attention_output_weight,
    recurrence_output_weight,
):
    row_count = tokens.shape[0]
    weights = (
        attention_query_weight,
        attention_key_weight,
        attention_value_weight,
        recurrence_query_weight,
        forget_weight,
        input_weight,
        output_gate_weight,
    )
    values = gathered_copies(tokens, "tp", 1).astype(jnp.float32)
    scaled = (values * input_norm_gain[None, :]).astype(jnp.bfloat16)
    partials = tuple(
        (jnp.dot(scaled, weight, preferred_element_type=jnp.float32) for weight in weights)
    )
    partials, squares = (partials, jnp.sum(values * values, axis=1))
    inverse = lax.rsqrt(squares / D + epsilon)[:, None]
    query_stick, key_stick, value_stick, query_rows, forget_rows, input_rows, gate_rows = tuple(
        ((running_total * inverse).astype(jnp.bfloat16) for running_total in partials)
    )
    position = lax.axis_index(SP)
    kv = jnp.concatenate([key_stick, value_stick], axis=1)
    kv_all = lax.all_gather(kv, SP, axis=0, tiled=True)
    padded = jnp.pad(query_stick, ((0, 0), (0, HEAD)))
    pos = position.astype(jnp.int32).reshape(1)
    stick_heads = stick(pos, attention_score_bias, padded, kv_all)[:, HEAD:]
    local_out, faded, memory_end, offset_end = local_scan(
        query_rows, forget_rows, input_rows, forget_minimum, decay_spikes
    )
    decay_all = jnp.exp(offset_end)

    def chain_combine(earlier, later_part):
        return (earlier[0] * later_part[0], earlier[1] * later_part[0] + later_part[1])

    identity = (jnp.ones_like(decay_all), jnp.zeros_like(memory_end))
    decay_before, incoming_state = entering((decay_all, memory_end), SP, chain_combine, identity)
    outputs = local_out + dot(faded, incoming_state.astype(jnp.bfloat16), tb=True)
    normed = (
        outputs
        * lax.rsqrt(jnp.mean(outputs * outputs, axis=1, keepdims=True) + epsilon)
        * head_norm_gain
    )
    recurrence_heads = (normed * jax.nn.silu(gate_rows.astype(jnp.float32))).astype(jnp.bfloat16)
    partial_out = jnp.dot(stick_heads, attention_output_weight, preferred_element_type=jnp.float32)
    partial_out = partial_out + jnp.dot(
        recurrence_heads, recurrence_output_weight, preferred_element_type=jnp.float32
    )
    mixed_out = summed_on_arrival(partial_out.astype(jnp.bfloat16), "tp", 1).astype(jnp.bfloat16)
    return mixed_out


def solution(mesh):
    torus = Mesh(mesh.devices.reshape(16, 4, mesh.shape["tp"]), ("sp_0", "sp_1", "tp"))
    placed = (
        P(SP, "tp"),
        P(),
        P(None, "tp"),
        P(None, "tp"),
        P(None, "tp"),
        P("tp"),
        P(None, "tp"),
        P(None, "tp"),
        P(None, "tp"),
        P(None, "tp"),
        P("tp", None),
        P(SP, "tp"),
        P(),
        P("tp", None),
        P("tp", None),
    )
    return jax.shard_map(
        shards, mesh=torus, in_specs=placed, out_specs=P(SP, "tp"), check_vma=False
    )
```

```python
import functools

import jax
import jax.numpy as jnp
from jax import lax
from jax.experimental import pallas as pl
from jax.experimental.pallas import tpu as pltpu
from jax.sharding import PartitionSpec as P

D = 2048
HEAD = 64
REC_KEY = 128
REC_VAL = 64
REC_SPAN = 64
TOK = 256
LOG2E = 1.4426950408889634
EARLY = 192
STATE_ROWS = REC_VAL + 8
epsilon = 1e-06
F32, BF16 = jnp.float32, jnp.bfloat16
VMEM = pl.BlockSpec(memory_space=pltpu.VMEM)
SMEM = pl.BlockSpec(memory_space=pltpu.SMEM)
ANY = pl.BlockSpec(memory_space=pl.ANY)
MESH = pl.DeviceIdType.MESH


def dot(a, b, ta=False, tb=False):
    dims = (((0 if ta else 1,), (1 if tb else 0,)), ((), ()))
    return lax.dot_general(a, b, dims, preferred_element_type=F32)


def to(src, dst, send, recv, sp):
    return pltpu.make_async_remote_copy(
        src_ref=src, dst_ref=dst, send_sem=send, recv_sem=recv,
        device_id={"sp": sp}, device_id_type=MESH,
    )


def place():
    sp = lax.axis_index("sp")
    return sp, sp // 16, (sp // 4) % 4, sp % 4


def greet(peers):
    barrier = pltpu.get_barrier_semaphore()
    for peer in peers:
        pl.semaphore_signal(barrier, inc=1, device_id={"sp": peer}, device_id_type=MESH)
    pl.semaphore_wait(barrier, len(peers))


def share_kernel(
    kv_ref, kv_hbm, query_ref, state_ref,
    early_ref, late_ref, queries_ref, before_ref, group_ref,
    rows_ref, planes_ref, send, recv, query_send, query_recv, own_sem,
):
    sp, c, zl, y = place()
    base = c * 16
    in_row = [base + zl * 4 + (y + d) % 4 for d in (1, 2, 3)]
    in_line = [base + ((zl + d) % 4) * 4 + y for d in (1, 2, 3)]
    far = [(sp + 16 * d) % 64 for d in (1, 2, 3)]
    own_early = pltpu.make_async_copy(kv_hbm.at[0:EARLY], early_ref.at[y, zl], own_sem.at[0])
    own_late = pltpu.make_async_copy(kv_hbm.at[EARLY:TOK], late_ref.at[zl, y], own_sem.at[1])
    own_early.start()
    own_late.start()
    rows_ref[y] = state_ref[...]
    greet(in_row + in_line + far)

    def step(n, src, dst, peers):
        return [to(src, dst, send.at[n, d], recv.at[n, d], peers[d]) for d in range(3)]

    first = (
        step(0, kv_ref.at[0:EARLY], early_ref.at[y, zl], in_line)
        + step(1, kv_ref.at[EARLY:TOK], late_ref.at[zl, y], in_row)
        + step(2, state_ref, rows_ref.at[y], in_row)
    )
    for copy in first:
        copy.start()
    for d in (1, 2, 3):

        @pl.when(c >= d)
        def _():
            to(
                query_ref, queries_ref.at[c - 1], query_send.at[d - 1], query_recv.at[c - 1], sp - 16 * d
            ).start()

    own_early.wait()
    own_late.wait()
    for copy in first:
        copy.wait_recv()
    second = step(3, early_ref.at[y], early_ref.at[y], in_row) + step(
        4, late_ref.at[zl], late_ref.at[zl], in_line
    )
    for copy in second:
        copy.start()
    state = rows_ref[0, 0:REC_VAL, :]
    total = rows_ref[0, REC_VAL : REC_VAL + 1, :]
    ahead = jnp.zeros_like(state)
    ahead_total = jnp.zeros_like(total)
    for n in range(1, 4):
        ahead = jnp.where(n <= y, state, ahead)
        ahead_total = jnp.where(n <= y, total, ahead_total)
        more = rows_ref[n, REC_VAL : REC_VAL + 1, :]
        state = state * jnp.exp(more) + rows_ref[n, 0:REC_VAL, :]
        total = total + more
    planes_ref[zl, 0:REC_VAL, :] = state
    planes_ref[zl, REC_VAL:STATE_ROWS, :] = jnp.broadcast_to(total, (8, REC_KEY))
    third = step(5, planes_ref.at[zl], planes_ref.at[zl], in_line)
    for copy in third:
        copy.start()
    for copy in third:
        copy.wait_recv()
    state = planes_ref[0, 0:REC_VAL, :]
    total = planes_ref[0, REC_VAL : REC_VAL + 1, :]
    low = jnp.zeros_like(state)
    low_total = jnp.zeros_like(total)
    for n in range(1, 4):
        low = jnp.where(n <= zl, state, low)
        low_total = jnp.where(n <= zl, total, low_total)
        more = planes_ref[n, REC_VAL : REC_VAL + 1, :]
        state = state * jnp.exp(more) + planes_ref[n, 0:REC_VAL, :]
        total = total + more
    group_ref[0:REC_VAL, :] = state
    group_ref[REC_VAL:STATE_ROWS, :] = jnp.broadcast_to(total, (8, REC_KEY))
    before_ref[0:REC_VAL, :] = low * jnp.exp(ahead_total) + ahead
    before_ref[REC_VAL:STATE_ROWS, :] = jnp.broadcast_to(low_total + ahead_total, (8, REC_KEY))
    for copy in second:
        copy.wait_recv()
    for n in (1, 2, 3):

        @pl.when(c < n)
        def _():
            to(
                query_ref, queries_ref.at[n - 1], query_send.at[0], query_recv.at[n - 1], sp
            ).wait_recv()

    for copy in first + second + third:
        copy.wait_send()
    for d in (1, 2, 3):

        @pl.when(c >= d)
        def _():
            to(
                query_ref, queries_ref.at[c - 1], query_send.at[d - 1], query_recv.at[c - 1], sp - 16 * d
            ).wait_send()


def share(kv, query, state):
    dma = pltpu.SemaphoreType.DMA
    return pl.pallas_call(
        share_kernel,
        out_shape=(
            jax.ShapeDtypeStruct((4, 4, EARLY, 128), BF16),
            jax.ShapeDtypeStruct((4, 4, TOK - EARLY, 128), BF16),
            jax.ShapeDtypeStruct((3, 128, 128), BF16),
            jax.ShapeDtypeStruct((STATE_ROWS, REC_KEY), F32),
            jax.ShapeDtypeStruct((STATE_ROWS, REC_KEY), F32),
        ),
        in_specs=[VMEM, ANY, VMEM, VMEM],
        out_specs=(VMEM,) * 5,
        scratch_shapes=[
            pltpu.VMEM((4, STATE_ROWS, REC_KEY), F32),
            pltpu.VMEM((4, STATE_ROWS, REC_KEY), F32),
            dma((6, 3)), dma((6, 3)), dma((3,)), dma((3,)), dma((2,)),
        ],
        compiler_params=pltpu.CompilerParams(collective_id=0, has_side_effects=True),
        name="share",
    )(kv, kv, query, state)


def stick_tile(q, kv, tri, bias2, keep=None):
    z = dot(q, kv, tb=True) * (LOG2E / 8.0) + bias2
    soft = jnp.maximum(z, jnp.log(1.0 + jnp.exp2(jnp.minimum(z, 30.0))) * LOG2E)
    if keep is not None:
        soft = jnp.where(keep, soft, 0.0)
    later = dot(soft.astype(BF16), tri)
    return z, soft, later


def stick_kernel(
    bias_ref, query_ref, queries_ref, early_ref, late_ref,
    own_ref, own_left_ref, far_ref, far_left_ref,
    q_ref, tri_ref, acc_ref, left_ref,
):
    sp, c, zl, y = place()
    here = zl * 4 + y
    bias2 = bias_ref[0] * LOG2E
    rows = lax.broadcasted_iota(jnp.int32, (TOK, TOK), 0)
    cols = lax.broadcasted_iota(jnp.int32, (TOK, TOK), 1)
    tri_ref[...] = jnp.where(rows > cols, -1.0, 0.0).astype(BF16)
    acc_ref[...] = jnp.zeros_like(acc_ref)
    left_ref[...] = jnp.zeros_like(left_ref)
    lane = lax.broadcasted_iota(jnp.int32, (128, 128), 1)
    for n in range(4):
        packed = (query_ref[...] if n == 0 else queries_ref[n - 1]).astype(F32)
        for half in range(2):
            part = packed if half == 0 else pltpu.roll(packed, 64, 1)
            at = n * TOK + half * 128
            q_ref[at : at + 128, :] = jnp.where(lane < HEAD, part, 0.0).astype(BF16)

    def pair(i, _):
        tri = tri_ref[...]
        q_own, q_far = q_ref[0:TOK, :], q_ref[TOK:, :]
        kvs, own, far = [], [], []
        for u in range(2):
            m = 15 - 2 * i - u
            kv = jnp.concatenate([early_ref[m % 4, m // 4], late_ref[m // 4, m % 4]], axis=0)
            keep = cols - rows < (here - m) * TOK
            kvs.append(kv)
            own.append(stick_tile(q_own, kv, tri, bias2, keep) + (keep,))
            far.append(stick_tile(q_far, kv, tri, bias2))
        left_own, left_far = left_ref[0:TOK, 0:1], left_ref[TOK:, 0:1]
        acc_own, acc_far = acc_ref[0:TOK, :], acc_ref[TOK:, :]
        for u in range(2):
            z, soft, later, keep = own[u]
            weight = jnp.where(keep, jnp.exp2((z - soft) + (later + left_own)), 0.0)
            acc_own = acc_own + dot(weight.astype(BF16), kvs[u])
            left_own = left_own + (later[:, 0:1] - soft[:, 0:1])
            z, soft, later = far[u]
            weight = jnp.exp2((z - soft) + (later + left_far))
            acc_far = acc_far + dot(weight.astype(BF16), kvs[u])
            left_far = left_far + (later[:, 0:1] - soft[:, 0:1])
        acc_ref[0:TOK, :] = acc_own
        acc_ref[TOK:, :] = acc_far
        left_ref[0:TOK, :] = jnp.broadcast_to(left_own, (TOK, 128))
        left_ref[TOK:, :] = jnp.broadcast_to(left_far, (3 * TOK, 128))
        return 0

    lax.fori_loop(0, 8, pair, 0)
    own_ref[...] = acc_ref[0:TOK, :]
    own_left_ref[...] = left_ref[0:TOK, :]
    for n in range(3):
        at = (n + 1) * TOK
        top = acc_ref[at : at + 128, :]
        low = pltpu.roll(acc_ref[at + 128 : at + 256, :], 64, 1)
        far_ref[n] = jnp.where(lane < HEAD, low, top).astype(BF16)
        for half in range(2):
            turned = jnp.transpose(left_ref[at + half * 128 : at + half * 128 + 128, :])
            far_left_ref[n, :, half * 128 : half * 128 + 128] = turned[0:8, :]


def stick(bias, query, queries, early, late):
    return pl.pallas_call(
        stick_kernel,
        out_shape=(
            jax.ShapeDtypeStruct((TOK, 128), F32),
            jax.ShapeDtypeStruct((TOK, 128), F32),
            jax.ShapeDtypeStruct((3, 128, 128), BF16),
            jax.ShapeDtypeStruct((3, 8, TOK), F32),
        ),
        in_specs=[SMEM, VMEM, VMEM, VMEM, VMEM],
        out_specs=(VMEM,) * 4,
        scratch_shapes=[
            pltpu.VMEM((4 * TOK, 128), BF16),
            pltpu.VMEM((TOK, TOK), BF16),
            pltpu.VMEM((4 * TOK, 128), F32),
            pltpu.VMEM((4 * TOK, 128), F32),
        ],
        name="stick",
    )(bias, query, queries, early, late)


def finish_kernel(
    own_ref, own_left_ref, far_ref, far_left_ref, before_ref, group_ref,
    local_ref, faded_ref, gate_ref, gain_ref,
    heads_ref,
    part_ref, part_left_ref, states_ref, acc_ref, left_ref, in_ref, send, recv,
):
    sp, c, zl, y = place()
    greet([(sp + 16 * d) % 64 for d in (1, 2, 3)])

    def copies(n, there, to_sp):
        pairs = (
            (far_ref.at[there - 1], part_ref.at[c]),
            (far_left_ref.at[there - 1], part_left_ref.at[c]),
            (group_ref, states_ref.at[c]),
        )
        return [
            to(src, dst, send.at[k, n], recv.at[k, c], to_sp) for k, (src, dst) in enumerate(pairs)
        ]

    def arrivals(source):
        pairs = ((far_ref.at[0], part_ref), (far_left_ref.at[0], part_left_ref), (group_ref, states_ref))
        return [
            to(src, dst.at[source], send.at[k, 0], recv.at[k, source], sp)
            for k, (src, dst) in enumerate(pairs)
        ]

    for d in (1, 2, 3):

        @pl.when(c + d < 4)
        def _():
            for copy in copies(d - 1, c + d, sp + 16 * d):
                copy.start()

    acc_ref[...] = own_ref[...]
    left_ref[...] = own_left_ref[...]
    in_ref[...] = jnp.zeros_like(in_ref)
    for g in (2, 1, 0):

        @pl.when(g < c)
        def _():
            for copy in arrivals(g)[0:2]:
                copy.wait_recv()
            packed = part_ref[g].astype(F32)
            scale = jnp.exp2(left_ref[...])
            acc_ref[0:128, :] += packed * scale[0:128, :]
            acc_ref[128:256, :] += pltpu.roll(packed, 64, 1) * scale[128:256, :]
            for half in range(2):
                at = slice(half * 128, half * 128 + 128)
                flat = jnp.broadcast_to(part_left_ref[g, 0:1, at], (128, 128))
                left_ref[at, :] += jnp.transpose(flat)

    for g in (0, 1, 2):

        @pl.when(g < c)
        def _():
            arrivals(g)[2].wait_recv()
            in_ref[...] = in_ref[...] * jnp.exp(states_ref[g, REC_VAL : REC_VAL + 1, :]) + states_ref[
                g, 0:REC_VAL, :
            ]

    state = in_ref[...] * jnp.exp(before_ref[REC_VAL : REC_VAL + 1, :]) + before_ref[0:REC_VAL, :]
    raw = local_ref[...] + dot(faded_ref[...], state.astype(BF16), tb=True)
    normed = raw * lax.rsqrt(jnp.mean(raw * raw, axis=1, keepdims=True) + epsilon) * gain_ref[...]
    gate = gate_ref[...].astype(F32)
    state_heads = normed * (gate * jax.nn.sigmoid(gate))
    heads_ref[:, 0:REC_VAL] = state_heads.astype(BF16)
    heads_ref[:, REC_VAL:] = acc_ref[:, HEAD:].astype(BF16)
    for d in (1, 2, 3):

        @pl.when(c + d < 4)
        def _():
            for copy in copies(d - 1, c + d, sp + 16 * d):
                copy.wait_send()


def finish(*operands):
    dma = pltpu.SemaphoreType.DMA
    return pl.pallas_call(
        finish_kernel,
        out_shape=jax.ShapeDtypeStruct((TOK, 128), BF16),
        in_specs=[VMEM] * 10,
        out_specs=VMEM,
        scratch_shapes=[
            pltpu.VMEM((3, 128, 128), BF16),
            pltpu.VMEM((3, 8, TOK), F32),
            pltpu.VMEM((3, STATE_ROWS, REC_KEY), F32),
            pltpu.VMEM((TOK, 128), F32),
            pltpu.VMEM((TOK, 128), F32),
            pltpu.VMEM((REC_VAL, REC_KEY), F32),
            dma((3, 3)), dma((3, 3)),
        ],
        compiler_params=pltpu.CompilerParams(collective_id=1, has_side_effects=True),
        name="finish",
    )(*operands)


def scan_kernel(query_ref, forget_ref, input_ref, low_ref, spike_ref, out_ref, lift_ref, state_ref):
    span = REC_SPAN
    rows = lax.broadcasted_iota(jnp.int32, (span, span), 0)
    cols = lax.broadcasted_iota(jnp.int32, (span, span), 1)
    causal = cols <= rows
    ones = jnp.where(causal, 1.0, 0.0)
    state = jnp.zeros((REC_VAL, REC_KEY), F32)
    offset = jnp.zeros((1, REC_KEY), F32)
    for n in range(query_ref.shape[0] // span):
        at = slice(n * span, (n + 1) * span)
        query = query_ref[at, :].astype(F32)
        lifted = query * jax.nn.sigmoid(query)
        intake = (1.0 - low_ref[...]) * jax.nn.sigmoid(-forget_ref[at, :].astype(F32))
        log_forget = jnp.log1p(-intake) + spike_ref[at, :]
        running = lax.dot_general(
            ones, log_forget, (((1,), (0,)), ((), ())),
            precision=lax.Precision.HIGHEST, preferred_element_type=F32,
        )
        total = running[span - 1 : span, :]
        middle = running[span // 2 - 1 : span // 2, :]
        value = input_ref[at, :]
        grown = (lifted * jnp.exp(running - middle)).astype(BF16)
        shrunk = (intake * jnp.exp(middle - running)).astype(BF16)
        inner = jnp.where(causal, dot(grown, shrunk, tb=True), 0.0)
        faded = (lifted * jnp.exp(running)).astype(BF16)
        out_ref[at, :] = dot(inner.astype(BF16), value) + dot(faded, state.astype(BF16), tb=True)
        lift_ref[at, :] = (lifted * jnp.exp(running + offset)).astype(BF16)
        kept = (intake * jnp.exp(total - running)).astype(BF16)
        state = state * jnp.exp(total) + dot(value, kept, ta=True)
        offset = offset + total
    state_ref[0:REC_VAL, :] = state
    state_ref[REC_VAL:STATE_ROWS, :] = jnp.broadcast_to(offset, (8, REC_KEY))


def local_scan(query, forget, inputs, low, spikes):
    n = query.shape[0]
    return pl.pallas_call(
        scan_kernel,
        out_shape=(
            jax.ShapeDtypeStruct((n, REC_VAL), F32),
            jax.ShapeDtypeStruct((n, REC_KEY), BF16),
            jax.ShapeDtypeStruct((STATE_ROWS, REC_KEY), F32),
        ),
        in_specs=[VMEM] * 5,
        out_specs=(VMEM,) * 3,
        name="local_scan",
    )(query, forget, inputs, low, spikes)


def gathered_copies(array, axis, dim):
    copies = jnp.broadcast_to(array, (lax.axis_size(axis), *array.shape))
    pieces = lax.all_to_all(copies, axis, split_axis=0, concat_axis=0, tiled=True)
    lengths = list(array.shape)
    lengths[dim] *= pieces.shape[0]
    return jnp.moveaxis(pieces, 0, dim).reshape(lengths)


def summed_on_arrival(array, axis, dim):
    size, lengths = lax.axis_size(axis), array.shape
    pieces = array.reshape(*lengths[:dim], size, lengths[dim] // size, *lengths[dim + 1 :])
    pieces = jnp.moveaxis(pieces, dim, 0)
    arrived = lax.all_to_all(pieces, axis, split_axis=0, concat_axis=0, tiled=True)
    return arrived.astype(F32).sum(axis=0)


def shards(
    tokens,
    input_norm_gain,
    attention_query_weight,
    attention_key_weight,
    attention_value_weight,
    attention_score_bias,
    recurrence_query_weight,
    forget_weight,
    input_weight,
    output_gate_weight,
    forget_minimum,
    decay_spikes,
    head_norm_gain,
    attention_output_weight,
    recurrence_output_weight,
):
    values = gathered_copies(tokens, "tp", 1).astype(F32)
    scaled = (values * input_norm_gain[None, :]).astype(BF16)
    weights = (
        attention_query_weight,
        attention_key_weight,
        attention_value_weight,
        recurrence_query_weight,
        forget_weight,
        input_weight,
        output_gate_weight,
    )
    inverse = lax.rsqrt(jnp.sum(values * values, axis=1) / D + epsilon)[:, None]
    query_stick, key_stick, value_stick, query_rows, forget_rows, input_rows, gate_rows = (
        (jnp.dot(scaled, weight, preferred_element_type=F32) * inverse).astype(BF16)
        for weight in weights
    )
    kv = jnp.concatenate([key_stick, value_stick], axis=1)
    query = jnp.concatenate([query_stick[0:128], query_stick[128:256]], axis=1)
    local_out, faded, state = local_scan(
        query_rows, forget_rows, input_rows, forget_minimum, decay_spikes
    )
    early, late, queries, before, group = share(kv, query, state)
    own, own_left, far, far_left = stick(attention_score_bias, query, queries, early, late)
    heads = finish(
        own, own_left, far, far_left, before, group, local_out, faded, gate_rows, head_norm_gain[None, :]
    )
    output_weight = jnp.concatenate([recurrence_output_weight, attention_output_weight], axis=0)
    partial_out = jnp.dot(heads, output_weight, preferred_element_type=F32)
    return summed_on_arrival(partial_out.astype(BF16), "tp", 1).astype(BF16)


def solution(mesh):
    placed = (
        P("sp", "tp"),
        P(),
        P(None, "tp"),
        P(None, "tp"),
        P(None, "tp"),
        P("tp"),
        P(None, "tp"),
        P(None, "tp"),
        P(None, "tp"),
        P(None, "tp"),
        P("tp", None),
        P("sp", "tp"),
        P(),
        P("tp", None),
        P("tp", None),
    )
    return jax.shard_map(
        shards, mesh=mesh, in_specs=placed, out_specs=P("sp", "tp"), check_vma=False
    )
```

```python
import functools

import jax
import jax.numpy as jnp
from jax import lax
from jax.experimental import pallas as pl
from jax.experimental.pallas import tpu as pltpu
from jax.sharding import PartitionSpec as P

D = 2048
HEAD = 64
REC_KEY = 128
REC_VAL = 64
REC_SPAN = 64
TOK = 256
LOG2E = 1.4426950408889634
EARLY = 192
STATE_ROWS = REC_VAL + 8
epsilon = 1e-06
F32, BF16 = jnp.float32, jnp.bfloat16
VMEM = pl.BlockSpec(memory_space=pltpu.VMEM)
SMEM = pl.BlockSpec(memory_space=pltpu.SMEM)
ANY = pl.BlockSpec(memory_space=pl.ANY)
MESH = pl.DeviceIdType.MESH


def dot(a, b, ta=False, tb=False):
    dims = (((0 if ta else 1,), (1 if tb else 0,)), ((), ()))
    return lax.dot_general(a, b, dims, preferred_element_type=F32)


def to(src, dst, send, recv, sp):
    return pltpu.make_async_remote_copy(
        src_ref=src, dst_ref=dst, send_sem=send, recv_sem=recv,
        device_id={"sp": sp}, device_id_type=MESH,
    )


def place():
    sp = lax.axis_index("sp")
    return sp, sp // 16, (sp // 4) % 4, sp % 4


def greet(peers, lane_peers=(), meanwhile=lambda: None):
    barrier = pltpu.get_barrier_semaphore()
    for peer in peers:
        pl.semaphore_signal(barrier, inc=1, device_id={"sp": peer}, device_id_type=MESH)
    for peer in lane_peers:
        pl.semaphore_signal(barrier, inc=1, device_id={"tp": peer}, device_id_type=MESH)
    meanwhile()
    pl.semaphore_wait(barrier, len(peers) + len(lane_peers))


def lanes():
    tp = lax.axis_index("tp")
    x, core = tp // 2, tp % 2
    return tp, tp + 1 - 2 * core, (tp + 2) % 8, (tp + 6) % 8, (tp + 4) % 8, 1 - 2 * core


def ring_gather(chunk_ref, slots_ref, send, recv, meanwhile, use):
    tp, partner, right, left, across, twist = lanes()
    half = chunk_ref.shape[0] // 2
    top, low = slice(0, half), slice(half, 2 * half)

    def copy(n, src, dst, target):
        return pltpu.make_async_remote_copy(
            src_ref=src, dst_ref=dst, send_sem=send.at[n], recv_sem=recv.at[n],
            device_id={"tp": target}, device_id_type=MESH,
        )

    def relay(n, source, part, target):
        return copy(n, slots_ref.at[source, part], slots_ref.at[source, part], target)

    barrier = pltpu.get_barrier_semaphore()
    for peer in (partner, right, left):
        pl.semaphore_signal(barrier, inc=1, device_id={"tp": peer}, device_id_type=MESH)
    pl.semaphore_wait(barrier, 3)
    copies = [
        copy(0, chunk_ref, slots_ref.at[tp], partner),
        copy(1, chunk_ref.at[top], slots_ref.at[tp, top], right),
        copy(2, chunk_ref.at[low], slots_ref.at[tp, low], left),
        copy(3, chunk_ref.at[low], slots_ref.at[tp, low], right),
        copy(4, chunk_ref.at[top], slots_ref.at[tp, top], left),
        relay(5, left, top, right),
        relay(6, right, low, left),
        relay(7, left, top, partner),
        relay(8, right, low, partner),
        relay(9, left, low, partner),
        relay(10, right, top, partner),
        relay(11, across, top, partner),
        relay(12, across, low, partner),
    ]
    for n in range(5):
        copies[n].start()
    meanwhile()
    use(tp, chunk_ref)
    copies[1].wait_recv()
    copies[5].start()
    copies[7].start()
    copies[2].wait_recv()
    copies[6].start()
    copies[8].start()
    copies[0].wait_recv()
    use(partner, slots_ref.at[partner])
    copies[3].wait_recv()
    copies[9].start()
    copies[4].wait_recv()
    copies[10].start()
    use(left, slots_ref.at[left])
    use(right, slots_ref.at[right])
    copies[7].wait_recv()
    copies[9].wait_recv()
    use(left + twist, slots_ref.at[left + twist])
    copies[8].wait_recv()
    copies[10].wait_recv()
    use(right + twist, slots_ref.at[right + twist])
    copies[5].wait_recv()
    copies[11].start()
    copies[6].wait_recv()
    copies[12].start()
    use(across, slots_ref.at[across])
    copies[11].wait_recv()
    copies[12].wait_recv()
    use(across + twist, slots_ref.at[across + twist])
    for one in copies:
        one.wait_send()


def project_kernel(
    token_ref, gain_ref, query_w, key_w, value_w, rec_w, forget_w, input_w, gate_w,
    kv_ref, query_ref, rec_ref, forget_ref, input_ref, gate_ref,
    slots_ref, raw_ref, weight_ref, acc_ref, square_ref, send, recv, load,
):
    narrow = (key_w, value_w, input_w, gate_w, query_w)
    loads = [pltpu.make_async_copy(w, raw_ref.at[n], load.at[n]) for n, w in enumerate(narrow)]
    loads += [
        pltpu.make_async_copy(rec_w, weight_ref.at[:, 128:256], load.at[5]),
        pltpu.make_async_copy(forget_w, weight_ref.at[:, 256:384], load.at[6]),
    ]
    for one in loads:
        one.start()
    acc_ref[...] = jnp.zeros_like(acc_ref)
    square_ref[...] = jnp.zeros_like(square_ref)

    def meanwhile():
        for one in loads:
            one.wait()

        def assemble(n, _):
            at = pl.ds(pl.multiple_of(n * 256, 256), 256)
            weight_ref[at, 0:128] = jnp.concatenate([raw_ref[0, at, :], raw_ref[1, at, :]], axis=1)
            weight_ref[at, 384:512] = jnp.concatenate([raw_ref[2, at, :], raw_ref[3, at, :]], axis=1)
            weight_ref[at, 512:576] = raw_ref[4, at, :]
            return 0

        lax.fori_loop(0, 8, assemble, 0)

    def use(source, ref):
        values = ref[...].astype(F32)
        squares = values * values
        square_ref[...] += squares[:, 0:128] + squares[:, 128:256]
        scaled = (values * gain_ref[pl.ds(source, 1), :]).astype(BF16)
        at = pl.ds(pl.multiple_of(source * 256, 256), 256)
        acc_ref[...] += dot(scaled, weight_ref[at, :])

    ring_gather(token_ref, slots_ref, send, recv, meanwhile, use)
    inverse = lax.rsqrt(jnp.sum(square_ref[...], axis=1, keepdims=True) / D + epsilon)
    kv_ref[...] = (acc_ref[:, 0:128] * inverse).astype(BF16)
    rec_ref[...] = (acc_ref[:, 128:256] * inverse).astype(BF16)
    forget_ref[...] = (acc_ref[:, 256:384] * inverse).astype(BF16)
    input_ref[...] = (acc_ref[:, 384:448] * inverse).astype(BF16)
    gate_ref[...] = (acc_ref[:, 448:512] * inverse).astype(BF16)
    query = (acc_ref[:, 512:576] * inverse).astype(BF16)
    query_ref[...] = jnp.concatenate([query[0:128], query[128:256]], axis=1)


def project(tokens, gain, *weights):
    dma = pltpu.SemaphoreType.DMA
    wide, narrow = jax.ShapeDtypeStruct((TOK, 128), BF16), jax.ShapeDtypeStruct((TOK, 64), BF16)
    return pl.pallas_call(
        project_kernel,
        out_shape=(wide, jax.ShapeDtypeStruct((128, 128), BF16), wide, wide, narrow, narrow),
        in_specs=[VMEM, VMEM] + [ANY] * 7,
        out_specs=(VMEM,) * 6,
        scratch_shapes=[
            pltpu.VMEM((8, TOK, 256), BF16),
            pltpu.VMEM((5, D, 64), BF16),
            pltpu.VMEM((D, 576), BF16),
            pltpu.VMEM((TOK, 576), F32),
            pltpu.VMEM((TOK, 128), F32),
            dma((13,)), dma((13,)), dma((7,)),
        ],
        compiler_params=pltpu.CompilerParams(collective_id=2, has_side_effects=True),
        name="project",
    )(tokens, gain, *weights)


def output_kernel(heads_ref, weight_ref, out_ref, slots_ref, acc_ref, send, recv):
    acc_ref[...] = jnp.zeros_like(acc_ref)

    def use(source, ref):
        acc_ref[...] += dot(ref[...], weight_ref[source])

    ring_gather(heads_ref, slots_ref, send, recv, lambda: None, use)
    out_ref[...] = acc_ref[...].astype(BF16)


def output(heads, weight):
    dma = pltpu.SemaphoreType.DMA
    return pl.pallas_call(
        output_kernel,
        out_shape=jax.ShapeDtypeStruct((TOK, 256), BF16),
        in_specs=[VMEM, VMEM],
        out_specs=VMEM,
        scratch_shapes=[
            pltpu.VMEM((8, TOK, 128), BF16),
            pltpu.VMEM((TOK, 256), F32),
            dma((13,)), dma((13,)),
        ],
        compiler_params=pltpu.CompilerParams(collective_id=3, has_side_effects=True),
        name="output",
    )(heads, weight)


def local_scan(query_ref, forget_ref, input_ref, low_ref, spike_ref, out_ref, lift_ref, state_ref):
    span = REC_SPAN
    rows = lax.broadcasted_iota(jnp.int32, (span, span), 0)
    cols = lax.broadcasted_iota(jnp.int32, (span, span), 1)
    causal = cols <= rows
    ones = jnp.where(causal, 1.0, 0.0)
    state = jnp.zeros((REC_VAL, REC_KEY), F32)
    offset = jnp.zeros((1, REC_KEY), F32)
    for n in range(query_ref.shape[0] // span):
        at = slice(n * span, (n + 1) * span)
        query = query_ref[at, :].astype(F32)
        lifted = query * jax.nn.sigmoid(query)
        intake = (1.0 - low_ref[...]) * jax.nn.sigmoid(-forget_ref[at, :].astype(F32))
        log_forget = jnp.log1p(-intake) + spike_ref[at, :]
        running = lax.dot_general(
            ones, log_forget, (((1,), (0,)), ((), ())),
            precision=lax.Precision.HIGHEST, preferred_element_type=F32,
        )
        total = running[span - 1 : span, :]
        middle = running[span // 2 - 1 : span // 2, :]
        value = input_ref[at, :]
        grown = (lifted * jnp.exp(running - middle)).astype(BF16)
        shrunk = (intake * jnp.exp(middle - running)).astype(BF16)
        inner = jnp.where(causal, dot(grown, shrunk, tb=True), 0.0)
        faded = (lifted * jnp.exp(running)).astype(BF16)
        out_ref[at, :] = dot(inner.astype(BF16), value) + dot(faded, state.astype(BF16), tb=True)
        lift_ref[at, :] = (lifted * jnp.exp(running + offset)).astype(BF16)
        kept = (intake * jnp.exp(total - running)).astype(BF16)
        state = state * jnp.exp(total) + dot(value, kept, ta=True)
        offset = offset + total
    state_ref[0:REC_VAL, :] = state
    state_ref[REC_VAL:STATE_ROWS, :] = jnp.broadcast_to(offset, (8, REC_KEY))


def share_kernel(
    kv_ref, kv_hbm, query_ref, rec_ref, forget_ref, input_ref, low_ref, spike_ref, rec_out_w, att_out_w,
    early_ref, late_ref, queries_ref, before_ref, group_ref, local_ref, faded_ref, columns_ref,
    state_ref, rows_ref, planes_ref, send, recv, query_send, query_recv, column_send, column_recv, own_sem,
):
    sp, c, zl, y = place()
    base = c * 16
    in_row = [base + zl * 4 + (y + d) % 4 for d in (1, 2, 3)]
    in_line = [base + ((zl + d) % 4) * 4 + y for d in (1, 2, 3)]
    far = [(sp + 16 * d) % 64 for d in (1, 2, 3)]
    own_early = pltpu.make_async_copy(kv_hbm.at[0:EARLY], early_ref.at[y, zl], own_sem.at[0])
    own_late = pltpu.make_async_copy(kv_hbm.at[EARLY:TOK], late_ref.at[zl, y], own_sem.at[1])
    own_early.start()
    own_late.start()
    tp = lax.axis_index("tp")
    lane_peers = [(tp + d) % 8 for d in range(1, 8)]

    def columns(w, there):
        return w.at[:, pl.ds(pl.multiple_of(there * 256, 256), 256)]

    own_columns = [
        pltpu.make_async_copy(columns(w, tp), columns_ref.at[tp, n * 64 : n * 64 + 64], own_sem.at[2 + n])
        for n, w in enumerate((rec_out_w, att_out_w))
    ]
    column_copies = [
        pltpu.make_async_remote_copy(
            src_ref=columns(w, there), dst_ref=columns_ref.at[tp, n * 64 : n * 64 + 64],
            send_sem=column_send.at[n, d], recv_sem=column_recv.at[n, d],
            device_id={"tp": there}, device_id_type=MESH,
        )
        for n, w in enumerate((rec_out_w, att_out_w))
        for d, there in enumerate(lane_peers)
    ]

    def scan():
        local_scan(
            rec_ref, forget_ref, input_ref, low_ref, spike_ref, local_ref, faded_ref, state_ref
        )
        rows_ref[y] = state_ref[...]

    greet(in_row + in_line + far, lane_peers, scan)

    def step(n, src, dst, peers):
        return [to(src, dst, send.at[n, d], recv.at[n, d], peers[d]) for d in range(3)]

    first = (
        step(0, kv_ref.at[0:EARLY], early_ref.at[y, zl], in_line)
        + step(1, kv_ref.at[EARLY:TOK], late_ref.at[zl, y], in_row)
        + step(2, state_ref, rows_ref.at[y], in_row)
    )
    for copy in first:
        copy.start()
    for d in (1, 2, 3):

        @pl.when(c >= d)
        def _():
            to(
                query_ref, queries_ref.at[c - 1], query_send.at[d - 1], query_recv.at[c - 1], sp - 16 * d
            ).start()

    for copy in own_columns + column_copies:
        copy.start()
    own_early.wait()
    own_late.wait()
    for copy in first:
        copy.wait_recv()
    second = step(3, early_ref.at[y], early_ref.at[y], in_row) + step(
        4, late_ref.at[zl], late_ref.at[zl], in_line
    )
    for copy in second:
        copy.start()
    state = rows_ref[0, 0:REC_VAL, :]
    total = rows_ref[0, REC_VAL : REC_VAL + 1, :]
    ahead = jnp.zeros_like(state)
    ahead_total = jnp.zeros_like(total)
    for n in range(1, 4):
        ahead = jnp.where(n <= y, state, ahead)
        ahead_total = jnp.where(n <= y, total, ahead_total)
        more = rows_ref[n, REC_VAL : REC_VAL + 1, :]
        state = state * jnp.exp(more) + rows_ref[n, 0:REC_VAL, :]
        total = total + more
    planes_ref[zl, 0:REC_VAL, :] = state
    planes_ref[zl, REC_VAL:STATE_ROWS, :] = jnp.broadcast_to(total, (8, REC_KEY))
    third = step(5, planes_ref.at[zl], planes_ref.at[zl], in_line)
    for copy in third:
        copy.start()
    for copy in third:
        copy.wait_recv()
    state = planes_ref[0, 0:REC_VAL, :]
    total = planes_ref[0, REC_VAL : REC_VAL + 1, :]
    low = jnp.zeros_like(state)
    low_total = jnp.zeros_like(total)
    for n in range(1, 4):
        low = jnp.where(n <= zl, state, low)
        low_total = jnp.where(n <= zl, total, low_total)
        more = planes_ref[n, REC_VAL : REC_VAL + 1, :]
        state = state * jnp.exp(more) + planes_ref[n, 0:REC_VAL, :]
        total = total + more
    group_ref[0:REC_VAL, :] = state
    group_ref[REC_VAL:STATE_ROWS, :] = jnp.broadcast_to(total, (8, REC_KEY))
    before_ref[0:REC_VAL, :] = low * jnp.exp(ahead_total) + ahead
    before_ref[REC_VAL:STATE_ROWS, :] = jnp.broadcast_to(low_total + ahead_total, (8, REC_KEY))
    for copy in second:
        copy.wait_recv()
    for n in (1, 2, 3):

        @pl.when(c < n)
        def _():
            to(
                query_ref, queries_ref.at[n - 1], query_send.at[0], query_recv.at[n - 1], sp
            ).wait_recv()

    for copy in own_columns:
        copy.wait()
    for copy in column_copies:
        copy.wait_recv()
    for copy in first + second + third + column_copies:
        copy.wait_send()
    for d in (1, 2, 3):

        @pl.when(c >= d)
        def _():
            to(
                query_ref, queries_ref.at[c - 1], query_send.at[d - 1], query_recv.at[c - 1], sp - 16 * d
            ).wait_send()


def share(kv, query, *operands):
    dma = pltpu.SemaphoreType.DMA
    return pl.pallas_call(
        share_kernel,
        out_shape=(
            jax.ShapeDtypeStruct((4, 4, EARLY, 128), BF16),
            jax.ShapeDtypeStruct((4, 4, TOK - EARLY, 128), BF16),
            jax.ShapeDtypeStruct((3, 128, 128), BF16),
            jax.ShapeDtypeStruct((STATE_ROWS, REC_KEY), F32),
            jax.ShapeDtypeStruct((STATE_ROWS, REC_KEY), F32),
            jax.ShapeDtypeStruct((TOK, REC_VAL), F32),
            jax.ShapeDtypeStruct((TOK, REC_KEY), BF16),
            jax.ShapeDtypeStruct((8, 128, 256), BF16),
        ),
        in_specs=[VMEM, ANY] + [VMEM] * 6 + [ANY] * 2,
        out_specs=(VMEM,) * 8,
        scratch_shapes=[
            pltpu.VMEM((STATE_ROWS, REC_KEY), F32),
            pltpu.VMEM((4, STATE_ROWS, REC_KEY), F32),
            pltpu.VMEM((4, STATE_ROWS, REC_KEY), F32),
            dma((6, 3)), dma((6, 3)), dma((3,)), dma((3,)), dma((2, 7)), dma((2, 7)), dma((4,)),
        ],
        compiler_params=pltpu.CompilerParams(collective_id=0, has_side_effects=True),
        name="share",
    )(kv, kv, query, *operands)


def stick_tile(q, kv, tri, bias2, keep=None):
    z = dot(q, kv, tb=True) * (LOG2E / 8.0) + bias2
    soft = jnp.maximum(z, jnp.log(1.0 + jnp.exp2(jnp.minimum(z, 30.0))) * LOG2E)
    if keep is not None:
        soft = jnp.where(keep, soft, 0.0)
    later = dot(soft.astype(BF16), tri)
    return z, soft, later


def stick_kernel(
    bias_ref, query_ref, queries_ref, early_ref, late_ref,
    own_ref, own_left_ref, far_ref, far_left_ref,
    q_ref, tri_ref, acc_ref, left_ref,
):
    sp, c, zl, y = place()
    here = zl * 4 + y
    bias2 = bias_ref[0] * LOG2E
    rows = lax.broadcasted_iota(jnp.int32, (TOK, TOK), 0)
    cols = lax.broadcasted_iota(jnp.int32, (TOK, TOK), 1)
    tri_ref[...] = jnp.where(rows > cols, -1.0, 0.0).astype(BF16)
    acc_ref[...] = jnp.zeros_like(acc_ref)
    left_ref[...] = jnp.zeros_like(left_ref)
    lane = lax.broadcasted_iota(jnp.int32, (128, 128), 1)
    for n in range(4):
        packed = (query_ref[...] if n == 0 else queries_ref[n - 1]).astype(F32)
        for half in range(2):
            part = packed if half == 0 else pltpu.roll(packed, 64, 1)
            at = n * TOK + half * 128
            q_ref[at : at + 128, :] = jnp.where(lane < HEAD, part, 0.0).astype(BF16)

    def pair(i, _):
        tri = tri_ref[...]
        q_own, q_far = q_ref[0:TOK, :], q_ref[TOK:, :]
        kvs, own, far = [], [], []
        for u in range(2):
            m = 15 - 2 * i - u
            kv = jnp.concatenate([early_ref[m % 4, m // 4], late_ref[m // 4, m % 4]], axis=0)
            keep = cols - rows < (here - m) * TOK
            kvs.append(kv)
            own.append(stick_tile(q_own, kv, tri, bias2, keep) + (keep,))
            far.append(stick_tile(q_far, kv, tri, bias2))
        left_own, left_far = left_ref[0:TOK, 0:1], left_ref[TOK:, 0:1]
        acc_own, acc_far = acc_ref[0:TOK, :], acc_ref[TOK:, :]
        for u in range(2):
            z, soft, later, keep = own[u]
            weight = jnp.where(keep, jnp.exp2((z - soft) + (later + left_own)), 0.0)
            acc_own = acc_own + dot(weight.astype(BF16), kvs[u])
            left_own = left_own + (later[:, 0:1] - soft[:, 0:1])
            z, soft, later = far[u]
            weight = jnp.exp2((z - soft) + (later + left_far))
            acc_far = acc_far + dot(weight.astype(BF16), kvs[u])
            left_far = left_far + (later[:, 0:1] - soft[:, 0:1])
        acc_ref[0:TOK, :] = acc_own
        acc_ref[TOK:, :] = acc_far
        left_ref[0:TOK, :] = jnp.broadcast_to(left_own, (TOK, 128))
        left_ref[TOK:, :] = jnp.broadcast_to(left_far, (3 * TOK, 128))
        return 0

    lax.fori_loop(0, 8, pair, 0)
    own_ref[...] = acc_ref[0:TOK, :]
    own_left_ref[...] = left_ref[0:TOK, :]
    for n in range(3):
        at = (n + 1) * TOK
        top = acc_ref[at : at + 128, :]
        low = pltpu.roll(acc_ref[at + 128 : at + 256, :], 64, 1)
        far_ref[n] = jnp.where(lane < HEAD, low, top).astype(BF16)
        for half in range(2):
            turned = jnp.transpose(left_ref[at + half * 128 : at + half * 128 + 128, :])
            far_left_ref[n, :, half * 128 : half * 128 + 128] = turned[0:8, :]


def stick(bias, query, queries, early, late):
    return pl.pallas_call(
        stick_kernel,
        out_shape=(
            jax.ShapeDtypeStruct((TOK, 128), F32),
            jax.ShapeDtypeStruct((TOK, 128), F32),
            jax.ShapeDtypeStruct((3, 128, 128), BF16),
            jax.ShapeDtypeStruct((3, 8, TOK), F32),
        ),
        in_specs=[SMEM, VMEM, VMEM, VMEM, VMEM],
        out_specs=(VMEM,) * 4,
        scratch_shapes=[
            pltpu.VMEM((4 * TOK, 128), BF16),
            pltpu.VMEM((TOK, TOK), BF16),
            pltpu.VMEM((4 * TOK, 128), F32),
            pltpu.VMEM((4 * TOK, 128), F32),
        ],
        name="stick",
    )(bias, query, queries, early, late)


def finish_kernel(
    own_ref, own_left_ref, far_ref, far_left_ref, before_ref, group_ref,
    local_ref, faded_ref, gate_ref, gain_ref,
    heads_ref,
    part_ref, part_left_ref, states_ref, acc_ref, left_ref, in_ref, send, recv,
):
    sp, c, zl, y = place()
    greet([(sp + 16 * d) % 64 for d in (1, 2, 3)])

    def copies(n, there, to_sp):
        pairs = (
            (far_ref.at[there - 1], part_ref.at[c]),
            (far_left_ref.at[there - 1], part_left_ref.at[c]),
            (group_ref, states_ref.at[c]),
        )
        return [
            to(src, dst, send.at[k, n], recv.at[k, c], to_sp) for k, (src, dst) in enumerate(pairs)
        ]

    def arrivals(source):
        pairs = ((far_ref.at[0], part_ref), (far_left_ref.at[0], part_left_ref), (group_ref, states_ref))
        return [
            to(src, dst.at[source], send.at[k, 0], recv.at[k, source], sp)
            for k, (src, dst) in enumerate(pairs)
        ]

    for d in (1, 2, 3):

        @pl.when(c + d < 4)
        def _():
            for copy in copies(d - 1, c + d, sp + 16 * d):
                copy.start()

    acc_ref[...] = own_ref[...]
    left_ref[...] = own_left_ref[...]
    in_ref[...] = jnp.zeros_like(in_ref)
    for g in (2, 1, 0):

        @pl.when(g < c)
        def _():
            for copy in arrivals(g)[0:2]:
                copy.wait_recv()
            packed = part_ref[g].astype(F32)
            scale = jnp.exp2(left_ref[...])
            acc_ref[0:128, :] += packed * scale[0:128, :]
            acc_ref[128:256, :] += pltpu.roll(packed, 64, 1) * scale[128:256, :]
            for half in range(2):
                at = slice(half * 128, half * 128 + 128)
                flat = jnp.broadcast_to(part_left_ref[g, 0:1, at], (128, 128))
                left_ref[at, :] += jnp.transpose(flat)

    for g in (0, 1, 2):

        @pl.when(g < c)
        def _():
            arrivals(g)[2].wait_recv()
            in_ref[...] = in_ref[...] * jnp.exp(states_ref[g, REC_VAL : REC_VAL + 1, :]) + states_ref[
                g, 0:REC_VAL, :
            ]

    state = in_ref[...] * jnp.exp(before_ref[REC_VAL : REC_VAL + 1, :]) + before_ref[0:REC_VAL, :]
    raw = local_ref[...] + dot(faded_ref[...], state.astype(BF16), tb=True)
    normed = raw * lax.rsqrt(jnp.mean(raw * raw, axis=1, keepdims=True) + epsilon) * gain_ref[...]
    gate = gate_ref[...].astype(F32)
    state_heads = normed * (gate * jax.nn.sigmoid(gate))
    heads_ref[:, 0:REC_VAL] = state_heads.astype(BF16)
    heads_ref[:, REC_VAL:] = acc_ref[:, HEAD:].astype(BF16)
    for d in (1, 2, 3):

        @pl.when(c + d < 4)
        def _():
            for copy in copies(d - 1, c + d, sp + 16 * d):
                copy.wait_send()


def finish(*operands):
    dma = pltpu.SemaphoreType.DMA
    return pl.pallas_call(
        finish_kernel,
        out_shape=jax.ShapeDtypeStruct((TOK, 128), BF16),
        in_specs=[VMEM] * 10,
        out_specs=VMEM,
        scratch_shapes=[
            pltpu.VMEM((3, 128, 128), BF16),
            pltpu.VMEM((3, 8, TOK), F32),
            pltpu.VMEM((3, STATE_ROWS, REC_KEY), F32),
            pltpu.VMEM((TOK, 128), F32),
            pltpu.VMEM((TOK, 128), F32),
            pltpu.VMEM((REC_VAL, REC_KEY), F32),
            dma((3, 3)), dma((3, 3)),
        ],
        compiler_params=pltpu.CompilerParams(collective_id=1, has_side_effects=True),
        name="finish",
    )(*operands)


def shards(
    tokens,
    input_norm_gain,
    attention_query_weight,
    attention_key_weight,
    attention_value_weight,
    attention_score_bias,
    recurrence_query_weight,
    forget_weight,
    input_weight,
    output_gate_weight,
    forget_minimum,
    decay_spikes,
    head_norm_gain,
    attention_output_weight,
    recurrence_output_weight,
):
    kv, query, rec, forget, inputs, gate = project(
        tokens,
        input_norm_gain.reshape(8, 256),
        attention_query_weight,
        attention_key_weight,
        attention_value_weight,
        recurrence_query_weight,
        forget_weight,
        input_weight,
        output_gate_weight,
    )
    early, late, queries, before, group, local_out, faded, columns = share(
        kv, query, rec, forget, inputs, forget_minimum, decay_spikes,
        recurrence_output_weight, attention_output_weight,
    )
    own, own_left, far, far_left = stick(attention_score_bias, query, queries, early, late)
    heads = finish(
        own, own_left, far, far_left, before, group, local_out, faded, gate, head_norm_gain[None, :]
    )
    return output(heads, columns)


def solution(mesh):
    placed = (
        P("sp", "tp"),
        P(),
        P(None, "tp"),
        P(None, "tp"),
        P(None, "tp"),
        P("tp"),
        P(None, "tp"),
        P(None, "tp"),
        P(None, "tp"),
        P(None, "tp"),
        P("tp", None),
        P("sp", "tp"),
        P(),
        P("tp", None),
        P("tp", None),
    )
    return jax.shard_map(
        shards, mesh=mesh, in_specs=placed, out_specs=P("sp", "tp"), check_vma=False
    )
```

```python
import functools

import jax
import jax.numpy as jnp
from jax import lax
from jax.experimental import pallas as pl
from jax.experimental.pallas import tpu as pltpu
from jax.sharding import PartitionSpec as P

D = 2048
HEAD = 64
REC_KEY = 128
REC_VAL = 64
REC_SPAN = 64
TOK = 256
LOG2E = 1.4426950408889634
STATE_ROWS = REC_VAL + 8
epsilon = 1e-06
F32, BF16 = jnp.float32, jnp.bfloat16
VMEM = pl.BlockSpec(memory_space=pltpu.VMEM)
SMEM = pl.BlockSpec(memory_space=pltpu.SMEM)
ANY = pl.BlockSpec(memory_space=pl.ANY)
MESH = pl.DeviceIdType.MESH


def dot(a, b, ta=False, tb=False):
    dims = (((0 if ta else 1,), (1 if tb else 0,)), ((), ()))
    return lax.dot_general(a, b, dims, preferred_element_type=F32)


def to(src, dst, send, recv, sp):
    return pltpu.make_async_remote_copy(
        src_ref=src, dst_ref=dst, send_sem=send, recv_sem=recv,
        device_id={"sp": sp}, device_id_type=MESH,
    )


def place():
    sp = lax.axis_index("sp")
    return sp, sp // 16, (sp // 4) % 4, sp % 4


def greet(peers, lane_peers=(), meanwhile=lambda: None):
    barrier = pltpu.get_barrier_semaphore()
    for peer in peers:
        pl.semaphore_signal(barrier, inc=1, device_id={"sp": peer}, device_id_type=MESH)
    for peer in lane_peers:
        pl.semaphore_signal(barrier, inc=1, device_id={"tp": peer}, device_id_type=MESH)
    meanwhile()
    pl.semaphore_wait(barrier, len(peers) + len(lane_peers))


def lanes():
    tp = lax.axis_index("tp")
    x, core = tp // 2, tp % 2
    return tp, tp + 1 - 2 * core, (tp + 2) % 8, (tp + 6) % 8, (tp + 4) % 8, 1 - 2 * core


def ring_gather(chunk_ref, slots_ref, send, recv, meanwhile, use):
    tp, partner, right, left, across, twist = lanes()
    half = chunk_ref.shape[0] // 2
    top, low = slice(0, half), slice(half, 2 * half)

    def copy(n, src, dst, target):
        return pltpu.make_async_remote_copy(
            src_ref=src, dst_ref=dst, send_sem=send.at[n], recv_sem=recv.at[n],
            device_id={"tp": target}, device_id_type=MESH,
        )

    def relay(n, source, part, target):
        return copy(n, slots_ref.at[source, part], slots_ref.at[source, part], target)

    barrier = pltpu.get_barrier_semaphore()
    for peer in (partner, right, left):
        pl.semaphore_signal(barrier, inc=1, device_id={"tp": peer}, device_id_type=MESH)
    pl.semaphore_wait(barrier, 3)
    copies = [
        copy(0, chunk_ref, slots_ref.at[tp], partner),
        copy(1, chunk_ref.at[top], slots_ref.at[tp, top], right),
        copy(2, chunk_ref.at[low], slots_ref.at[tp, low], left),
        copy(3, chunk_ref.at[low], slots_ref.at[tp, low], right),
        copy(4, chunk_ref.at[top], slots_ref.at[tp, top], left),
        relay(5, left, top, right),
        relay(6, right, low, left),
        relay(7, left, top, partner),
        relay(8, right, low, partner),
        relay(9, left, low, partner),
        relay(10, right, top, partner),
        relay(11, across, top, partner),
        relay(12, across, low, partner),
    ]
    for n in range(5):
        copies[n].start()
    meanwhile()
    use(tp, chunk_ref)
    copies[1].wait_recv()
    copies[5].start()
    copies[7].start()
    copies[2].wait_recv()
    copies[6].start()
    copies[8].start()
    copies[0].wait_recv()
    use(partner, slots_ref.at[partner])
    copies[3].wait_recv()
    copies[9].start()
    copies[4].wait_recv()
    copies[10].start()
    use(left, slots_ref.at[left])
    use(right, slots_ref.at[right])
    copies[7].wait_recv()
    copies[9].wait_recv()
    use(left + twist, slots_ref.at[left + twist])
    copies[8].wait_recv()
    copies[10].wait_recv()
    use(right + twist, slots_ref.at[right + twist])
    copies[5].wait_recv()
    copies[11].start()
    copies[6].wait_recv()
    copies[12].start()
    use(across, slots_ref.at[across])
    copies[11].wait_recv()
    copies[12].wait_recv()
    use(across + twist, slots_ref.at[across + twist])
    for one in copies:
        one.wait_send()


def project_kernel(
    token_ref, gain_ref, key_w, value_w, input_w, gate_w, query_w, rec_w, forget_w,
    kv_ref, query_ref, rec_ref, forget_ref, input_ref, gate_ref,
    slots_ref, narrow_ref, wide_ref, first_ref, second_ref, square_ref, send, recv, load,
):
    narrow = (key_w, value_w, input_w, gate_w, query_w)
    loads = [
        pltpu.make_async_copy(w, narrow_ref.at[n * 64 : n * 64 + 64], load.at[n])
        for n, w in enumerate(narrow)
    ]
    loads += [
        pltpu.make_async_copy(w, wide_ref.at[:, n * 128 : n * 128 + 128], load.at[5 + n])
        for n, w in enumerate((rec_w, forget_w))
    ]
    for one in loads:
        one.start()
    first_ref[...] = jnp.zeros_like(first_ref)
    second_ref[...] = jnp.zeros_like(second_ref)
    square_ref[...] = jnp.zeros_like(square_ref)

    def meanwhile():
        for one in loads:
            one.wait()

    def use(source, ref):
        at = pl.ds(pl.multiple_of(source * 256, 256), 256)
        values = ref[...].astype(F32)
        squares = values * values
        square_ref[...] += squares[:, 0:128] + squares[:, 128:256]
        scaled = (values * gain_ref[:, at]).astype(BF16)
        first_ref[...] += dot(scaled, narrow_ref[:, at], tb=True)
        second_ref[...] += dot(scaled, wide_ref[at, :])

    ring_gather(token_ref, slots_ref, send, recv, meanwhile, use)
    inverse = lax.rsqrt(jnp.sum(square_ref[...], axis=1, keepdims=True) / D + epsilon)
    kv_ref[...] = (first_ref[:, 0:128] * inverse).astype(BF16)
    input_ref[...] = (first_ref[:, 128:192] * inverse).astype(BF16)
    gate_ref[...] = (first_ref[:, 192:256] * inverse).astype(BF16)
    query = (first_ref[:, 256:320] * inverse).astype(BF16)
    query_ref[...] = jnp.concatenate([query[0:128], query[128:256]], axis=1)
    rec_ref[...] = (second_ref[:, 0:128] * inverse).astype(BF16)
    forget_ref[...] = (second_ref[:, 128:256] * inverse).astype(BF16)


def project(tokens, gain, *weights):
    dma = pltpu.SemaphoreType.DMA
    wide, narrow = jax.ShapeDtypeStruct((TOK, 128), BF16), jax.ShapeDtypeStruct((TOK, 64), BF16)
    return pl.pallas_call(
        project_kernel,
        out_shape=(wide, jax.ShapeDtypeStruct((128, 128), BF16), wide, wide, narrow, narrow),
        in_specs=[VMEM, VMEM] + [ANY] * 7,
        out_specs=(VMEM,) * 6,
        scratch_shapes=[
            pltpu.VMEM((8, TOK, 256), BF16),
            pltpu.VMEM((320, D), BF16),
            pltpu.VMEM((D, 256), BF16),
            pltpu.VMEM((TOK, 320), F32),
            pltpu.VMEM((TOK, 256), F32),
            pltpu.VMEM((TOK, 128), F32),
            dma((13,)), dma((13,)), dma((7,)),
        ],
        compiler_params=pltpu.CompilerParams(collective_id=2, has_side_effects=True),
        name="project",
    )(tokens, gain, *weights)


def output_kernel(heads_ref, weight_ref, out_ref, slots_ref, acc_ref, send, recv):
    acc_ref[...] = jnp.zeros_like(acc_ref)

    def use(source, ref):
        acc_ref[...] += dot(ref[...], weight_ref[source])

    ring_gather(heads_ref, slots_ref, send, recv, lambda: None, use)
    out_ref[...] = acc_ref[...].astype(BF16)


def output(heads, weight):
    dma = pltpu.SemaphoreType.DMA
    return pl.pallas_call(
        output_kernel,
        out_shape=jax.ShapeDtypeStruct((TOK, 256), BF16),
        in_specs=[VMEM, VMEM],
        out_specs=VMEM,
        scratch_shapes=[
            pltpu.VMEM((8, TOK, 128), BF16),
            pltpu.VMEM((TOK, 256), F32),
            dma((13,)), dma((13,)),
        ],
        compiler_params=pltpu.CompilerParams(collective_id=3, has_side_effects=True),
        name="output",
    )(heads, weight)


def column(row):
    return jnp.transpose(jnp.broadcast_to(row, (128, 128)))


def local_scan(query_ref, forget_ref, input_ref, low_ref, spike_ref, out_ref, lift_ref, state_ref):
    span = REC_SPAN
    rows = lax.broadcasted_iota(jnp.int32, (span, span), 0)
    cols = lax.broadcasted_iota(jnp.int32, (span, span), 1)
    causal = cols <= rows
    ones = jnp.where(causal, 1.0, 0.0)
    spikes = jnp.concatenate([column(spike_ref[:, n : n + 128]) for n in (0, 128)], axis=0)
    state = jnp.zeros((REC_VAL, REC_KEY), F32)
    offset = jnp.zeros((1, REC_KEY), F32)
    for n in range(query_ref.shape[0] // span):
        at = slice(n * span, (n + 1) * span)
        query = query_ref[at, :].astype(F32)
        lifted = query * jax.nn.sigmoid(query)
        intake = (1.0 - low_ref[...]) * jax.nn.sigmoid(-forget_ref[at, :].astype(F32))
        log_forget = jnp.log1p(-intake) + spikes[at, :]
        running = lax.dot_general(
            ones, log_forget, (((1,), (0,)), ((), ())),
            precision=lax.Precision.HIGHEST, preferred_element_type=F32,
        )
        total = running[span - 1 : span, :]
        middle = running[span // 2 - 1 : span // 2, :]
        value = input_ref[at, :]
        grown = (lifted * jnp.exp(running - middle)).astype(BF16)
        shrunk = (intake * jnp.exp(middle - running)).astype(BF16)
        inner = jnp.where(causal, dot(grown, shrunk, tb=True), 0.0)
        faded = (lifted * jnp.exp(running)).astype(BF16)
        out_ref[at, :] = dot(inner.astype(BF16), value) + dot(faded, state.astype(BF16), tb=True)
        lift_ref[at, :] = (lifted * jnp.exp(running + offset)).astype(BF16)
        kept = (intake * jnp.exp(total - running)).astype(BF16)
        state = state * jnp.exp(total) + dot(value, kept, ta=True)
        offset = offset + total
    state_ref[0:REC_VAL, :] = state
    state_ref[REC_VAL:STATE_ROWS, :] = jnp.broadcast_to(offset, (8, REC_KEY))


def stick_tile(q, kv, tri, bias2, keep=None):
    z = dot(q, kv, tb=True) * (LOG2E / 8.0) + bias2
    soft = jnp.maximum(z, jnp.log(1.0 + jnp.exp2(jnp.minimum(z, 30.0))) * LOG2E)
    if keep is not None:
        soft = jnp.where(keep, soft, 0.0)
    later = dot(soft.astype(BF16), tri)
    return z, soft, later


def attend(here, bias2, q_ref, kvs_ref, tri_ref, acc_ref, left_ref):
    rows = lax.broadcasted_iota(jnp.int32, (TOK, TOK), 0)
    cols = lax.broadcasted_iota(jnp.int32, (TOK, TOK), 1)
    tri_ref[...] = jnp.where(rows > cols, -1.0, 0.0).astype(BF16)
    acc_ref[...] = jnp.zeros_like(acc_ref)
    left_ref[...] = jnp.zeros_like(left_ref)

    def pair(i, _):
        tri = tri_ref[...]
        q_own, q_far = q_ref[0:TOK, :], q_ref[TOK:, :]
        kvs, own, far = [], [], []
        for u in range(2):
            m = 15 - 2 * i - u
            kv = kvs_ref[m // 4, m % 4]
            keep = cols - rows < (here - m) * TOK
            kvs.append(kv)
            own.append(stick_tile(q_own, kv, tri, bias2, keep) + (keep,))
            far.append(stick_tile(q_far, kv, tri, bias2))
        left_own, left_far = left_ref[0:TOK, 0:1], left_ref[TOK:, 0:1]
        acc_own, acc_far = acc_ref[0:TOK, :], acc_ref[TOK:, :]
        for u in range(2):
            z, soft, later, keep = own[u]
            weight = jnp.where(keep, jnp.exp2((z - soft) + (later + left_own)), 0.0)
            acc_own = acc_own + dot(weight.astype(BF16), kvs[u])
            left_own = left_own + (later[:, 0:1] - soft[:, 0:1])
            z, soft, later = far[u]
            weight = jnp.exp2((z - soft) + (later + left_far))
            acc_far = acc_far + dot(weight.astype(BF16), kvs[u])
            left_far = left_far + (later[:, 0:1] - soft[:, 0:1])
        acc_ref[0:TOK, :] = acc_own
        acc_ref[TOK:, :] = acc_far
        left_ref[0:TOK, :] = jnp.broadcast_to(left_own, (TOK, 128))
        left_ref[TOK:, :] = jnp.broadcast_to(left_far, (3 * TOK, 128))
        return 0

    lax.fori_loop(0, 8, pair, 0)


def chain(states_ref, here):
    state = states_ref[0, 0:REC_VAL, :]
    total = states_ref[0, REC_VAL : REC_VAL + 1, :]
    ahead, ahead_total = jnp.zeros_like(state), jnp.zeros_like(total)
    for n in range(1, 4):
        ahead = jnp.where(n <= here, state, ahead)
        ahead_total = jnp.where(n <= here, total, ahead_total)
        more = states_ref[n, REC_VAL : REC_VAL + 1, :]
        state = state * jnp.exp(more) + states_ref[n, 0:REC_VAL, :]
        total = total + more
    return state, total, ahead, ahead_total


def mix_kernel(
    bias_ref, kv_ref, query_ref, rec_ref, forget_ref, input_ref, gate_ref, low_ref, spike_ref, gain_ref,
    rec_out_w, att_out_w,
    heads_ref, columns_ref,
    kvs_ref, queries_ref, state_ref, rows_ref, planes_ref, group_ref, groups_ref,
    local_ref, faded_ref, q_ref, tri_ref, acc_ref, left_ref,
    far_ref, far_left_ref, part_ref, part_left_ref, in_ref,
    line_send, line_recv, row_send, row_recv, half_send, half_recv, state_send, state_recv,
    query_send, query_recv, column_send, column_recv, back_send, back_recv, own_sem,
):
    sp, c, zl, y = place()
    tp = lax.axis_index("tp")
    base = c * 16
    row = [base + zl * 4 + (y + d) % 4 for d in range(4)]
    line = [base + ((zl + d) % 4) * 4 + y for d in range(4)]
    far = [(sp + 16 * d) % 64 for d in range(4)]
    lane_peers = [(tp + d) % 8 for d in range(1, 8)]

    def columns(w, there):
        return w.at[:, pl.ds(pl.multiple_of(there * 256, 256), 256)]

    out_w = ((0, rec_out_w), (1, att_out_w))
    own_columns = [
        pltpu.make_async_copy(columns(w, tp), columns_ref.at[tp, n * 64 : n * 64 + 64], own_sem.at[n])
        for n, w in out_w
    ]
    column_copies = [
        pltpu.make_async_remote_copy(
            src_ref=columns(w, there), dst_ref=columns_ref.at[tp, n * 64 : n * 64 + 64],
            send_sem=column_send.at[n, d], recv_sem=column_recv.at[n, d],
            device_id={"tp": there}, device_id_type=MESH,
        )
        for n, w in out_w
        for d, there in enumerate(lane_peers)
    ]
    for copy in own_columns:
        copy.start()

    def scan():
        local_scan(
            rec_ref, forget_ref, input_ref, low_ref, spike_ref, local_ref, faded_ref, state_ref
        )
        rows_ref[y] = state_ref[...]
        kvs_ref[zl, y] = kv_ref[...]
        for n in (1, 2, 3):

            @pl.when(c >= n)
            def _():
                queries_ref[n - 1] = jnp.zeros((128, 128), BF16)

    greet(row[1:] + line[1:] + far[1:], lane_peers, scan)

    def query_copy(d):
        slot = (c + 3) % 4
        return to(query_ref, queries_ref.at[slot], query_send.at[d - 1], query_recv.at[slot], far[4 - d])

    for d in (1, 2, 3):

        @pl.when(c >= d)
        def _():
            query_copy(d).start()

    along_line = [
        to(kv_ref, kvs_ref.at[zl, y], line_send.at[d - 1], line_recv.at[d - 1], line[d]) for d in (1, 2, 3)
    ]
    along_row = [
        [
            to(
                kv_ref if d == 0 else kvs_ref.at[(zl - d + 4) % 4, y],
                kvs_ref.at[(zl - d + 4) % 4, y], row_send.at[d, k], row_recv.at[d, k], row[1 if k == 0 else 3],
            )
            for k in range(2)
        ]
        for d in range(4)
    ]

    def onward(d, k):
        block = kvs_ref.at[(zl - d + 4) % 4, (y + 3) % 4 if k == 0 else (y + 1) % 4, k * 128 : k * 128 + 128]
        return to(block, block, half_send.at[d, k], half_recv.at[d, k], row[1 if k == 0 else 3])

    halves = [[onward(d, k) for k in range(2)] for d in range(4)]
    for copy in along_row[0] + along_line:
        copy.start()
    row_states = [
        to(state_ref, rows_ref.at[y], state_send.at[0, d - 1], state_recv.at[0, d - 1], row[d])
        for d in (1, 2, 3)
    ]
    for copy in row_states + column_copies:
        copy.start()
    for d in range(4):
        if d < 3:
            along_line[d].wait_recv()
            for copy in along_row[d + 1]:
                copy.start()
        for k in range(2):
            along_row[d][k].wait_recv()
            halves[d][k].start()
        if d == 0:
            for copy in row_states:
                copy.wait_recv()
            state, total, ahead, ahead_total = chain(rows_ref, y)
            planes_ref[zl, 0:REC_VAL, :] = state
            planes_ref[zl, REC_VAL:STATE_ROWS, :] = jnp.broadcast_to(total, (8, REC_KEY))
            line_states = [
                to(planes_ref.at[zl], planes_ref.at[zl], state_send.at[1, n - 1], state_recv.at[1, n - 1], line[n])
                for n in (1, 2, 3)
            ]
            for copy in line_states:
                copy.start()
    for copy in line_states:
        copy.wait_recv()
    state, total, low, low_total = chain(planes_ref, zl)
    group_ref[0:REC_VAL, :] = state
    group_ref[REC_VAL:STATE_ROWS, :] = jnp.broadcast_to(total, (8, REC_KEY))
    before = low * jnp.exp(ahead_total) + ahead
    before_total = low_total + ahead_total

    def back(k, d):
        slot = (c + d + 3) % 4
        src, dst = ((group_ref, groups_ref), (far_ref, part_ref), (far_left_ref, part_left_ref))[k]
        src = src if k == 0 else src.at[slot % 3]
        return to(src, dst.at[c % 3], back_send.at[k, d - 1], back_recv.at[k, c % 3], far[d])

    def arrival(k, g):
        src, dst = ((group_ref, groups_ref), (far_ref.at[0], part_ref), (far_left_ref.at[0], part_left_ref))[k]
        return to(src, dst.at[g], back_send.at[k, 0], back_recv.at[k, g], far[1])

    for d in (1, 2, 3):

        @pl.when(c + d < 4)
        def _():
            back(0, d).start()

    for pair in halves:
        for copy in pair:
            copy.wait_recv()
    for n in (1, 2, 3):

        @pl.when(c < n)
        def _():
            to(
                query_ref, queries_ref.at[n - 1], query_send.at[0], query_recv.at[n - 1], far[1]
            ).wait_recv()

    lane = lax.broadcasted_iota(jnp.int32, (128, 128), 1)
    for n in range(4):
        packed = (query_ref[...] if n == 0 else queries_ref[n - 1]).astype(F32)
        for half in range(2):
            part = packed if half == 0 else pltpu.roll(packed, 64, 1)
            at = n * TOK + half * 128
            q_ref[at : at + 128, :] = jnp.where(lane < HEAD, part, 0.0).astype(BF16)

    attend(zl * 4 + y, bias_ref[0] * LOG2E, q_ref, kvs_ref, tri_ref, acc_ref, left_ref)

    for n in range(3):
        at = (n + 1) * TOK
        top = acc_ref[at : at + 128, :]
        bottom = pltpu.roll(acc_ref[at + 128 : at + 256, :], 64, 1)
        far_ref[n] = jnp.where(lane < HEAD, bottom, top).astype(BF16)
        for half in range(2):
            turned = jnp.transpose(left_ref[at + half * 128 : at + half * 128 + 128, :])
            far_left_ref[n, :, half * 128 : half * 128 + 128] = turned[0:8, :]
    for d in (1, 2, 3):

        @pl.when(c + d < 4)
        def _():
            back(1, d).start()
            back(2, d).start()

    in_ref[...] = jnp.zeros_like(in_ref)
    for g in (0, 1, 2):

        @pl.when(g < c)
        def _():
            arrival(0, g).wait_recv()
            in_ref[...] = in_ref[...] * jnp.exp(groups_ref[g, REC_VAL : REC_VAL + 1, :]) + groups_ref[
                g, 0:REC_VAL, :
            ]

    entering = in_ref[...] * jnp.exp(before_total) + before
    raw = local_ref[...] + dot(faded_ref[...], entering.astype(BF16), tb=True)
    normed = raw * lax.rsqrt(jnp.mean(raw * raw, axis=1, keepdims=True) + epsilon) * gain_ref[...]
    gate = gate_ref[...].astype(F32)
    heads_ref[:, 0:REC_VAL] = (normed * (gate * jax.nn.sigmoid(gate))).astype(BF16)

    for g in (2, 1, 0):

        @pl.when(g < c)
        def _():
            arrival(1, g).wait_recv()
            arrival(2, g).wait_recv()
            packed = part_ref[g].astype(F32)
            scale = jnp.exp2(left_ref[0:TOK, :])
            acc_ref[0:128, :] += packed * scale[0:128, :]
            acc_ref[128:256, :] += pltpu.roll(packed, 64, 1) * scale[128:256, :]
            for at in (0, 128):
                left_ref[at : at + 128, :] += column(part_left_ref[g, 0:1, at : at + 128])

    heads_ref[:, REC_VAL:] = acc_ref[0:TOK, HEAD:].astype(BF16)

    for copy in own_columns:
        copy.wait()
    for copy in column_copies:
        copy.wait_recv()
    sent = along_line + row_states + line_states + column_copies
    for d in range(4):
        sent = sent + along_row[d] + halves[d]
    for copy in sent:
        copy.wait_send()
    for d in (1, 2, 3):

        @pl.when(c >= d)
        def _():
            query_copy(d).wait_send()

        @pl.when(c + d < 4)
        def _():
            for k in range(3):
                back(k, d).wait_send()


def mix(*operands):
    dma = pltpu.SemaphoreType.DMA
    return pl.pallas_call(
        mix_kernel,
        out_shape=(
            jax.ShapeDtypeStruct((TOK, 128), BF16),
            jax.ShapeDtypeStruct((8, 128, 256), BF16),
        ),
        in_specs=[SMEM] + [VMEM] * 9 + [ANY] * 2,
        out_specs=(VMEM,) * 2,
        scratch_shapes=[
            pltpu.VMEM((4, 4, TOK, 128), BF16),
            pltpu.VMEM((3, 128, 128), BF16),
            pltpu.VMEM((STATE_ROWS, REC_KEY), F32),
            pltpu.VMEM((4, STATE_ROWS, REC_KEY), F32),
            pltpu.VMEM((4, STATE_ROWS, REC_KEY), F32),
            pltpu.VMEM((STATE_ROWS, REC_KEY), F32),
            pltpu.VMEM((3, STATE_ROWS, REC_KEY), F32),
            pltpu.VMEM((TOK, REC_VAL), F32),
            pltpu.VMEM((TOK, REC_KEY), BF16),
            pltpu.VMEM((4 * TOK, 128), BF16),
            pltpu.VMEM((TOK, TOK), BF16),
            pltpu.VMEM((4 * TOK, 128), F32),
            pltpu.VMEM((4 * TOK, 128), F32),
            pltpu.VMEM((3, 128, 128), BF16),
            pltpu.VMEM((3, 8, TOK), F32),
            pltpu.VMEM((3, 128, 128), BF16),
            pltpu.VMEM((3, 8, TOK), F32),
            pltpu.VMEM((REC_VAL, REC_KEY), F32),
            dma((3,)), dma((3,)), dma((4, 2)), dma((4, 2)), dma((4, 2)), dma((4, 2)), dma((2, 3)), dma((2, 3)),
            dma((3,)), dma((3,)), dma((2, 7)), dma((2, 7)), dma((3, 3)), dma((3, 3)), dma((2,)),
        ],
        compiler_params=pltpu.CompilerParams(collective_id=0, has_side_effects=True),
        name="mix",
    )(*operands)


def shards(
    tokens,
    input_norm_gain,
    attention_query_weight,
    attention_key_weight,
    attention_value_weight,
    attention_score_bias,
    recurrence_query_weight,
    forget_weight,
    input_weight,
    output_gate_weight,
    forget_minimum,
    decay_spikes,
    head_norm_gain,
    attention_output_weight,
    recurrence_output_weight,
):
    narrow = (
        attention_key_weight, attention_value_weight, input_weight, output_gate_weight, attention_query_weight
    )
    kv, query, rec, forget, inputs, gate = project(
        tokens, input_norm_gain[None, :], *(w.T for w in narrow), recurrence_query_weight, forget_weight
    )
    heads, columns = mix(
        attention_score_bias, kv, query, rec, forget, inputs, gate,
        forget_minimum, decay_spikes.reshape(1, TOK), head_norm_gain[None, :],
        recurrence_output_weight, attention_output_weight,
    )
    return output(heads, columns)


def solution(mesh):
    placed = (
        P("sp", "tp"),
        P(),
        P(None, "tp"),
        P(None, "tp"),
        P(None, "tp"),
        P("tp"),
        P(None, "tp"),
        P(None, "tp"),
        P(None, "tp"),
        P(None, "tp"),
        P("tp", None),
        P("sp", "tp"),
        P(),
        P("tp", None),
        P("tp", None),
    )
    return jax.shard_map(
        shards, mesh=mesh, in_specs=placed, out_specs=P("sp", "tp"), check_vma=False
    )
```

```python
import functools

import jax
import jax.numpy as jnp
from jax import lax
from jax.experimental import pallas as pl
from jax.experimental.pallas import tpu as pltpu
from jax.sharding import PartitionSpec as P

D = 2048
HEAD = 64
REC_KEY = 128
REC_VAL = 64
REC_SPAN = 64
TOK = 256
LOG2E = 1.4426950408889634
STATE_ROWS = REC_VAL + 8
epsilon = 1e-06
F32, BF16 = jnp.float32, jnp.bfloat16
VMEM = pl.BlockSpec(memory_space=pltpu.VMEM)
SMEM = pl.BlockSpec(memory_space=pltpu.SMEM)
ANY = pl.BlockSpec(memory_space=pl.ANY)
MESH = pl.DeviceIdType.MESH


def dot(a, b, ta=False, tb=False):
    dims = (((0 if ta else 1,), (1 if tb else 0,)), ((), ()))
    return lax.dot_general(a, b, dims, preferred_element_type=F32)


def to(src, dst, send, recv, sp):
    return pltpu.make_async_remote_copy(
        src_ref=src, dst_ref=dst, send_sem=send, recv_sem=recv,
        device_id={"sp": sp}, device_id_type=MESH,
    )


def place():
    sp = lax.axis_index("sp")
    return sp, sp // 16, (sp // 4) % 4, sp % 4


def lanes():
    tp = lax.axis_index("tp")
    x, core = tp // 2, tp % 2
    return tp, tp + 1 - 2 * core, (tp + 2) % 8, (tp + 6) % 8, (tp + 4) % 8, 1 - 2 * core


def ring_gather(chunk_ref, slots_ref, send, recv, meanwhile, use):
    tp, partner, right, left, across, twist = lanes()
    half = chunk_ref.shape[0] // 2
    top, low = slice(0, half), slice(half, 2 * half)

    def copy(n, src, dst, target):
        return pltpu.make_async_remote_copy(
            src_ref=src, dst_ref=dst, send_sem=send.at[n], recv_sem=recv.at[n],
            device_id={"tp": target}, device_id_type=MESH,
        )

    def relay(n, source, part, target):
        return copy(n, slots_ref.at[source, part], slots_ref.at[source, part], target)

    copies = [
        copy(0, chunk_ref, slots_ref.at[tp], partner),
        copy(1, chunk_ref.at[top], slots_ref.at[tp, top], right),
        copy(2, chunk_ref.at[low], slots_ref.at[tp, low], left),
        copy(3, chunk_ref.at[low], slots_ref.at[tp, low], right),
        copy(4, chunk_ref.at[top], slots_ref.at[tp, top], left),
        relay(5, left, top, right),
        relay(6, right, low, left),
        relay(7, left, top, partner),
        relay(8, right, low, partner),
        relay(9, left, low, partner),
        relay(10, right, top, partner),
        relay(11, across, top, partner),
        relay(12, across, low, partner),
    ]
    for n in range(5):
        copies[n].start()
    meanwhile()
    use(tp, chunk_ref)
    copies[1].wait_recv()
    copies[5].start()
    copies[7].start()
    copies[2].wait_recv()
    copies[6].start()
    copies[8].start()
    copies[0].wait_recv()
    use(partner, slots_ref.at[partner])
    copies[3].wait_recv()
    copies[9].start()
    copies[4].wait_recv()
    copies[10].start()
    use(left, slots_ref.at[left])
    use(right, slots_ref.at[right])
    copies[7].wait_recv()
    copies[9].wait_recv()
    use(left + twist, slots_ref.at[left + twist])
    copies[8].wait_recv()
    copies[10].wait_recv()
    use(right + twist, slots_ref.at[right + twist])
    copies[5].wait_recv()
    copies[11].start()
    copies[6].wait_recv()
    copies[12].start()
    use(across, slots_ref.at[across])
    copies[11].wait_recv()
    copies[12].wait_recv()
    use(across + twist, slots_ref.at[across + twist])
    for one in copies:
        one.wait_send()


def column(row):
    return jnp.transpose(jnp.broadcast_to(row, (128, 128)))


def local_scan(query_ref, forget_ref, input_ref, low_ref, spike_ref, out_ref, lift_ref, state_ref):
    span = REC_SPAN
    rows = lax.broadcasted_iota(jnp.int32, (span, span), 0)
    cols = lax.broadcasted_iota(jnp.int32, (span, span), 1)
    causal = cols <= rows
    ones = jnp.where(causal, 1.0, 0.0)
    spikes = jnp.concatenate([column(spike_ref[:, n : n + 128]) for n in (0, 128)], axis=0)
    state = jnp.zeros((REC_VAL, REC_KEY), F32)
    offset = jnp.zeros((1, REC_KEY), F32)
    for n in range(query_ref.shape[0] // span):
        at = slice(n * span, (n + 1) * span)
        query = query_ref[at, :].astype(F32)
        lifted = query * jax.nn.sigmoid(query)
        intake = (1.0 - low_ref[...]) * jax.nn.sigmoid(-forget_ref[at, :].astype(F32))
        log_forget = jnp.log1p(-intake) + spikes[at, :]
        running = lax.dot_general(
            ones, log_forget, (((1,), (0,)), ((), ())),
            precision=lax.Precision.HIGHEST, preferred_element_type=F32,
        )
        total = running[span - 1 : span, :]
        middle = running[span // 2 - 1 : span // 2, :]
        value = input_ref[at, :]
        grown = (lifted * jnp.exp(running - middle)).astype(BF16)
        shrunk = (intake * jnp.exp(middle - running)).astype(BF16)
        inner = jnp.where(causal, dot(grown, shrunk, tb=True), 0.0)
        faded = (lifted * jnp.exp(running)).astype(BF16)
        out_ref[at, :] = dot(inner.astype(BF16), value) + dot(faded, state.astype(BF16), tb=True)
        lift_ref[at, :] = (lifted * jnp.exp(running + offset)).astype(BF16)
        kept = (intake * jnp.exp(total - running)).astype(BF16)
        state = state * jnp.exp(total) + dot(value, kept, ta=True)
        offset = offset + total
    state_ref[0:REC_VAL, :] = state
    state_ref[REC_VAL:STATE_ROWS, :] = jnp.broadcast_to(offset, (8, REC_KEY))


def stick_tile(q, kv, tri, bias2, keep=None):
    z = dot(q, kv, tb=True) * (LOG2E / 8.0) + bias2
    soft = jnp.maximum(z, jnp.log(1.0 + jnp.exp2(jnp.minimum(z, 30.0))) * LOG2E)
    if keep is not None:
        soft = jnp.where(keep, soft, 0.0)
    later = dot(soft.astype(BF16), tri)
    return z, soft, later


def attend(here, plane, bias2, q_ref, kvs_ref, tri_ref, acc_ref, left_ref):
    rows = lax.broadcasted_iota(jnp.int32, (TOK, TOK), 0)
    cols = lax.broadcasted_iota(jnp.int32, (TOK, TOK), 1)
    acc_ref[...] = jnp.zeros_like(acc_ref)
    left_ref[...] = jnp.zeros_like(left_ref)

    def pair(i, _):
        tri = tri_ref[...]
        q_own, q_far = q_ref[0:TOK, :], q_ref[TOK:, :]
        kvs, own, far = [], [], []
        for u in range(2):
            n = 3 - 2 * i - u
            kv = kvs_ref[plane, n]
            keep = cols - rows < (here - plane * 4 - n) * TOK
            kvs.append(kv)
            own.append(stick_tile(q_own, kv, tri, bias2, keep) + (keep,))
            far.append(stick_tile(q_far, kv, tri, bias2))
        left_own, left_far = left_ref[0:TOK, 0:1], left_ref[TOK:, 0:1]
        acc_own, acc_far = acc_ref[0:TOK, :], acc_ref[TOK:, :]
        for u in range(2):
            z, soft, later, keep = own[u]
            weight = jnp.where(keep, jnp.exp2((z - soft) + (later + left_own)), 0.0)
            acc_own = acc_own + dot(weight.astype(BF16), kvs[u])
            left_own = left_own + (later[:, 0:1] - soft[:, 0:1])
            z, soft, later = far[u]
            weight = jnp.exp2((z - soft) + (later + left_far))
            acc_far = acc_far + dot(weight.astype(BF16), kvs[u])
            left_far = left_far + (later[:, 0:1] - soft[:, 0:1])
        acc_ref[0:TOK, :] = acc_own
        acc_ref[TOK:, :] = acc_far
        left_ref[0:TOK, :] = jnp.broadcast_to(left_own, (TOK, 128))
        left_ref[TOK:, :] = jnp.broadcast_to(left_far, (3 * TOK, 128))
        return 0

    lax.fori_loop(0, 2, pair, 0)


def chain(states_ref, here):
    state = states_ref[0, 0:REC_VAL, :]
    total = states_ref[0, REC_VAL : REC_VAL + 1, :]
    ahead, ahead_total = jnp.zeros_like(state), jnp.zeros_like(total)
    for n in range(1, 4):
        ahead = jnp.where(n <= here, state, ahead)
        ahead_total = jnp.where(n <= here, total, ahead_total)
        more = states_ref[n, REC_VAL : REC_VAL + 1, :]
        state = state * jnp.exp(more) + states_ref[n, 0:REC_VAL, :]
        total = total + more
    return state, total, ahead, ahead_total


def layer_kernel(
    bias_ref, token_ref, feature_gain_ref, low_ref, spike_ref, gain_ref,
    key_w, value_w, input_w, gate_w, query_w, rec_w, forget_w, rec_out_w, att_out_w,
    out_ref,
    slots_ref, narrow_ref, wide_ref, first_ref, second_ref, square_ref,
    kv_ref, query_ref, rec_ref, forget_ref, input_ref, gate_ref,
    kvs_ref, queries_ref, state_ref, rows_ref, planes_ref, group_ref, groups_ref,
    local_ref, faded_ref, q_ref, tri_ref, acc_ref, left_ref,
    far_ref, far_left_ref, part_ref, part_left_ref, in_ref,
    heads_ref, columns_ref, head_slots_ref, sum_ref,
    load, token_send, token_recv, head_send, head_recv,
    line_send, line_recv, row_send, row_recv, half_send, half_recv, state_send, state_recv,
    query_send, query_recv, column_send, column_recv, back_send, back_recv, own_sem, near_sem,
):
    sp, c, zl, y = place()
    tp = lax.axis_index("tp")
    base = c * 16
    row = [base + zl * 4 + (y + d) % 4 for d in range(4)]
    line = [base + ((zl + d) % 4) * 4 + y for d in range(4)]
    far = [(sp + 16 * d) % 64 for d in range(4)]
    lane_peers = [(tp + d) % 8 for d in range(1, 8)]

    narrow = (key_w, value_w, input_w, gate_w, query_w)
    loads = [
        pltpu.make_async_copy(w, narrow_ref.at[n * 64 : n * 64 + 64], load.at[n])
        for n, w in enumerate(narrow)
    ]
    loads += [
        pltpu.make_async_copy(w, wide_ref.at[:, n * 128 : n * 128 + 128], load.at[5 + n])
        for n, w in enumerate((rec_w, forget_w))
    ]

    def columns(w, there):
        return w.at[:, pl.ds(pl.multiple_of(there * 256, 256), 256)]

    out_w = ((0, rec_out_w), (1, att_out_w))
    own_columns = [
        pltpu.make_async_copy(columns(w, tp), columns_ref.at[tp, n * 64 : n * 64 + 64], own_sem.at[n])
        for n, w in out_w
    ]
    column_copies = [
        pltpu.make_async_remote_copy(
            src_ref=columns(w, there), dst_ref=columns_ref.at[tp, n * 64 : n * 64 + 64],
            send_sem=column_send.at[n, d], recv_sem=column_recv.at[n, d],
            device_id={"tp": there}, device_id_type=MESH,
        )
        for n, w in out_w
        for d, there in enumerate(lane_peers)
    ]

    barrier = pltpu.get_barrier_semaphore()
    near = row[1:] + line[1:] + [far[1], far[3]]
    for peer in lane_peers:
        pl.semaphore_signal(barrier, inc=1, device_id={"tp": peer}, device_id_type=MESH)
    for peer in near:
        pl.semaphore_signal(barrier, inc=1, device_id={"sp": peer}, device_id_type=MESH)
    for copy in loads + own_columns:
        copy.start()
    first_ref[...] = jnp.zeros_like(first_ref)
    second_ref[...] = jnp.zeros_like(second_ref)
    square_ref[...] = jnp.zeros_like(square_ref)
    rows = lax.broadcasted_iota(jnp.int32, (TOK, TOK), 0)
    cols = lax.broadcasted_iota(jnp.int32, (TOK, TOK), 1)
    tri_ref[...] = jnp.where(rows > cols, -1.0, 0.0).astype(BF16)
    pl.semaphore_wait(barrier, len(lane_peers) + len(near))
    for peer in (far[1], far[3]):
        pl.semaphore_signal(near_sem, inc=1, device_id={"sp": peer}, device_id_type=MESH)

    def meanwhile():
        for one in loads:
            one.wait()

    def use(source, ref):
        at = pl.ds(pl.multiple_of(source * 256, 256), 256)
        values = ref[...].astype(F32)
        squares = values * values
        square_ref[...] += squares[:, 0:128] + squares[:, 128:256]
        scaled = (values * feature_gain_ref[:, at]).astype(BF16)
        first_ref[...] += dot(scaled, narrow_ref[:, at], tb=True)
        second_ref[...] += dot(scaled, wide_ref[at, :])

    ring_gather(token_ref, slots_ref, token_send, token_recv, meanwhile, use)
    inverse = lax.rsqrt(jnp.sum(square_ref[...], axis=1, keepdims=True) / D + epsilon)
    query = (first_ref[:, 256:320] * inverse).astype(BF16)
    query_ref[...] = jnp.concatenate([query[0:128], query[128:256]], axis=1)
    kv = (first_ref[:, 0:128] * inverse).astype(BF16)
    kv_ref[...] = kv
    kvs_ref[zl, y] = kv
    for n in (1, 2, 3):

        @pl.when(c >= n)
        def _():
            queries_ref[n - 1] = jnp.zeros((128, 128), BF16)

    input_ref[...] = (first_ref[:, 128:192] * inverse).astype(BF16)
    gate_ref[...] = (first_ref[:, 192:256] * inverse).astype(BF16)
    rec_ref[...] = (second_ref[:, 0:128] * inverse).astype(BF16)
    forget_ref[...] = (second_ref[:, 128:256] * inverse).astype(BF16)

    def query_copy(d):
        slot = (c + 3) % 4
        return to(query_ref, queries_ref.at[slot], query_send.at[d - 1], query_recv.at[slot], far[4 - d])

    pl.semaphore_wait(near_sem, 2)
    for d in (1, 2, 3):

        @pl.when(c >= d)
        def _():
            query_copy(d).start()

    along_line = [
        to(kv_ref, kvs_ref.at[zl, y], line_send.at[d - 1], line_recv.at[d - 1], line[d]) for d in (1, 2, 3)
    ]
    along_row = [
        [
            to(
                kv_ref if d == 0 else kvs_ref.at[(zl - d + 4) % 4, y],
                kvs_ref.at[(zl - d + 4) % 4, y], row_send.at[d, k], row_recv.at[d, k], row[1 if k == 0 else 3],
            )
            for k in range(2)
        ]
        for d in range(4)
    ]

    def onward(d, k):
        block = kvs_ref.at[(zl - d + 4) % 4, (y + 3) % 4 if k == 0 else (y + 1) % 4, k * 128 : k * 128 + 128]
        return to(block, block, half_send.at[d, k], half_recv.at[d, k], row[1 if k == 0 else 3])

    halves = [[onward(d, k) for k in range(2)] for d in range(4)]
    for copy in along_row[0] + along_line:
        copy.start()
    local_scan(rec_ref, forget_ref, input_ref, low_ref, spike_ref, local_ref, faded_ref, state_ref)
    rows_ref[y] = state_ref[...]
    row_states = [
        to(state_ref, rows_ref.at[y], state_send.at[0, d - 1], state_recv.at[0, d - 1], row[d])
        for d in (1, 2, 3)
    ]

    def pass_on(d):
        for k in range(2):
            along_row[d][k].wait_recv()
            halves[d][k].start()

    along_line[0].wait_recv()
    for copy in along_row[1]:
        copy.start()
    pass_on(0)
    along_line[1].wait_recv()
    for copy in along_row[2] + row_states:
        copy.start()
    pass_on(1)
    along_line[2].wait_recv()
    for copy in along_row[3] + column_copies:
        copy.start()
    for copy in row_states:
        copy.wait_recv()
    state, total, ahead, ahead_total = chain(rows_ref, y)
    planes_ref[zl, 0:REC_VAL, :] = state
    planes_ref[zl, REC_VAL:STATE_ROWS, :] = jnp.broadcast_to(total, (8, REC_KEY))
    line_states = [
        to(planes_ref.at[zl], planes_ref.at[zl], state_send.at[1, n - 1], state_recv.at[1, n - 1], line[n])
        for n in (1, 2, 3)
    ]
    for copy in line_states:
        copy.start()
    for n in (1, 2, 3):

        @pl.when(c < n)
        def _():
            to(
                query_ref, queries_ref.at[n - 1], query_send.at[0], query_recv.at[n - 1], far[1]
            ).wait_recv()

    lane = lax.broadcasted_iota(jnp.int32, (128, 128), 1)
    for n in range(4):
        packed = (query_ref[...] if n == 0 else queries_ref[n - 1]).astype(F32)
        for half in range(2):
            part = packed if half == 0 else pltpu.roll(packed, 64, 1)
            at = n * TOK + half * 128
            q_ref[at : at + 128, :] = jnp.where(lane < HEAD, part, 0.0).astype(BF16)

    def attend_plane(d):
        for k in range(2):
            halves[d][k].wait_recv()
        attend(
            zl * 4 + y, (zl - d + 4) % 4, bias_ref[0] * LOG2E, q_ref, kvs_ref, tri_ref,
            acc_ref.at[d], left_ref.at[d],
        )

    attend_plane(0)
    pass_on(2)
    attend_plane(1)
    pass_on(3)
    for copy in line_states:
        copy.wait_recv()
    state, total, low, low_total = chain(planes_ref, zl)
    group_ref[0:REC_VAL, :] = state
    group_ref[REC_VAL:STATE_ROWS, :] = jnp.broadcast_to(total, (8, REC_KEY))
    before = low * jnp.exp(ahead_total) + ahead
    before_total = low_total + ahead_total

    def back(k, d):
        slot = (c + d + 3) % 4
        src, dst = ((group_ref, groups_ref), (far_ref, part_ref), (far_left_ref, part_left_ref))[k]
        src = src if k == 0 else src.at[slot % 3]
        return to(src, dst.at[c % 3], back_send.at[k, d - 1], back_recv.at[k, c % 3], far[d])

    def arrival(k, g):
        src, dst = ((group_ref, groups_ref), (far_ref.at[0], part_ref), (far_left_ref.at[0], part_left_ref))[k]
        return to(src, dst.at[g], back_send.at[k, 0], back_recv.at[k, g], far[1])

    for d in (1, 2, 3):

        @pl.when(c + d < 4)
        def _():
            back(0, d).start()

    attend_plane(2)
    attend_plane(3)

    def joined(at):
        n = (zl + 1) % 4
        acc, left = acc_ref[n, at, :], left_ref[n, at, :]
        for p in (2, 1, 0):
            n = (zl - p + 4) % 4
            acc = acc + acc_ref[n, at, :] * jnp.exp2(left)
            left = left + left_ref[n, at, :]
        return acc, left

    for n in range(3):
        at = (n + 1) * TOK
        top, top_left = joined(slice(at, at + 128))
        bottom, bottom_left = joined(slice(at + 128, at + 256))
        far_ref[n] = jnp.where(lane < HEAD, pltpu.roll(bottom, 64, 1), top).astype(BF16)
        far_left_ref[n, :, 0:128] = jnp.transpose(top_left)[0:1, :]
        far_left_ref[n, :, 128:256] = jnp.transpose(bottom_left)[0:1, :]
    for d in (3, 2, 1):

        @pl.when(c + d < 4)
        def _():
            back(1, d).start()
            back(2, d).start()

    own_acc, own_left = joined(slice(0, TOK))
    acc_ref[0, 0:TOK, :] = own_acc
    left_ref[0, 0:TOK, :] = own_left

    in_ref[...] = jnp.zeros_like(in_ref)
    for g in (0, 1, 2):

        @pl.when(g < c)
        def _():
            arrival(0, g).wait_recv()
            in_ref[...] = in_ref[...] * jnp.exp(groups_ref[g, REC_VAL : REC_VAL + 1, :]) + groups_ref[
                g, 0:REC_VAL, :
            ]

    entering = in_ref[...] * jnp.exp(before_total) + before
    raw = local_ref[...] + dot(faded_ref[...], entering.astype(BF16), tb=True)
    normed = raw * lax.rsqrt(jnp.mean(raw * raw, axis=1, keepdims=True) + epsilon) * gain_ref[...]
    gate = gate_ref[...].astype(F32)
    heads_ref[:, 0:REC_VAL] = (normed * (gate * jax.nn.sigmoid(gate))).astype(BF16)

    for g in (2, 1, 0):

        @pl.when(g < c)
        def _():
            arrival(1, g).wait_recv()
            arrival(2, g).wait_recv()
            packed = part_ref[g].astype(F32)
            scale = jnp.exp2(left_ref[0, 0:TOK, :])
            acc_ref[0, 0:128, :] += packed * scale[0:128, :]
            acc_ref[0, 128:256, :] += pltpu.roll(packed, 64, 1) * scale[128:256, :]
            for at in (0, 128):
                left_ref[0, at : at + 128, :] += column(part_left_ref[g, 0:1, at : at + 128])

    heads_ref[:, REC_VAL:] = acc_ref[0, 0:TOK, HEAD:].astype(BF16)

    def columns_here():
        for copy in own_columns:
            copy.wait()
        for copy in column_copies:
            copy.wait_recv()

    sum_ref[...] = jnp.zeros_like(sum_ref)

    def add(source, ref):
        sum_ref[...] += dot(ref[...], columns_ref[source])

    ring_gather(heads_ref, head_slots_ref, head_send, head_recv, columns_here, add)
    out_ref[...] = sum_ref[...].astype(BF16)
    sent = along_line + row_states + line_states + column_copies
    for d in range(4):
        sent = sent + along_row[d] + halves[d]
    for copy in sent:
        copy.wait_send()
    for d in (1, 2, 3):

        @pl.when(c >= d)
        def _():
            query_copy(d).wait_send()

        @pl.when(c + d < 4)
        def _():
            for k in range(3):
                back(k, d).wait_send()


def layer(*operands):
    dma = pltpu.SemaphoreType.DMA

    def both(*shape):
        return [dma(shape), dma(shape)]

    return pl.pallas_call(
        layer_kernel,
        out_shape=jax.ShapeDtypeStruct((TOK, 256), BF16),
        in_specs=[SMEM] + [VMEM] * 5 + [ANY] * 9,
        out_specs=VMEM,
        scratch_shapes=[
            pltpu.VMEM((8, TOK, 256), BF16),
            pltpu.VMEM((320, D), BF16),
            pltpu.VMEM((D, 256), BF16),
            pltpu.VMEM((TOK, 320), F32),
            pltpu.VMEM((TOK, 256), F32),
            pltpu.VMEM((TOK, 128), F32),
            pltpu.VMEM((TOK, 128), BF16),
            pltpu.VMEM((128, 128), BF16),
            pltpu.VMEM((TOK, 128), BF16),
            pltpu.VMEM((TOK, 128), BF16),
            pltpu.VMEM((TOK, 64), BF16),
            pltpu.VMEM((TOK, 64), BF16),
            pltpu.VMEM((4, 4, TOK, 128), BF16),
            pltpu.VMEM((3, 128, 128), BF16),
            pltpu.VMEM((STATE_ROWS, REC_KEY), F32),
            pltpu.VMEM((4, STATE_ROWS, REC_KEY), F32),
            pltpu.VMEM((4, STATE_ROWS, REC_KEY), F32),
            pltpu.VMEM((STATE_ROWS, REC_KEY), F32),
            pltpu.VMEM((3, STATE_ROWS, REC_KEY), F32),
            pltpu.VMEM((TOK, REC_VAL), F32),
            pltpu.VMEM((TOK, REC_KEY), BF16),
            pltpu.VMEM((4 * TOK, 128), BF16),
            pltpu.VMEM((TOK, TOK), BF16),
            pltpu.VMEM((4, 4 * TOK, 128), F32),
            pltpu.VMEM((4, 4 * TOK, 128), F32),
            pltpu.VMEM((3, 128, 128), BF16),
            pltpu.VMEM((3, 1, TOK), F32),
            pltpu.VMEM((3, 128, 128), BF16),
            pltpu.VMEM((3, 1, TOK), F32),
            pltpu.VMEM((REC_VAL, REC_KEY), F32),
            pltpu.VMEM((TOK, 128), BF16),
            pltpu.VMEM((8, 128, 256), BF16),
            pltpu.VMEM((8, TOK, 128), BF16),
            pltpu.VMEM((TOK, 256), F32),
            dma((7,)), *both(13), *both(13),
            *both(3), *both(4, 2), *both(4, 2), *both(2, 3),
            *both(3), *both(2, 7), *both(3, 3), dma((2,)), pltpu.SemaphoreType.REGULAR,
        ],
        compiler_params=pltpu.CompilerParams(collective_id=0, has_side_effects=True),
        name="layer",
    )(*operands)


def shards(
    tokens,
    input_norm_gain,
    attention_query_weight,
    attention_key_weight,
    attention_value_weight,
    attention_score_bias,
    recurrence_query_weight,
    forget_weight,
    input_weight,
    output_gate_weight,
    forget_minimum,
    decay_spikes,
    head_norm_gain,
    attention_output_weight,
    recurrence_output_weight,
):
    narrow = (
        attention_key_weight, attention_value_weight, input_weight, output_gate_weight, attention_query_weight
    )
    return layer(
        attention_score_bias, tokens, input_norm_gain[None, :], forget_minimum,
        decay_spikes.reshape(1, TOK), head_norm_gain[None, :],
        *(w.T for w in narrow), recurrence_query_weight, forget_weight,
        recurrence_output_weight, attention_output_weight,
    )


def solution(mesh):
    placed = (
        P("sp", "tp"),
        P(),
        P(None, "tp"),
        P(None, "tp"),
        P(None, "tp"),
        P("tp"),
        P(None, "tp"),
        P(None, "tp"),
        P(None, "tp"),
        P(None, "tp"),
        P("tp", None),
        P("sp", "tp"),
        P(),
        P("tp", None),
        P("tp", None),
    )
    return jax.shard_map(
        shards, mesh=mesh, in_specs=placed, out_specs=P("sp", "tp"), check_vma=False
    )
```

```python
import functools

import jax
import jax.numpy as jnp
from jax import lax
from jax.experimental import pallas as pl
from jax.experimental.pallas import tpu as pltpu
from jax.sharding import PartitionSpec as P

D = 2048
HEAD = 64
REC_KEY = 128
REC_VAL = 64
REC_SPAN = 64
TOK = 256
LOG2E = 1.4426950408889634
STATE_ROWS = REC_VAL + 8
epsilon = 1e-06
F32, BF16 = jnp.float32, jnp.bfloat16
VMEM = pl.BlockSpec(memory_space=pltpu.VMEM)
SMEM = pl.BlockSpec(memory_space=pltpu.SMEM)
ANY = pl.BlockSpec(memory_space=pl.ANY)
MESH = pl.DeviceIdType.MESH


def dot(a, b, ta=False, tb=False):
    dims = (((0 if ta else 1,), (1 if tb else 0,)), ((), ()))
    return lax.dot_general(a, b, dims, preferred_element_type=F32)


def to(src, dst, send, recv, sp):
    return pltpu.make_async_remote_copy(
        src_ref=src, dst_ref=dst, send_sem=send, recv_sem=recv,
        device_id={"sp": sp}, device_id_type=MESH,
    )


def place():
    sp = lax.axis_index("sp")
    return sp, sp // 16, (sp // 4) % 4, sp % 4


def lanes():
    tp = lax.axis_index("tp")
    x, core = tp // 2, tp % 2
    return tp, tp + 1 - 2 * core, (tp + 2) % 8, (tp + 6) % 8, (tp + 4) % 8, 1 - 2 * core


def ring_gather(chunk_ref, slots_ref, send, recv, meanwhile, use):
    tp, partner, right, left, across, twist = lanes()
    half = chunk_ref.shape[0] // 2
    top, low = slice(0, half), slice(half, 2 * half)

    def copy(n, src, dst, target):
        return pltpu.make_async_remote_copy(
            src_ref=src, dst_ref=dst, send_sem=send.at[n], recv_sem=recv.at[n],
            device_id={"tp": target}, device_id_type=MESH,
        )

    def relay(n, source, part, target):
        return copy(n, slots_ref.at[source, part], slots_ref.at[source, part], target)

    copies = [
        copy(0, chunk_ref, slots_ref.at[tp], partner),
        copy(1, chunk_ref.at[top], slots_ref.at[tp, top], right),
        copy(2, chunk_ref.at[low], slots_ref.at[tp, low], left),
        copy(3, chunk_ref.at[low], slots_ref.at[tp, low], right),
        copy(4, chunk_ref.at[top], slots_ref.at[tp, top], left),
        relay(5, left, top, right),
        relay(6, right, low, left),
        relay(7, left, top, partner),
        relay(8, right, low, partner),
        relay(9, left, low, partner),
        relay(10, right, top, partner),
        relay(11, across, top, partner),
        relay(12, across, low, partner),
    ]
    for n in range(5):
        copies[n].start()
    meanwhile()
    use(tp, chunk_ref)
    copies[1].wait_recv()
    copies[5].start()
    copies[7].start()
    copies[2].wait_recv()
    copies[6].start()
    copies[8].start()
    copies[0].wait_recv()
    use(partner, slots_ref.at[partner])
    copies[3].wait_recv()
    copies[9].start()
    copies[4].wait_recv()
    copies[10].start()
    use(left, slots_ref.at[left])
    use(right, slots_ref.at[right])
    copies[7].wait_recv()
    copies[9].wait_recv()
    use(left + twist, slots_ref.at[left + twist])
    copies[8].wait_recv()
    copies[10].wait_recv()
    use(right + twist, slots_ref.at[right + twist])
    copies[5].wait_recv()
    copies[11].start()
    copies[6].wait_recv()
    copies[12].start()
    use(across, slots_ref.at[across])
    copies[11].wait_recv()
    copies[12].wait_recv()
    use(across + twist, slots_ref.at[across + twist])
    for one in copies:
        one.wait_send()


def column(row):
    return jnp.transpose(jnp.broadcast_to(row, (128, 128)))


def local_scan(query_ref, forget_ref, input_ref, low_ref, spike_ref, out_ref, lift_ref, state_ref):
    span = REC_SPAN
    rows = lax.broadcasted_iota(jnp.int32, (span, span), 0)
    cols = lax.broadcasted_iota(jnp.int32, (span, span), 1)
    causal = cols <= rows
    ones = jnp.where(causal, 1.0, 0.0)
    spikes = jnp.concatenate([column(spike_ref[:, n : n + 128]) for n in (0, 128)], axis=0)
    state = jnp.zeros((REC_VAL, REC_KEY), F32)
    offset = jnp.zeros((1, REC_KEY), F32)
    for n in range(query_ref.shape[0] // span):
        at = slice(n * span, (n + 1) * span)
        query = query_ref[at, :].astype(F32)
        lifted = query * jax.nn.sigmoid(query)
        intake = (1.0 - low_ref[...]) * jax.nn.sigmoid(-forget_ref[at, :].astype(F32))
        log_forget = jnp.log1p(-intake) + spikes[at, :]
        running = lax.dot_general(
            ones, log_forget, (((1,), (0,)), ((), ())),
            precision=lax.Precision.HIGHEST, preferred_element_type=F32,
        )
        total = running[span - 1 : span, :]
        middle = running[span // 2 - 1 : span // 2, :]
        value = input_ref[at, :]
        grown = (lifted * jnp.exp(running - middle)).astype(BF16)
        shrunk = (intake * jnp.exp(middle - running)).astype(BF16)
        inner = jnp.where(causal, dot(grown, shrunk, tb=True), 0.0)
        faded = (lifted * jnp.exp(running)).astype(BF16)
        out_ref[at, :] = dot(inner.astype(BF16), value) + dot(faded, state.astype(BF16), tb=True)
        lift_ref[at, :] = (lifted * jnp.exp(running + offset)).astype(BF16)
        kept = (intake * jnp.exp(total - running)).astype(BF16)
        state = state * jnp.exp(total) + dot(value, kept, ta=True)
        offset = offset + total
    state_ref[0:REC_VAL, :] = state
    state_ref[REC_VAL:STATE_ROWS, :] = jnp.broadcast_to(offset, (8, REC_KEY))


def attend(first, here, plane, bias2, q_ref, kvs_ref, tri_ref, acc_ref, left_ref):
    at = slice(first, first + 2 * TOK)
    ahead = lax.broadcasted_iota(jnp.int32, (TOK, TOK), 1) - lax.broadcasted_iota(jnp.int32, (TOK, TOK), 0)
    q, tri = q_ref[at, :], tri_ref[...]
    acc = jnp.zeros((2 * TOK, 128), F32)
    left = jnp.zeros((2 * TOK, 1), F32)
    for n in (3, 2, 1, 0):

        def masked(x):
            if first > 0:
                return x
            keep = ahead < (here - plane * 4 - n) * TOK
            return jnp.concatenate([jnp.where(keep, x[0:TOK], 0.0), x[TOK:]], axis=0)

        kv = kvs_ref[plane, n]
        z = dot(q, kv, tb=True) * (LOG2E / 8.0) + bias2
        soft = masked(jnp.maximum(z, jnp.log(1.0 + jnp.exp2(jnp.minimum(z, 30.0))) * LOG2E))
        later = dot(soft.astype(BF16), tri)
        weight = masked(jnp.exp2((z - soft) + (later + left)))
        acc = acc + dot(weight.astype(BF16), kv)
        left = left + (later[:, 0:1] - soft[:, 0:1])
    acc_ref[at, :] = acc
    left_ref[at, :] = jnp.broadcast_to(left, (2 * TOK, 128))


def pack(top, low, natural):
    lane = lax.broadcasted_iota(jnp.int32, (128, 128), 1)
    return jnp.where((lane < HEAD) == (natural == 0), top, pltpu.roll(low, 64, 1)).astype(BF16)


def unpack(packed, natural):
    lane = lax.broadcasted_iota(jnp.int32, (128, 128), 1)
    keep = (lane < HEAD) == (natural == 0)
    packed = packed.astype(F32)
    low = pltpu.roll(packed, 64, 1)
    return jnp.concatenate([jnp.where(keep, packed, 0.0), jnp.where(keep, low, 0.0)], axis=0).astype(BF16)


def chain(states_ref, here):
    state = states_ref[0, 0:REC_VAL, :]
    total = states_ref[0, REC_VAL : REC_VAL + 1, :]
    ahead, ahead_total = jnp.zeros_like(state), jnp.zeros_like(total)
    for n in range(1, 4):
        ahead = jnp.where(n <= here, state, ahead)
        ahead_total = jnp.where(n <= here, total, ahead_total)
        more = states_ref[n, REC_VAL : REC_VAL + 1, :]
        state = state * jnp.exp(more) + states_ref[n, 0:REC_VAL, :]
        total = total + more
    return state, total, ahead, ahead_total


def layer_kernel(
    bias_ref, token_ref, feature_gain_ref, low_ref, spike_ref, gain_ref,
    key_w, value_w, input_w, gate_w, query_w, rec_w, forget_w, rec_out_w, att_out_w,
    out_ref,
    slots_ref, narrow_ref, wide_ref, first_ref, second_ref, square_ref,
    kv_ref, query_ref, rec_ref, forget_ref, input_ref, gate_ref,
    kvs_ref, queries_ref, state_ref, rows_ref, planes_ref, group_ref, groups_ref,
    local_ref, faded_ref, q_ref, tri_ref, acc_ref, left_ref,
    far_ref, far_left_ref, part_ref, part_left_ref, in_ref,
    heads_ref, columns_ref, head_slots_ref, early_ref, early_slots_ref,
    load, early_send, early_recv, token_send, token_recv, head_send, head_recv,
    line_send, line_recv, row_send, row_recv, half_send, half_recv, state_send, state_recv,
    query_send, query_recv, column_send, column_recv, back_send, back_recv, own_sem, near_sem,
):
    sp, c, zl, y = place()
    tp = lax.axis_index("tp")
    base = c * 16
    row = [base + zl * 4 + (y + d) % 4 for d in range(4)]
    line = [base + ((zl + d) % 4) * 4 + y for d in range(4)]
    far = [(sp + 16 * d) % 64 for d in range(4)]
    lane_peers = [(tp + d) % 8 for d in range(1, 8)]

    narrow = (key_w, value_w, input_w, gate_w, query_w)
    loads = [
        pltpu.make_async_copy(w, narrow_ref.at[n * 64 : n * 64 + 64], load.at[n])
        for n, w in enumerate(narrow)
    ]
    loads += [
        pltpu.make_async_copy(w, wide_ref.at[:, n * 128 : n * 128 + 128], load.at[5 + n])
        for n, w in enumerate((rec_w, forget_w))
    ]

    def columns(w, there):
        return w.at[:, pl.ds(pl.multiple_of(there * 256, 256), 256)]

    out_w = ((0, rec_out_w), (1, att_out_w))
    own_columns = [
        pltpu.make_async_copy(columns(w, tp), columns_ref.at[tp, n * 64 : n * 64 + 64], own_sem.at[n])
        for n, w in out_w
    ]
    column_copies = [
        pltpu.make_async_remote_copy(
            src_ref=columns(w, there), dst_ref=columns_ref.at[tp, n * 64 : n * 64 + 64],
            send_sem=column_send.at[n, d], recv_sem=column_recv.at[n, d],
            device_id={"tp": there}, device_id_type=MESH,
        )
        for n, w in out_w
        for d, there in enumerate(lane_peers)
    ]

    barrier = pltpu.get_barrier_semaphore()
    near = row[1:] + line[1:] + [far[1], far[3]]
    for peer in lane_peers:
        pl.semaphore_signal(barrier, inc=1, device_id={"tp": peer}, device_id_type=MESH)
    for peer in near:
        pl.semaphore_signal(barrier, inc=1, device_id={"sp": peer}, device_id_type=MESH)
    for copy in loads + own_columns:
        copy.start()
    first_ref[...] = jnp.zeros_like(first_ref)
    second_ref[...] = jnp.zeros_like(second_ref)
    square_ref[...] = jnp.zeros_like(square_ref)
    rows = lax.broadcasted_iota(jnp.int32, (TOK, TOK), 0)
    cols = lax.broadcasted_iota(jnp.int32, (TOK, TOK), 1)
    tri_ref[...] = jnp.where(rows > cols, -1.0, 0.0).astype(BF16)
    pl.semaphore_wait(barrier, len(lane_peers) + len(near))
    for peer in (far[1], far[3]):
        pl.semaphore_signal(near_sem, inc=1, device_id={"sp": peer}, device_id_type=MESH)

    def meanwhile():
        for one in loads:
            one.wait()

    def use(source, ref):
        at = pl.ds(pl.multiple_of(source * 256, 256), 256)
        values = ref[...].astype(F32)
        squares = values * values
        square_ref[...] += squares[:, 0:128] + squares[:, 128:256]
        scaled = (values * feature_gain_ref[:, at]).astype(BF16)
        first_ref[...] += dot(scaled, narrow_ref[:, at], tb=True)
        second_ref[...] += dot(scaled, wide_ref[at, :])

    ring_gather(token_ref, slots_ref, token_send, token_recv, meanwhile, use)
    inverse = lax.rsqrt(jnp.sum(square_ref[...], axis=1, keepdims=True) / D + epsilon)
    query = (first_ref[:, 256:320] * inverse).astype(BF16)
    query_ref[...] = jnp.concatenate([query[0:128], query[128:256]], axis=1)
    kv = (first_ref[:, 0:128] * inverse).astype(BF16)
    kv_ref[...] = kv
    kvs_ref[zl, y] = kv
    for n in (1, 2, 3):

        @pl.when(c >= n)
        def _():
            queries_ref[n - 1] = jnp.zeros((128, 128), BF16)

    input_ref[...] = (first_ref[:, 128:192] * inverse).astype(BF16)
    gate_ref[...] = (first_ref[:, 192:256] * inverse).astype(BF16)
    rec_ref[...] = (second_ref[:, 0:128] * inverse).astype(BF16)
    forget_ref[...] = (second_ref[:, 128:256] * inverse).astype(BF16)

    def query_copy(d):
        slot = (c + 3) % 4
        return to(query_ref, queries_ref.at[slot], query_send.at[d - 1], query_recv.at[slot], far[4 - d])

    pl.semaphore_wait(near_sem, 2)
    for d in (1, 2, 3):

        @pl.when(c >= d)
        def _():
            query_copy(d).start()

    along_line = [
        to(kv_ref, kvs_ref.at[zl, y], line_send.at[d - 1], line_recv.at[d - 1], line[d]) for d in (1, 2, 3)
    ]
    along_row = [
        [
            to(
                kv_ref if d == 0 else kvs_ref.at[(zl - d + 4) % 4, y],
                kvs_ref.at[(zl - d + 4) % 4, y], row_send.at[d, k], row_recv.at[d, k], row[1 if k == 0 else 3],
            )
            for k in range(2)
        ]
        for d in range(4)
    ]

    def onward(d, k):
        block = kvs_ref.at[(zl - d + 4) % 4, (y + 3) % 4 if k == 0 else (y + 1) % 4, k * 128 : k * 128 + 128]
        return to(block, block, half_send.at[d, k], half_recv.at[d, k], row[1 if k == 0 else 3])

    halves = [[onward(d, k) for k in range(2)] for d in range(4)]
    for copy in along_row[0] + along_line:
        copy.start()
    local_scan(rec_ref, forget_ref, input_ref, low_ref, spike_ref, local_ref, faded_ref, state_ref)
    rows_ref[y] = state_ref[...]
    row_states = [
        to(state_ref, rows_ref.at[y], state_send.at[0, d - 1], state_recv.at[0, d - 1], row[d])
        for d in (1, 2, 3)
    ]

    def pass_on(d):
        for k in range(2):
            along_row[d][k].wait_recv()
            halves[d][k].start()

    along_line[0].wait_recv()
    for copy in along_row[1]:
        copy.start()
    pass_on(0)
    along_line[1].wait_recv()
    for copy in along_row[2] + row_states:
        copy.start()
    pass_on(1)
    along_line[2].wait_recv()
    for copy in along_row[3] + column_copies:
        copy.start()
    for copy in row_states:
        copy.wait_recv()
    state, total, ahead, ahead_total = chain(rows_ref, y)
    planes_ref[zl, 0:REC_VAL, :] = state
    planes_ref[zl, REC_VAL:STATE_ROWS, :] = jnp.broadcast_to(total, (8, REC_KEY))
    line_states = [
        to(planes_ref.at[zl], planes_ref.at[zl], state_send.at[1, n - 1], state_recv.at[1, n - 1], line[n])
        for n in (1, 2, 3)
    ]
    for copy in line_states:
        copy.start()
    def take(n):
        if n > 0:

            @pl.when(c < n)
            def _():
                to(
                    query_ref, queries_ref.at[n - 1], query_send.at[0], query_recv.at[n - 1], far[1]
                ).wait_recv()

        packed = query_ref[...] if n == 0 else queries_ref[n - 1]
        q_ref[n * TOK : (n + 1) * TOK, :] = unpack(packed, 0)

    def attend_plane(d, first):
        if first == (0 if d == 0 or d == 1 else 2 * TOK):
            for k in range(2):
                halves[d][k].wait_recv()
        attend(
            first, zl * 4 + y, (zl - d + 4) % 4, bias_ref[0] * LOG2E, q_ref, kvs_ref, tri_ref,
            acc_ref.at[d], left_ref.at[d],
        )

    take(0)
    take(1)
    attend_plane(0, 0)
    take(2)
    take(3)
    attend_plane(0, 2 * TOK)
    pass_on(2)
    attend_plane(1, 0)
    pass_on(3)
    for copy in line_states:
        copy.wait_recv()
    state, total, low, low_total = chain(planes_ref, zl)
    group_ref[0:REC_VAL, :] = state
    group_ref[REC_VAL:STATE_ROWS, :] = jnp.broadcast_to(total, (8, REC_KEY))
    before = low * jnp.exp(ahead_total) + ahead
    before_total = low_total + ahead_total

    def back(k, d):
        slot = (c + d + 3) % 4
        src, dst = ((group_ref, groups_ref), (far_ref, part_ref), (far_left_ref, part_left_ref))[k]
        src = src if k == 0 else src.at[slot % 3]
        return to(src, dst.at[c % 3], back_send.at[k, d - 1], back_recv.at[k, c % 3], far[d])

    def arrival(k, g):
        src, dst = ((group_ref, groups_ref), (far_ref.at[0], part_ref), (far_left_ref.at[0], part_left_ref))[k]
        return to(src, dst.at[g], back_send.at[k, 0], back_recv.at[k, g], far[1])

    for d in (1, 2, 3):

        @pl.when(c + d < 4)
        def _():
            back(0, d).start()

    attend_plane(1, 2 * TOK)
    attend_plane(2, 2 * TOK)
    attend_plane(3, 2 * TOK)

    def joined(at):
        n = (zl + 1) % 4
        acc, left = acc_ref[n, at, :], left_ref[n, at, :]
        for p in (2, 1, 0):
            n = (zl - p + 4) % 4
            acc = acc + acc_ref[n, at, :] * jnp.exp2(left)
            left = left + left_ref[n, at, :]
        return acc, left

    def ready(n):
        at = (n + 1) * TOK
        top, top_left = joined(slice(at, at + 128))
        low, low_left = joined(slice(at + 128, at + 256))
        far_ref[n] = pack(top, low, 1)
        far_left_ref[n, :, 0:128] = jnp.transpose(top_left)[0:1, :]
        far_left_ref[n, :, 128:256] = jnp.transpose(low_left)[0:1, :]

    ready(1)
    ready(2)
    for d in (2, 3, 1):

        @pl.when((c + d < 4) & (c + d > 1))
        def _():
            back(1, d).start()
            back(2, d).start()

    in_ref[...] = jnp.zeros_like(in_ref)
    for g in (0, 1, 2):

        @pl.when(g < c)
        def _():
            arrival(0, g).wait_recv()
            in_ref[...] = in_ref[...] * jnp.exp(groups_ref[g, REC_VAL : REC_VAL + 1, :]) + groups_ref[
                g, 0:REC_VAL, :
            ]

    entering = in_ref[...] * jnp.exp(before_total) + before
    raw = local_ref[...] + dot(faded_ref[...], entering.astype(BF16), tb=True)
    normed = raw * lax.rsqrt(jnp.mean(raw * raw, axis=1, keepdims=True) + epsilon) * gain_ref[...]
    gate = gate_ref[...].astype(F32)
    state_heads = normed * (gate * jax.nn.sigmoid(gate))
    state_heads = jnp.concatenate([state_heads, jnp.zeros_like(state_heads)], axis=1)
    early_ref[...] = pack(state_heads[0:128], state_heads[128:256], 0)
    early_copies = [
        pltpu.make_async_remote_copy(
            src_ref=early_ref, dst_ref=early_slots_ref.at[tp], send_sem=early_send.at[d],
            recv_sem=early_recv.at[d], device_id={"tp": there}, device_id_type=MESH,
        )
        for d, there in enumerate(lane_peers)
    ]
    for copy in early_copies:
        copy.start()
    early_slots_ref[tp] = early_ref[...]

    attend_plane(2, 0)
    attend_plane(3, 0)
    ready(0)

    @pl.when(c == 0)
    def _():
        back(1, 1).start()
        back(2, 1).start()

    own_acc, own_left = joined(slice(0, TOK))
    acc_ref[0, 0:TOK, :] = own_acc
    left_ref[0, 0:TOK, :] = own_left

    for g in (2, 1, 0):

        @pl.when(g < c)
        def _():
            arrival(1, g).wait_recv()
            arrival(2, g).wait_recv()
            packed = part_ref[g].astype(F32)
            scale = jnp.exp2(left_ref[0, 0:TOK, :])
            acc_ref[0, 0:128, :] += packed * scale[0:128, :]
            acc_ref[0, 128:256, :] += pltpu.roll(packed, 64, 1) * scale[128:256, :]
            for at in (0, 128):
                left_ref[0, at : at + 128, :] += column(part_left_ref[g, 0:1, at : at + 128])

    heads_ref[...] = pack(acc_ref[0, 0:128, :], acc_ref[0, 128:256, :], 1)

    def columns_here():
        for copy in own_columns:
            copy.wait()
        for copy in column_copies + early_copies:
            copy.wait_recv()
        out_ref[...] = jnp.zeros_like(out_ref)
        for n in range(8):
            add(n, early_slots_ref.at[n], 0)

    def add(source, ref, natural=1):
        out_ref[...] += dot(unpack(ref[...], natural), columns_ref[source])

    ring_gather(heads_ref, head_slots_ref, head_send, head_recv, columns_here, add)
    sent = early_copies + along_line + row_states + line_states + column_copies
    for d in range(4):
        sent = sent + along_row[d] + halves[d]
    for copy in sent:
        copy.wait_send()
    for d in (1, 2, 3):

        @pl.when(c >= d)
        def _():
            query_copy(d).wait_send()

        @pl.when(c + d < 4)
        def _():
            for k in range(3):
                back(k, d).wait_send()


def layer(*operands):
    dma = pltpu.SemaphoreType.DMA

    def both(*shape):
        return [dma(shape), dma(shape)]

    return pl.pallas_call(
        layer_kernel,
        out_shape=jax.ShapeDtypeStruct((TOK, 256), F32),
        in_specs=[SMEM] + [VMEM] * 5 + [ANY] * 9,
        out_specs=VMEM,
        scratch_shapes=[
            pltpu.VMEM((8, TOK, 256), BF16),
            pltpu.VMEM((320, D), BF16),
            pltpu.VMEM((D, 256), BF16),
            pltpu.VMEM((TOK, 320), F32),
            pltpu.VMEM((TOK, 256), F32),
            pltpu.VMEM((TOK, 128), F32),
            pltpu.VMEM((TOK, 128), BF16),
            pltpu.VMEM((128, 128), BF16),
            pltpu.VMEM((TOK, 128), BF16),
            pltpu.VMEM((TOK, 128), BF16),
            pltpu.VMEM((TOK, 64), BF16),
            pltpu.VMEM((TOK, 64), BF16),
            pltpu.VMEM((4, 4, TOK, 128), BF16),
            pltpu.VMEM((3, 128, 128), BF16),
            pltpu.VMEM((STATE_ROWS, REC_KEY), F32),
            pltpu.VMEM((4, STATE_ROWS, REC_KEY), F32),
            pltpu.VMEM((4, STATE_ROWS, REC_KEY), F32),
            pltpu.VMEM((STATE_ROWS, REC_KEY), F32),
            pltpu.VMEM((3, STATE_ROWS, REC_KEY), F32),
            pltpu.VMEM((TOK, REC_VAL), F32),
            pltpu.VMEM((TOK, REC_KEY), BF16),
            pltpu.VMEM((4 * TOK, 128), BF16),
            pltpu.VMEM((TOK, TOK), BF16),
            pltpu.VMEM((4, 4 * TOK, 128), F32),
            pltpu.VMEM((4, 4 * TOK, 128), F32),
            pltpu.VMEM((3, 128, 128), BF16),
            pltpu.VMEM((3, 1, TOK), F32),
            pltpu.VMEM((3, 128, 128), BF16),
            pltpu.VMEM((3, 1, TOK), F32),
            pltpu.VMEM((REC_VAL, REC_KEY), F32),
            pltpu.VMEM((128, 128), BF16),
            pltpu.VMEM((8, 128, 256), BF16),
            pltpu.VMEM((8, 128, 128), BF16),
            pltpu.VMEM((128, 128), BF16),
            pltpu.VMEM((8, 128, 128), BF16),
            dma((7,)), *both(7), *both(13), *both(13),
            *both(3), *both(4, 2), *both(4, 2), *both(2, 3),
            *both(3), *both(2, 7), *both(3, 3), dma((2,)), pltpu.SemaphoreType.REGULAR,
        ],
        compiler_params=pltpu.CompilerParams(collective_id=0, has_side_effects=True),
        name="layer",
    )(*operands)


def shards(
    tokens,
    input_norm_gain,
    attention_query_weight,
    attention_key_weight,
    attention_value_weight,
    attention_score_bias,
    recurrence_query_weight,
    forget_weight,
    input_weight,
    output_gate_weight,
    forget_minimum,
    decay_spikes,
    head_norm_gain,
    attention_output_weight,
    recurrence_output_weight,
):
    narrow = (
        attention_key_weight, attention_value_weight, input_weight, output_gate_weight, attention_query_weight
    )
    return layer(
        attention_score_bias, tokens, input_norm_gain[None, :], forget_minimum,
        decay_spikes.reshape(1, TOK), head_norm_gain[None, :],
        *(w.T for w in narrow), recurrence_query_weight, forget_weight,
        recurrence_output_weight, attention_output_weight,
    ).astype(BF16)


def solution(mesh):
    placed = (
        P("sp", "tp"),
        P(),
        P(None, "tp"),
        P(None, "tp"),
        P(None, "tp"),
        P("tp"),
        P(None, "tp"),
        P(None, "tp"),
        P(None, "tp"),
        P(None, "tp"),
        P("tp", None),
        P("sp", "tp"),
        P(),
        P("tp", None),
        P("tp", None),
    )
    return jax.shard_map(
        shards, mesh=mesh, in_specs=placed, out_specs=P("sp", "tp"), check_vma=False
    )
```

```python
import functools

import jax
import jax.numpy as jnp
from jax import lax
from jax.experimental import pallas as pl
from jax.experimental.pallas import tpu as pltpu
from jax.sharding import PartitionSpec as P

D = 2048
HEAD = 64
REC_KEY = 128
REC_VAL = 64
REC_SPAN = 64
TOK = 256
LOG2E = 1.4426950408889634
STATE_ROWS = REC_VAL + 8
epsilon = 1e-06
F32, BF16 = jnp.float32, jnp.bfloat16
VMEM = pl.BlockSpec(memory_space=pltpu.VMEM)
SMEM = pl.BlockSpec(memory_space=pltpu.SMEM)
ANY = pl.BlockSpec(memory_space=pl.ANY)
MESH = pl.DeviceIdType.MESH


def dot(a, b, ta=False, tb=False):
    dims = (((0 if ta else 1,), (1 if tb else 0,)), ((), ()))
    return lax.dot_general(a, b, dims, preferred_element_type=F32)


def to(src, dst, send, recv, sp):
    return pltpu.make_async_remote_copy(
        src_ref=src, dst_ref=dst, send_sem=send, recv_sem=recv,
        device_id={"sp": sp}, device_id_type=MESH,
    )


def place():
    sp = lax.axis_index("sp")
    return sp, sp // 16, (sp // 4) % 4, sp % 4


def lanes():
    tp = lax.axis_index("tp")
    x, core = tp // 2, tp % 2
    return tp, tp + 1 - 2 * core, (tp + 2) % 8, (tp + 6) % 8, (tp + 4) % 8, 1 - 2 * core


def ring_gather(chunk_ref, slots_ref, send, recv, meanwhile, use):
    tp, partner, right, left, across, twist = lanes()
    half = chunk_ref.shape[0] // 2
    top, low = slice(0, half), slice(half, 2 * half)

    def copy(n, src, dst, target):
        return pltpu.make_async_remote_copy(
            src_ref=src, dst_ref=dst, send_sem=send.at[n], recv_sem=recv.at[n],
            device_id={"tp": target}, device_id_type=MESH,
        )

    def relay(n, source, part, target):
        return copy(n, slots_ref.at[source, part], slots_ref.at[source, part], target)

    copies = [
        copy(0, chunk_ref, slots_ref.at[tp], partner),
        copy(1, chunk_ref.at[top], slots_ref.at[tp, top], right),
        copy(2, chunk_ref.at[low], slots_ref.at[tp, low], left),
        copy(3, chunk_ref.at[low], slots_ref.at[tp, low], right),
        copy(4, chunk_ref.at[top], slots_ref.at[tp, top], left),
        relay(5, left, top, right),
        relay(6, right, low, left),
        relay(7, left, top, partner),
        relay(8, right, low, partner),
        relay(9, left, low, partner),
        relay(10, right, top, partner),
        relay(11, across, top, partner),
        relay(12, across, low, partner),
    ]
    for n in range(5):
        copies[n].start()
    meanwhile()
    use(tp, chunk_ref)
    copies[1].wait_recv()
    copies[5].start()
    copies[7].start()
    copies[2].wait_recv()
    copies[6].start()
    copies[8].start()
    copies[0].wait_recv()
    use(partner, slots_ref.at[partner])
    copies[3].wait_recv()
    copies[9].start()
    copies[4].wait_recv()
    copies[10].start()
    use(left, slots_ref.at[left])
    use(right, slots_ref.at[right])
    copies[7].wait_recv()
    copies[9].wait_recv()
    use(left + twist, slots_ref.at[left + twist])
    copies[8].wait_recv()
    copies[10].wait_recv()
    use(right + twist, slots_ref.at[right + twist])
    copies[5].wait_recv()
    copies[11].start()
    copies[6].wait_recv()
    copies[12].start()
    use(across, slots_ref.at[across])
    copies[11].wait_recv()
    copies[12].wait_recv()
    use(across + twist, slots_ref.at[across + twist])
    for one in copies:
        one.wait_send()


def column(row):
    return jnp.transpose(jnp.broadcast_to(row, (128, 128)))


def local_scan(query_ref, forget_ref, input_ref, low_ref, spike_ref, out_ref, lift_ref, state_ref):
    span = REC_SPAN
    rows = lax.broadcasted_iota(jnp.int32, (span, span), 0)
    cols = lax.broadcasted_iota(jnp.int32, (span, span), 1)
    causal = cols <= rows
    ones = jnp.where(causal, 1.0, 0.0)
    spikes = jnp.concatenate([column(spike_ref[:, n : n + 128]) for n in (0, 128)], axis=0)
    state = jnp.zeros((REC_VAL, REC_KEY), F32)
    offset = jnp.zeros((1, REC_KEY), F32)
    for n in range(query_ref.shape[0] // span):
        at = slice(n * span, (n + 1) * span)
        query = query_ref[at, :].astype(F32)
        lifted = query * jax.nn.sigmoid(query)
        intake = (1.0 - low_ref[...]) * jax.nn.sigmoid(-forget_ref[at, :].astype(F32))
        log_forget = jnp.log1p(-intake) + spikes[at, :]
        running = lax.dot_general(
            ones, log_forget, (((1,), (0,)), ((), ())),
            precision=lax.Precision.HIGHEST, preferred_element_type=F32,
        )
        total = running[span - 1 : span, :]
        middle = running[span // 2 - 1 : span // 2, :]
        value = input_ref[at, :]
        grown = (lifted * jnp.exp(running - middle)).astype(BF16)
        shrunk = (intake * jnp.exp(middle - running)).astype(BF16)
        inner = jnp.where(causal, dot(grown, shrunk, tb=True), 0.0)
        faded = (lifted * jnp.exp(running)).astype(BF16)
        out_ref[at, :] = dot(inner.astype(BF16), value) + dot(faded, state.astype(BF16), tb=True)
        lift_ref[at, :] = (lifted * jnp.exp(running + offset)).astype(BF16)
        kept = (intake * jnp.exp(total - running)).astype(BF16)
        state = state * jnp.exp(total) + dot(value, kept, ta=True)
        offset = offset + total
    state_ref[0:REC_VAL, :] = state
    state_ref[REC_VAL:STATE_ROWS, :] = jnp.broadcast_to(offset, (8, REC_KEY))


def attend(first, here, plane, bias2, q_ref, kvs_ref, tri_ref, acc_ref, left_ref):
    at = slice(first, first + 2 * TOK)
    ahead = lax.broadcasted_iota(jnp.int32, (TOK, TOK), 1) - lax.broadcasted_iota(jnp.int32, (TOK, TOK), 0)
    q, tri = q_ref[at, :], tri_ref[...]
    acc = jnp.zeros((2 * TOK, 128), F32)
    left = jnp.zeros((2 * TOK, 1), F32)
    for n in (3, 2, 1, 0):

        def masked(x):
            if first > 0:
                return x
            keep = ahead < (here - plane * 4 - n) * TOK
            return jnp.concatenate([jnp.where(keep, x[0:TOK], 0.0), x[TOK:]], axis=0)

        kv = kvs_ref[plane, n]
        z = dot(q, kv, tb=True) * (LOG2E / 8.0) + bias2
        soft = masked(jnp.maximum(z, jnp.log(1.0 + jnp.exp2(jnp.minimum(z, 30.0))) * LOG2E))
        later = dot(soft.astype(BF16), tri)
        weight = masked(jnp.exp2((z - soft) + (later + left)))
        acc = acc + dot(weight.astype(BF16), kv)
        left = left + (later[:, 0:1] - soft[:, 0:1])
    acc_ref[at, :] = acc
    left_ref[at, :] = jnp.broadcast_to(left, (2 * TOK, 128))


def pack(top, low, natural):
    lane = lax.broadcasted_iota(jnp.int32, (128, 128), 1)
    return jnp.where((lane < HEAD) == (natural == 0), top, pltpu.roll(low, 64, 1)).astype(BF16)


def unpack(packed, natural):
    lane = lax.broadcasted_iota(jnp.int32, (128, 128), 1)
    keep = (lane < HEAD) == (natural == 0)
    packed = packed.astype(F32)
    low = pltpu.roll(packed, 64, 1)
    return jnp.concatenate([jnp.where(keep, packed, 0.0), jnp.where(keep, low, 0.0)], axis=0).astype(BF16)


def chain(states_ref, here):
    state = states_ref[0, 0:REC_VAL, :]
    total = states_ref[0, REC_VAL : REC_VAL + 1, :]
    ahead, ahead_total = jnp.zeros_like(state), jnp.zeros_like(total)
    for n in range(1, 4):
        ahead = jnp.where(n <= here, state, ahead)
        ahead_total = jnp.where(n <= here, total, ahead_total)
        more = states_ref[n, REC_VAL : REC_VAL + 1, :]
        state = state * jnp.exp(more) + states_ref[n, 0:REC_VAL, :]
        total = total + more
    return state, total, ahead, ahead_total


def layer_kernel(
    bias_ref, token_ref, feature_gain_ref, low_ref, spike_ref, gain_ref,
    key_w, value_w, input_w, gate_w, query_w, rec_w, forget_w, rec_out_w, att_out_w,
    out_ref,
    slots_ref, narrow_ref, wide_ref, first_ref, second_ref, square_ref,
    kv_ref, query_ref, rec_ref, forget_ref, input_ref, gate_ref,
    kvs_ref, queries_ref, state_ref, rows_ref, planes_ref, group_ref, groups_ref,
    local_ref, faded_ref, q_ref, tri_ref, acc_ref, left_ref,
    far_ref, far_left_ref, part_ref, part_left_ref, in_ref,
    heads_ref, columns_ref, head_slots_ref, early_ref, early_slots_ref,
    load, early_send, early_recv, token_send, token_recv, head_send, head_recv,
    line_send, line_recv, row_send, row_recv, half_send, half_recv, state_send, state_recv,
    query_send, query_recv, column_send, column_recv, back_send, back_recv, own_sem, near_sem,
):
    sp, c, zl, y = place()
    tp = lax.axis_index("tp")
    base = c * 16
    row = [base + zl * 4 + (y + d) % 4 for d in range(4)]
    line = [base + ((zl + d) % 4) * 4 + y for d in range(4)]
    far = [(sp + 16 * d) % 64 for d in range(4)]
    lane_peers = [(tp + d) % 8 for d in range(1, 8)]

    narrow = (key_w, value_w, input_w, gate_w, query_w)
    loads = [
        pltpu.make_async_copy(w, narrow_ref.at[n * 64 : n * 64 + 64], load.at[n])
        for n, w in enumerate(narrow)
    ]
    loads += [
        pltpu.make_async_copy(w, wide_ref.at[:, n * 128 : n * 128 + 128], load.at[5 + n])
        for n, w in enumerate((rec_w, forget_w))
    ]

    def columns(w, there):
        return w.at[:, pl.ds(pl.multiple_of(there * 256, 256), 256)]

    out_w = ((0, rec_out_w), (1, att_out_w))
    own_columns = [
        pltpu.make_async_copy(columns(w, tp), columns_ref.at[tp, n * 64 : n * 64 + 64], own_sem.at[n])
        for n, w in out_w
    ]
    column_copies = [
        pltpu.make_async_remote_copy(
            src_ref=columns(w, there), dst_ref=columns_ref.at[tp, n * 64 : n * 64 + 64],
            send_sem=column_send.at[n, d], recv_sem=column_recv.at[n, d],
            device_id={"tp": there}, device_id_type=MESH,
        )
        for n, w in out_w
        for d, there in enumerate(lane_peers)
    ]

    barrier = pltpu.get_barrier_semaphore()
    planes = [[(sp + 4 * d) % 64, (sp + 64 - 4 * d) % 64] for d in (1, 2, 4)]
    near = row[1:] + planes[0]
    for peer in lane_peers:
        pl.semaphore_signal(barrier, inc=1, device_id={"tp": peer}, device_id_type=MESH)
    for peer in near:
        pl.semaphore_signal(barrier, inc=1, device_id={"sp": peer}, device_id_type=MESH)
    for copy in loads + own_columns:
        copy.start()
    first_ref[...] = jnp.zeros_like(first_ref)
    second_ref[...] = jnp.zeros_like(second_ref)
    square_ref[...] = jnp.zeros_like(square_ref)
    rows = lax.broadcasted_iota(jnp.int32, (TOK, TOK), 0)
    cols = lax.broadcasted_iota(jnp.int32, (TOK, TOK), 1)
    tri_ref[...] = jnp.where(rows > cols, -1.0, 0.0).astype(BF16)
    pl.semaphore_wait(barrier, len(lane_peers) + len(near))

    def vouch(n):
        for peer in planes[n]:
            pl.semaphore_signal(near_sem.at[n], inc=1, device_id={"sp": peer}, device_id_type=MESH)

    vouch(0)

    def meanwhile():
        pl.semaphore_wait(near_sem.at[0], 2)
        vouch(1)
        for one in loads:
            one.wait()
        pl.semaphore_wait(near_sem.at[1], 2)
        vouch(2)

    def use(source, ref):
        at = pl.ds(pl.multiple_of(source * 256, 256), 256)
        values = ref[...].astype(F32)
        squares = values * values
        square_ref[...] += squares[:, 0:128] + squares[:, 128:256]
        scaled = (values * feature_gain_ref[:, at]).astype(BF16)
        first_ref[...] += dot(scaled, narrow_ref[:, at], tb=True)
        second_ref[...] += dot(scaled, wide_ref[at, :])

    ring_gather(token_ref, slots_ref, token_send, token_recv, meanwhile, use)
    inverse = lax.rsqrt(jnp.sum(square_ref[...], axis=1, keepdims=True) / D + epsilon)
    query = (first_ref[:, 256:320] * inverse).astype(BF16)
    query_ref[...] = jnp.concatenate([query[0:128], query[128:256]], axis=1)
    kv = (first_ref[:, 0:128] * inverse).astype(BF16)
    kv_ref[...] = kv
    kvs_ref[zl, y] = kv
    for n in (1, 2, 3):

        @pl.when(c >= n)
        def _():
            queries_ref[n - 1] = jnp.zeros((128, 128), BF16)

    input_ref[...] = (first_ref[:, 128:192] * inverse).astype(BF16)
    gate_ref[...] = (first_ref[:, 192:256] * inverse).astype(BF16)
    rec_ref[...] = (second_ref[:, 0:128] * inverse).astype(BF16)
    forget_ref[...] = (second_ref[:, 128:256] * inverse).astype(BF16)

    def query_copy(d):
        slot = (c + 3) % 4
        return to(query_ref, queries_ref.at[slot], query_send.at[d - 1], query_recv.at[slot], far[4 - d])

    pl.semaphore_wait(near_sem.at[2], 2)
    along_line = [
        to(kv_ref, kvs_ref.at[zl, y], line_send.at[d - 1], line_recv.at[d - 1], line[d]) for d in (1, 2, 3)
    ]
    along_row = [
        [
            to(
                kv_ref if d == 0 else kvs_ref.at[(zl - d + 4) % 4, y],
                kvs_ref.at[(zl - d + 4) % 4, y], row_send.at[d, k], row_recv.at[d, k], row[1 if k == 0 else 3],
            )
            for k in range(2)
        ]
        for d in range(4)
    ]

    def onward(d, k):
        block = kvs_ref.at[(zl - d + 4) % 4, (y + 3) % 4 if k == 0 else (y + 1) % 4, k * 128 : k * 128 + 128]
        return to(block, block, half_send.at[d, k], half_recv.at[d, k], row[1 if k == 0 else 3])

    halves = [[onward(d, k) for k in range(2)] for d in range(4)]
    for copy in along_row[0]:
        copy.start()
    for d, n in ((2, 1), (1, 2), (3, 3)):

        @pl.when(c >= d)
        def _():
            query_copy(d).start()

        along_line[n - 1].start()
    local_scan(rec_ref, forget_ref, input_ref, low_ref, spike_ref, local_ref, faded_ref, state_ref)
    rows_ref[y] = state_ref[...]
    row_states = [
        to(state_ref, rows_ref.at[y], state_send.at[0, d - 1], state_recv.at[0, d - 1], row[d])
        for d in (1, 2, 3)
    ]
    for copy in row_states:
        copy.start()

    def pass_on(d):
        for k in range(2):
            along_row[d][k].wait_recv()
            halves[d][k].start()

    def from_line(d):
        along_line[d - 1].wait_recv()
        for copy in along_row[d]:
            copy.start()

    def take(n):
        if n > 0:

            @pl.when(c < n)
            def _():
                to(
                    query_ref, queries_ref.at[n - 1], query_send.at[0], query_recv.at[n - 1], far[1]
                ).wait_recv()

        packed = query_ref[...] if n == 0 else queries_ref[n - 1]
        q_ref[n * TOK : (n + 1) * TOK, :] = unpack(packed, 0)

    def attend_plane(d, first):
        if first == (0 if d == 0 else 2 * TOK):
            for k in range(2):
                halves[d][k].wait_recv()
        attend(
            first, zl * 4 + y, (zl - d + 4) % 4, bias_ref[0] * LOG2E, q_ref, kvs_ref, tri_ref,
            acc_ref.at[d], left_ref.at[d],
        )

    pass_on(0)
    from_line(1)
    take(0)
    take(1)
    attend_plane(0, 0)
    from_line(2)
    pass_on(1)
    from_line(3)
    for copy in column_copies:
        copy.start()
    for copy in row_states:
        copy.wait_recv()
    state, total, ahead, ahead_total = chain(rows_ref, y)
    planes_ref[zl, 0:REC_VAL, :] = state
    planes_ref[zl, REC_VAL:STATE_ROWS, :] = jnp.broadcast_to(total, (8, REC_KEY))
    line_states = [
        to(planes_ref.at[zl], planes_ref.at[zl], state_send.at[1, n - 1], state_recv.at[1, n - 1], line[n])
        for n in (1, 2, 3)
    ]
    for copy in line_states:
        copy.start()
    take(2)
    take(3)
    attend_plane(0, 2 * TOK)
    pass_on(2)
    attend_plane(1, 2 * TOK)
    pass_on(3)
    for copy in line_states:
        copy.wait_recv()
    state, total, low, low_total = chain(planes_ref, zl)
    group_ref[0:REC_VAL, :] = state
    group_ref[REC_VAL:STATE_ROWS, :] = jnp.broadcast_to(total, (8, REC_KEY))
    before = low * jnp.exp(ahead_total) + ahead
    before_total = low_total + ahead_total

    def back(k, d):
        slot = (c + d + 3) % 4
        src, dst = ((group_ref, groups_ref), (far_ref, part_ref), (far_left_ref, part_left_ref))[k]
        src = src if k == 0 else src.at[slot % 3]
        return to(src, dst.at[c % 3], back_send.at[k, d - 1], back_recv.at[k, c % 3], far[d])

    def arrival(k, g):
        src, dst = ((group_ref, groups_ref), (far_ref.at[0], part_ref), (far_left_ref.at[0], part_left_ref))[k]
        return to(src, dst.at[g], back_send.at[k, 0], back_recv.at[k, g], far[1])

    for d in (1, 2, 3):

        @pl.when(c + d < 4)
        def _():
            back(0, d).start()

    attend_plane(2, 2 * TOK)
    attend_plane(3, 2 * TOK)

    def joined(at):
        n = (zl + 1) % 4
        acc, left = acc_ref[n, at, :], left_ref[n, at, :]
        for p in (2, 1, 0):
            n = (zl - p + 4) % 4
            acc = acc + acc_ref[n, at, :] * jnp.exp2(left)
            left = left + left_ref[n, at, :]
        return acc, left

    def ready(n):
        at = (n + 1) * TOK
        top, top_left = joined(slice(at, at + 128))
        low, low_left = joined(slice(at + 128, at + 256))
        far_ref[n] = pack(top, low, 1)
        far_left_ref[n, :, 0:128] = jnp.transpose(top_left)[0:1, :]
        far_left_ref[n, :, 128:256] = jnp.transpose(low_left)[0:1, :]

    ready(1)
    ready(2)
    for d in (2, 3, 1):

        @pl.when((c + d < 4) & (c + d > 1))
        def _():
            back(1, d).start()
            back(2, d).start()

    attend_plane(1, 0)

    in_ref[...] = jnp.zeros_like(in_ref)
    for g in (0, 1, 2):

        @pl.when(g < c)
        def _():
            arrival(0, g).wait_recv()
            in_ref[...] = in_ref[...] * jnp.exp(groups_ref[g, REC_VAL : REC_VAL + 1, :]) + groups_ref[
                g, 0:REC_VAL, :
            ]

    entering = in_ref[...] * jnp.exp(before_total) + before
    raw = local_ref[...] + dot(faded_ref[...], entering.astype(BF16), tb=True)
    normed = raw * lax.rsqrt(jnp.mean(raw * raw, axis=1, keepdims=True) + epsilon) * gain_ref[...]
    gate = gate_ref[...].astype(F32)
    state_heads = normed * (gate * jax.nn.sigmoid(gate))
    state_heads = jnp.concatenate([state_heads, jnp.zeros_like(state_heads)], axis=1)
    early_ref[...] = pack(state_heads[0:128], state_heads[128:256], 0)
    early_copies = [
        pltpu.make_async_remote_copy(
            src_ref=early_ref, dst_ref=early_slots_ref.at[tp], send_sem=early_send.at[d],
            recv_sem=early_recv.at[d], device_id={"tp": there}, device_id_type=MESH,
        )
        for d, there in enumerate(lane_peers)
    ]
    for copy in early_copies:
        copy.start()
    early_slots_ref[tp] = early_ref[...]

    attend_plane(2, 0)
    attend_plane(3, 0)
    ready(0)

    @pl.when(c == 0)
    def _():
        back(1, 1).start()
        back(2, 1).start()

    own_acc, own_left = joined(slice(0, TOK))
    acc_ref[0, 0:TOK, :] = own_acc
    left_ref[0, 0:TOK, :] = own_left

    for g in (2, 1, 0):

        @pl.when(g < c)
        def _():
            arrival(1, g).wait_recv()
            arrival(2, g).wait_recv()
            packed = part_ref[g].astype(F32)
            scale = jnp.exp2(left_ref[0, 0:TOK, :])
            acc_ref[0, 0:128, :] += packed * scale[0:128, :]
            acc_ref[0, 128:256, :] += pltpu.roll(packed, 64, 1) * scale[128:256, :]
            for at in (0, 128):
                left_ref[0, at : at + 128, :] += column(part_left_ref[g, 0:1, at : at + 128])

    heads_ref[...] = pack(acc_ref[0, 0:128, :], acc_ref[0, 128:256, :], 1)

    def columns_here():
        for copy in own_columns:
            copy.wait()
        for copy in column_copies + early_copies:
            copy.wait_recv()
        out_ref[...] = jnp.zeros_like(out_ref)
        for n in range(8):
            add(n, early_slots_ref.at[n], 0)

    def add(source, ref, natural=1):
        out_ref[...] += dot(unpack(ref[...], natural), columns_ref[source])

    ring_gather(heads_ref, head_slots_ref, head_send, head_recv, columns_here, add)
    sent = early_copies + along_line + row_states + line_states + column_copies
    for d in range(4):
        sent = sent + along_row[d] + halves[d]
    for copy in sent:
        copy.wait_send()
    for d in (1, 2, 3):

        @pl.when(c >= d)
        def _():
            query_copy(d).wait_send()

        @pl.when(c + d < 4)
        def _():
            for k in range(3):
                back(k, d).wait_send()


def layer(*operands):
    dma = pltpu.SemaphoreType.DMA

    def both(*shape):
        return [dma(shape), dma(shape)]

    return pl.pallas_call(
        layer_kernel,
        out_shape=jax.ShapeDtypeStruct((TOK, 256), F32),
        in_specs=[SMEM] + [VMEM] * 5 + [ANY] * 9,
        out_specs=VMEM,
        scratch_shapes=[
            pltpu.VMEM((8, TOK, 256), BF16),
            pltpu.VMEM((320, D), BF16),
            pltpu.VMEM((D, 256), BF16),
            pltpu.VMEM((TOK, 320), F32),
            pltpu.VMEM((TOK, 256), F32),
            pltpu.VMEM((TOK, 128), F32),
            pltpu.VMEM((TOK, 128), BF16),
            pltpu.VMEM((128, 128), BF16),
            pltpu.VMEM((TOK, 128), BF16),
            pltpu.VMEM((TOK, 128), BF16),
            pltpu.VMEM((TOK, 64), BF16),
            pltpu.VMEM((TOK, 64), BF16),
            pltpu.VMEM((4, 4, TOK, 128), BF16),
            pltpu.VMEM((3, 128, 128), BF16),
            pltpu.VMEM((STATE_ROWS, REC_KEY), F32),
            pltpu.VMEM((4, STATE_ROWS, REC_KEY), F32),
            pltpu.VMEM((4, STATE_ROWS, REC_KEY), F32),
            pltpu.VMEM((STATE_ROWS, REC_KEY), F32),
            pltpu.VMEM((3, STATE_ROWS, REC_KEY), F32),
            pltpu.VMEM((TOK, REC_VAL), F32),
            pltpu.VMEM((TOK, REC_KEY), BF16),
            pltpu.VMEM((4 * TOK, 128), BF16),
            pltpu.VMEM((TOK, TOK), BF16),
            pltpu.VMEM((4, 4 * TOK, 128), F32),
            pltpu.VMEM((4, 4 * TOK, 128), F32),
            pltpu.VMEM((3, 128, 128), BF16),
            pltpu.VMEM((3, 1, TOK), F32),
            pltpu.VMEM((3, 128, 128), BF16),
            pltpu.VMEM((3, 1, TOK), F32),
            pltpu.VMEM((REC_VAL, REC_KEY), F32),
            pltpu.VMEM((128, 128), BF16),
            pltpu.VMEM((8, 128, 256), BF16),
            pltpu.VMEM((8, 128, 128), BF16),
            pltpu.VMEM((128, 128), BF16),
            pltpu.VMEM((8, 128, 128), BF16),
            dma((7,)), *both(7), *both(13), *both(13),
            *both(3), *both(4, 2), *both(4, 2), *both(2, 3),
            *both(3), *both(2, 7), *both(3, 3), dma((2,)), pltpu.SemaphoreType.REGULAR((3,)),
        ],
        compiler_params=pltpu.CompilerParams(collective_id=0, has_side_effects=True),
        name="layer",
    )(*operands)


def shards(
    tokens,
    input_norm_gain,
    attention_query_weight,
    attention_key_weight,
    attention_value_weight,
    attention_score_bias,
    recurrence_query_weight,
    forget_weight,
    input_weight,
    output_gate_weight,
    forget_minimum,
    decay_spikes,
    head_norm_gain,
    attention_output_weight,
    recurrence_output_weight,
):
    narrow = (
        attention_key_weight, attention_value_weight, input_weight, output_gate_weight, attention_query_weight
    )
    return layer(
        attention_score_bias, tokens, input_norm_gain[None, :], forget_minimum,
        decay_spikes.reshape(1, TOK), head_norm_gain[None, :],
        *(w.T for w in narrow), recurrence_query_weight, forget_weight,
        recurrence_output_weight, attention_output_weight,
    ).astype(BF16)


def solution(mesh):
    placed = (
        P("sp", "tp"),
        P(),
        P(None, "tp"),
        P(None, "tp"),
        P(None, "tp"),
        P("tp"),
        P(None, "tp"),
        P(None, "tp"),
        P(None, "tp"),
        P(None, "tp"),
        P("tp", None),
        P("sp", "tp"),
        P(),
        P("tp", None),
        P("tp", None),
    )
    return jax.shard_map(
        shards, mesh=mesh, in_specs=placed, out_specs=P("sp", "tp"), check_vma=False
    )
```

```python
import functools

import jax
import jax.numpy as jnp
from jax import lax
from jax.experimental import pallas as pl
from jax.experimental.pallas import tpu as pltpu
from jax.sharding import PartitionSpec as P

D = 2048
HEAD = 64
REC_KEY = 128
REC_VAL = 64
REC_SPAN = 64
TOK = 256
LOG2E = 1.4426950408889634
STATE_ROWS = REC_VAL + 8
epsilon = 1e-06
F32, BF16 = jnp.float32, jnp.bfloat16
VMEM = pl.BlockSpec(memory_space=pltpu.VMEM)
SMEM = pl.BlockSpec(memory_space=pltpu.SMEM)
HBM = pl.BlockSpec(memory_space=pltpu.HBM)
MESH = pl.DeviceIdType.MESH


def dot(a, b, ta=False, tb=False):
    dims = (((0 if ta else 1,), (1 if tb else 0,)), ((), ()))
    return lax.dot_general(a, b, dims, preferred_element_type=F32)


def to(src, dst, send, recv, sp):
    return pltpu.make_async_remote_copy(
        src_ref=src, dst_ref=dst, send_sem=send, recv_sem=recv,
        device_id={"sp": sp}, device_id_type=MESH,
    )


def place():
    sp = lax.axis_index("sp")
    return sp, sp // 16, (sp // 4) % 4, sp % 4


def lanes():
    tp = lax.axis_index("tp")
    x, core = tp // 2, tp % 2
    return tp, tp + 1 - 2 * core, (tp + 2) % 8, (tp + 6) % 8, (tp + 4) % 8, 1 - 2 * core


def ring_gather(chunk_ref, slots_ref, send, recv, meanwhile, use, small=False):
    tp, partner, right, left, across, twist = lanes()
    half = chunk_ref.shape[0] // 2
    top, low = slice(0, half), slice(half, 2 * half)

    def copy(n, src, dst, target):
        return pltpu.make_async_remote_copy(
            src_ref=src, dst_ref=dst, send_sem=send.at[n], recv_sem=recv.at[n],
            device_id={"tp": target}, device_id_type=MESH,
        )

    def relay(n, source, part, target):
        return copy(n, slots_ref.at[source, part], slots_ref.at[source, part], target)

    copies = [
        copy(0, chunk_ref, slots_ref.at[tp], partner),
        copy(1, chunk_ref.at[top], slots_ref.at[tp, top], right),
        copy(2, chunk_ref.at[low], slots_ref.at[tp, low], left),
        copy(3, chunk_ref.at[low], slots_ref.at[tp, low], right),
        copy(4, chunk_ref.at[top], slots_ref.at[tp, top], left),
        relay(5, left, top, right),
        relay(6, right, low, left),
        relay(7, left, top, partner),
        relay(8, right, low, partner),
        relay(9, left, low, partner),
        relay(10, right, top, partner),
    ]
    if small:
        copies += [relay(11, left, top, right + twist), relay(12, right, low, left + twist)]
    else:
        copies += [relay(11, across, top, partner), relay(12, across, low, partner)]
    for n in range(5):
        copies[n].start()
    meanwhile()
    use(tp, chunk_ref)
    copies[1].wait_recv()
    copies[5].start()
    if small:
        copies[11].start()
    copies[7].start()
    copies[2].wait_recv()
    copies[6].start()
    if small:
        copies[12].start()
    copies[8].start()
    copies[0].wait_recv()
    use(partner, slots_ref.at[partner])
    copies[3].wait_recv()
    copies[9].start()
    copies[4].wait_recv()
    copies[10].start()
    use(left, slots_ref.at[left])
    use(right, slots_ref.at[right])
    copies[7].wait_recv()
    copies[9].wait_recv()
    use(left + twist, slots_ref.at[left + twist])
    copies[8].wait_recv()
    copies[10].wait_recv()
    use(right + twist, slots_ref.at[right + twist])
    copies[5].wait_recv()
    if not small:
        copies[11].start()
    copies[6].wait_recv()
    if not small:
        copies[12].start()
    use(across, slots_ref.at[across])
    copies[11].wait_recv()
    copies[12].wait_recv()
    use(across + twist, slots_ref.at[across + twist])
    for one in copies:
        one.wait_send()


def column(row):
    return jnp.transpose(jnp.broadcast_to(row, (128, 128)))


def local_scan(query_ref, forget_ref, input_ref, low_ref, spike_ref, out_ref, lift_ref, state_ref):
    span = REC_SPAN
    rows = lax.broadcasted_iota(jnp.int32, (span, span), 0)
    cols = lax.broadcasted_iota(jnp.int32, (span, span), 1)
    causal = cols <= rows
    ones = jnp.where(causal, 1.0, 0.0)
    spikes = jnp.concatenate([column(spike_ref[:, n : n + 128]) for n in (0, 128)], axis=0)
    state = jnp.zeros((REC_VAL, REC_KEY), F32)
    offset = jnp.zeros((1, REC_KEY), F32)
    for n in range(query_ref.shape[0] // span):
        at = slice(n * span, (n + 1) * span)
        query = query_ref[at, :].astype(F32)
        lifted = query * jax.nn.sigmoid(query)
        intake = (1.0 - low_ref[...]) * jax.nn.sigmoid(-forget_ref[at, :].astype(F32))
        log_forget = jnp.log1p(-intake) + spikes[at, :]
        running = lax.dot_general(
            ones, log_forget, (((1,), (0,)), ((), ())),
            precision=lax.Precision.HIGHEST, preferred_element_type=F32,
        )
        total = running[span - 1 : span, :]
        middle = running[span // 2 - 1 : span // 2, :]
        value = input_ref[at, :]
        grown = (lifted * jnp.exp(running - middle)).astype(BF16)
        shrunk = (intake * jnp.exp(middle - running)).astype(BF16)
        inner = jnp.where(causal, dot(grown, shrunk, tb=True), 0.0)
        faded = (lifted * jnp.exp(running)).astype(BF16)
        out_ref[at, :] = dot(inner.astype(BF16), value) + dot(faded, state.astype(BF16), tb=True)
        lift_ref[at, :] = (lifted * jnp.exp(running + offset)).astype(BF16)
        kept = (intake * jnp.exp(total - running)).astype(BF16)
        state = state * jnp.exp(total) + dot(value, kept, ta=True)
        offset = offset + total
    state_ref[0:REC_VAL, :] = state
    state_ref[REC_VAL:STATE_ROWS, :] = jnp.broadcast_to(offset, (8, REC_KEY))


def attend(first, here, plane, bias2, q_ref, kvs_ref, tri_ref, acc_ref, left_ref):
    at = slice(first, first + 2 * TOK)
    ahead = lax.broadcasted_iota(jnp.int32, (TOK, TOK), 1) - lax.broadcasted_iota(jnp.int32, (TOK, TOK), 0)
    q, tri = q_ref[at, :], tri_ref[...]
    acc = jnp.zeros((2 * TOK, 128), F32)
    left = jnp.zeros((2 * TOK, 1), F32)
    for n in (3, 2, 1, 0):

        def masked(x):
            if first > 0:
                return x
            keep = ahead < (here - plane * 4 - n) * TOK
            return jnp.concatenate([jnp.where(keep, x[0:TOK], 0.0), x[TOK:]], axis=0)

        kv = kvs_ref[plane, n]
        z = dot(q, kv, tb=True) * (LOG2E / 8.0) + bias2
        soft = masked(jnp.maximum(z, jnp.log(1.0 + jnp.exp2(jnp.minimum(z, 30.0))) * LOG2E))
        later = dot(soft.astype(BF16), tri)
        weight = masked(jnp.exp2((z - soft) + (later + left)))
        acc = acc + dot(weight.astype(BF16), kv)
        left = left + (later[:, 0:1] - soft[:, 0:1])
    acc_ref[at, :] = acc
    left_ref[at, :] = jnp.broadcast_to(left, (2 * TOK, 128))


def pack(top, low, natural):
    lane = lax.broadcasted_iota(jnp.int32, (128, 128), 1)
    return jnp.where((lane < HEAD) == (natural == 0), top, pltpu.roll(low, 64, 1)).astype(BF16)


def unpack(packed, natural):
    lane = lax.broadcasted_iota(jnp.int32, (128, 128), 1)
    keep = (lane < HEAD) == (natural == 0)
    packed = packed.astype(F32)
    low = pltpu.roll(packed, 64, 1)
    return jnp.concatenate([jnp.where(keep, packed, 0.0), jnp.where(keep, low, 0.0)], axis=0).astype(BF16)


def chain(states_ref, here):
    state = states_ref[0, 0:REC_VAL, :]
    total = states_ref[0, REC_VAL : REC_VAL + 1, :]
    ahead, ahead_total = jnp.zeros_like(state), jnp.zeros_like(total)
    for n in range(1, 4):
        ahead = jnp.where(n <= here, state, ahead)
        ahead_total = jnp.where(n <= here, total, ahead_total)
        more = states_ref[n, REC_VAL : REC_VAL + 1, :]
        state = state * jnp.exp(more) + states_ref[n, 0:REC_VAL, :]
        total = total + more
    return state, total, ahead, ahead_total


def layer_kernel(
    bias_ref, token_hbm, feature_gain_hbm, low_hbm, spike_hbm, gain_hbm,
    key_w, value_w, input_w, gate_w, query_w, rec_w, forget_w, rec_out_w, att_out_w,
    out_ref,
    token_ref, feature_gain_ref, low_ref, spike_ref, gain_ref,
    slots_ref, narrow_ref, wide_ref, first_ref, second_ref, square_ref,
    kv_ref, query_ref, rec_ref, forget_ref, input_ref, gate_ref,
    kvs_ref, queries_ref, state_ref, rows_ref, planes_ref, group_ref, groups_ref,
    local_ref, faded_ref, q_ref, tri_ref, acc_ref, left_ref,
    far_ref, far_left_ref, part_ref, part_left_ref, in_ref,
    heads_ref, columns_ref, head_slots_ref, early_ref, early_slots_ref,
    load, early_send, early_recv, token_send, token_recv, head_send, head_recv,
    line_send, line_recv, row_send, row_recv, half_send, half_recv, state_send, state_recv,
    query_send, query_recv, column_send, column_recv, back_send, back_recv, own_sem, near_sem,
):
    sp, c, zl, y = place()
    tp = lax.axis_index("tp")
    base = c * 16
    row = [base + zl * 4 + (y + d) % 4 for d in range(4)]
    line = [base + ((zl + d) % 4) * 4 + y for d in range(4)]
    far = [(sp + 16 * d) % 64 for d in range(4)]
    lane_peers = [(tp + d) % 8 for d in range(1, 8)]

    narrow = (key_w, value_w, input_w, gate_w, query_w)
    loads = [
        pltpu.make_async_copy(w, narrow_ref.at[n * 64 : n * 64 + 64], load.at[n])
        for n, w in enumerate(narrow)
    ]
    loads += [
        pltpu.make_async_copy(w, wide_ref.at[:, n * 128 : n * 128 + 128], load.at[5 + n])
        for n, w in enumerate((rec_w, forget_w))
    ]
    small = (
        (token_hbm, token_ref), (feature_gain_hbm, feature_gain_ref), (low_hbm, low_ref),
        (spike_hbm, spike_ref), (gain_hbm, gain_ref),
    )
    first_loads = [pltpu.make_async_copy(src, dst, load.at[7 + n]) for n, (src, dst) in enumerate(small)]

    def columns(w, there):
        return w.at[:, pl.ds(pl.multiple_of(there * 256, 256), 256)]

    out_w = ((0, rec_out_w), (1, att_out_w))
    own_columns = [
        pltpu.make_async_copy(columns(w, tp), columns_ref.at[tp, n * 64 : n * 64 + 64], own_sem.at[n])
        for n, w in out_w
    ]
    column_copies = [
        pltpu.make_async_remote_copy(
            src_ref=columns(w, there), dst_ref=columns_ref.at[tp, n * 64 : n * 64 + 64],
            send_sem=column_send.at[n, d], recv_sem=column_recv.at[n, d],
            device_id={"tp": there}, device_id_type=MESH,
        )
        for n, w in out_w
        for d, there in enumerate(lane_peers)
    ]

    barrier = pltpu.get_barrier_semaphore()
    planes = [[(sp + 4 * d) % 64, (sp + 64 - 4 * d) % 64] for d in (1, 2, 4)]
    near = row[1:] + planes[0]
    for peer in lane_peers:
        pl.semaphore_signal(barrier, inc=1, device_id={"tp": peer}, device_id_type=MESH)
    for peer in near:
        pl.semaphore_signal(barrier, inc=1, device_id={"sp": peer}, device_id_type=MESH)
    for copy in first_loads + loads + own_columns:
        copy.start()
    first_ref[...] = jnp.zeros_like(first_ref)
    second_ref[...] = jnp.zeros_like(second_ref)
    square_ref[...] = jnp.zeros_like(square_ref)
    rows = lax.broadcasted_iota(jnp.int32, (TOK, TOK), 0)
    cols = lax.broadcasted_iota(jnp.int32, (TOK, TOK), 1)
    tri_ref[...] = jnp.where(rows > cols, -1.0, 0.0).astype(BF16)
    pl.semaphore_wait(barrier, len(lane_peers) + len(near))

    def vouch(n):
        for peer in planes[n]:
            pl.semaphore_signal(near_sem.at[n], inc=1, device_id={"sp": peer}, device_id_type=MESH)

    vouch(0)
    for copy in first_loads:
        copy.wait()

    def meanwhile():
        pl.semaphore_wait(near_sem.at[0], 2)
        vouch(1)
        for one in loads:
            one.wait()
        pl.semaphore_wait(near_sem.at[1], 2)
        vouch(2)

    def use(source, ref):
        at = pl.ds(pl.multiple_of(source * 256, 256), 256)
        values = ref[...].astype(F32)
        squares = values * values
        square_ref[...] += squares[:, 0:128] + squares[:, 128:256]
        scaled = (values * feature_gain_ref[:, at]).astype(BF16)
        first_ref[...] += dot(scaled, narrow_ref[:, at], tb=True)
        second_ref[...] += dot(scaled, wide_ref[at, :])

    ring_gather(token_ref, slots_ref, token_send, token_recv, meanwhile, use)
    inverse = lax.rsqrt(jnp.sum(square_ref[...], axis=1, keepdims=True) / D + epsilon)
    query = (first_ref[:, 256:320] * inverse).astype(BF16)
    query_ref[...] = jnp.concatenate([query[0:128], query[128:256]], axis=1)
    kv = (first_ref[:, 0:128] * inverse).astype(BF16)
    kv_ref[...] = kv
    kvs_ref[zl, y] = kv
    for n in (1, 2, 3):

        @pl.when(c >= n)
        def _():
            queries_ref[n - 1] = jnp.zeros((128, 128), BF16)

    input_ref[...] = (first_ref[:, 128:192] * inverse).astype(BF16)
    gate_ref[...] = (first_ref[:, 192:256] * inverse).astype(BF16)
    rec_ref[...] = (second_ref[:, 0:128] * inverse).astype(BF16)
    forget_ref[...] = (second_ref[:, 128:256] * inverse).astype(BF16)

    def query_copy(d):
        slot = (c + 3) % 4
        return to(query_ref, queries_ref.at[slot], query_send.at[d - 1], query_recv.at[slot], far[4 - d])

    pl.semaphore_wait(near_sem.at[2], 2)
    along_line = [
        to(kv_ref, kvs_ref.at[zl, y], line_send.at[d - 1], line_recv.at[d - 1], line[d]) for d in (1, 2, 3)
    ]
    along_row = [
        [
            to(
                kv_ref if d == 0 else kvs_ref.at[(zl - d + 4) % 4, y],
                kvs_ref.at[(zl - d + 4) % 4, y], row_send.at[d, k], row_recv.at[d, k], row[1 if k == 0 else 3],
            )
            for k in range(2)
        ]
        for d in range(4)
    ]

    def onward(d, k):
        block = kvs_ref.at[(zl - d + 4) % 4, (y + 3) % 4 if k == 0 else (y + 1) % 4, k * 128 : k * 128 + 128]
        return to(block, block, half_send.at[d, k], half_recv.at[d, k], row[1 if k == 0 else 3])

    halves = [[onward(d, k) for k in range(2)] for d in range(4)]
    for copy in along_row[0]:
        copy.start()
    for d, n in ((2, 1), (1, 2), (3, 3)):

        @pl.when(c >= d)
        def _():
            query_copy(d).start()

        along_line[n - 1].start()
    local_scan(rec_ref, forget_ref, input_ref, low_ref, spike_ref, local_ref, faded_ref, state_ref)
    rows_ref[y] = state_ref[...]
    row_states = [
        to(state_ref, rows_ref.at[y], state_send.at[0, d - 1], state_recv.at[0, d - 1], row[d])
        for d in (1, 2, 3)
    ]
    for copy in row_states:
        copy.start()

    def pass_on(d):
        for k in range(2):
            along_row[d][k].wait_recv()
            halves[d][k].start()

    def from_line(d):
        along_line[d - 1].wait_recv()
        for copy in along_row[d]:
            copy.start()

    def take(n):
        if n > 0:

            @pl.when(c < n)
            def _():
                to(
                    query_ref, queries_ref.at[n - 1], query_send.at[0], query_recv.at[n - 1], far[1]
                ).wait_recv()

        packed = query_ref[...] if n == 0 else queries_ref[n - 1]
        q_ref[n * TOK : (n + 1) * TOK, :] = unpack(packed, 0)

    def attend_plane(d, first):
        if first == (0 if d == 0 else 2 * TOK):
            for k in range(2):
                halves[d][k].wait_recv()
        attend(
            first, zl * 4 + y, (zl - d + 4) % 4, bias_ref[0] * LOG2E, q_ref, kvs_ref, tri_ref,
            acc_ref.at[d], left_ref.at[d],
        )

    pass_on(0)
    from_line(1)
    take(0)
    take(1)
    attend_plane(0, 0)
    from_line(2)
    pass_on(1)
    from_line(3)
    for copy in column_copies:
        copy.start()
    for copy in row_states:
        copy.wait_recv()
    state, total, ahead, ahead_total = chain(rows_ref, y)
    planes_ref[zl, 0:REC_VAL, :] = state
    planes_ref[zl, REC_VAL:STATE_ROWS, :] = jnp.broadcast_to(total, (8, REC_KEY))
    line_states = [
        to(planes_ref.at[zl], planes_ref.at[zl], state_send.at[1, n - 1], state_recv.at[1, n - 1], line[n])
        for n in (1, 2, 3)
    ]
    for copy in line_states:
        copy.start()
    take(2)
    take(3)
    attend_plane(0, 2 * TOK)
    pass_on(2)
    attend_plane(1, 2 * TOK)
    pass_on(3)
    for copy in line_states:
        copy.wait_recv()
    state, total, low, low_total = chain(planes_ref, zl)
    group_ref[0:REC_VAL, :] = state
    group_ref[REC_VAL:STATE_ROWS, :] = jnp.broadcast_to(total, (8, REC_KEY))
    before = low * jnp.exp(ahead_total) + ahead
    before_total = low_total + ahead_total

    def back(k, d):
        slot = (c + d + 3) % 4
        src, dst = ((group_ref, groups_ref), (far_ref, part_ref), (far_left_ref, part_left_ref))[k]
        src = src if k == 0 else src.at[slot % 3]
        return to(src, dst.at[c % 3], back_send.at[k, d - 1], back_recv.at[k, c % 3], far[d])

    def arrival(k, g):
        src, dst = ((group_ref, groups_ref), (far_ref.at[0], part_ref), (far_left_ref.at[0], part_left_ref))[k]
        return to(src, dst.at[g], back_send.at[k, 0], back_recv.at[k, g], far[1])

    for d in (1, 2, 3):

        @pl.when(c + d < 4)
        def _():
            back(0, d).start()

    attend_plane(2, 2 * TOK)
    attend_plane(3, 2 * TOK)

    def joined(at):
        n = (zl + 1) % 4
        acc, left = acc_ref[n, at, :], left_ref[n, at, :]
        for p in (2, 1, 0):
            n = (zl - p + 4) % 4
            acc = acc + acc_ref[n, at, :] * jnp.exp2(left)
            left = left + left_ref[n, at, :]
        return acc, left

    def ready(n):
        at = (n + 1) * TOK
        top, top_left = joined(slice(at, at + 128))
        low, low_left = joined(slice(at + 128, at + 256))
        far_ref[n] = pack(top, low, 1)
        far_left_ref[n, :, 0:128] = jnp.transpose(top_left)[0:1, :]
        far_left_ref[n, :, 128:256] = jnp.transpose(low_left)[0:1, :]

    ready(1)
    ready(2)
    for d in (2, 3, 1):

        @pl.when((c + d < 4) & (c + d > 1))
        def _():
            back(1, d).start()
            back(2, d).start()

    attend_plane(1, 0)

    in_ref[...] = jnp.zeros_like(in_ref)
    for g in (0, 1, 2):

        @pl.when(g < c)
        def _():
            arrival(0, g).wait_recv()
            in_ref[...] = in_ref[...] * jnp.exp(groups_ref[g, REC_VAL : REC_VAL + 1, :]) + groups_ref[
                g, 0:REC_VAL, :
            ]

    entering = in_ref[...] * jnp.exp(before_total) + before
    raw = local_ref[...] + dot(faded_ref[...], entering.astype(BF16), tb=True)
    normed = raw * lax.rsqrt(jnp.mean(raw * raw, axis=1, keepdims=True) + epsilon) * gain_ref[...]
    gate = gate_ref[...].astype(F32)
    state_heads = normed * (gate * jax.nn.sigmoid(gate))
    state_heads = jnp.concatenate([state_heads, jnp.zeros_like(state_heads)], axis=1)
    early_ref[...] = pack(state_heads[0:128], state_heads[128:256], 0)
    early_copies = [
        pltpu.make_async_remote_copy(
            src_ref=early_ref, dst_ref=early_slots_ref.at[tp], send_sem=early_send.at[d],
            recv_sem=early_recv.at[d], device_id={"tp": there}, device_id_type=MESH,
        )
        for d, there in enumerate(lane_peers)
    ]
    for copy in early_copies:
        copy.start()
    early_slots_ref[tp] = early_ref[...]

    attend_plane(2, 0)
    attend_plane(3, 0)
    ready(0)

    @pl.when(c == 0)
    def _():
        back(1, 1).start()
        back(2, 1).start()

    own_acc, own_left = joined(slice(0, TOK))
    acc_ref[0, 0:TOK, :] = own_acc
    left_ref[0, 0:TOK, :] = own_left

    for g in (2, 1, 0):

        @pl.when(g < c)
        def _():
            arrival(1, g).wait_recv()
            arrival(2, g).wait_recv()
            packed = part_ref[g].astype(F32)
            scale = jnp.exp2(left_ref[0, 0:TOK, :])
            acc_ref[0, 0:128, :] += packed * scale[0:128, :]
            acc_ref[0, 128:256, :] += pltpu.roll(packed, 64, 1) * scale[128:256, :]
            for at in (0, 128):
                left_ref[0, at : at + 128, :] += column(part_left_ref[g, 0:1, at : at + 128])

    heads_ref[...] = pack(acc_ref[0, 0:128, :], acc_ref[0, 128:256, :], 1)

    def columns_here():
        for copy in own_columns:
            copy.wait()
        for copy in column_copies + early_copies:
            copy.wait_recv()
        out_ref[...] = jnp.zeros_like(out_ref)
        for n in range(8):
            add(n, early_slots_ref.at[n], 0)

    def add(source, ref, natural=1):
        out_ref[...] += dot(unpack(ref[...], natural), columns_ref[source])

    ring_gather(heads_ref, head_slots_ref, head_send, head_recv, columns_here, add, small=True)
    sent = early_copies + along_line + row_states + line_states + column_copies
    for d in range(4):
        sent = sent + along_row[d] + halves[d]
    for copy in sent:
        copy.wait_send()
    for d in (1, 2, 3):

        @pl.when(c >= d)
        def _():
            query_copy(d).wait_send()

        @pl.when(c + d < 4)
        def _():
            for k in range(3):
                back(k, d).wait_send()


def layer(*operands):
    dma = pltpu.SemaphoreType.DMA

    def both(*shape):
        return [dma(shape), dma(shape)]

    return pl.pallas_call(
        layer_kernel,
        out_shape=jax.ShapeDtypeStruct((TOK, 256), F32),
        in_specs=[SMEM] + [HBM] * 14,
        out_specs=VMEM,
        scratch_shapes=[
            pltpu.VMEM((TOK, 256), BF16),
            pltpu.VMEM((1, D), F32),
            pltpu.VMEM((1, REC_KEY), F32),
            pltpu.VMEM((1, TOK), F32),
            pltpu.VMEM((1, REC_VAL), F32),
            pltpu.VMEM((8, TOK, 256), BF16),
            pltpu.VMEM((320, D), BF16),
            pltpu.VMEM((D, 256), BF16),
            pltpu.VMEM((TOK, 320), F32),
            pltpu.VMEM((TOK, 256), F32),
            pltpu.VMEM((TOK, 128), F32),
            pltpu.VMEM((TOK, 128), BF16),
            pltpu.VMEM((128, 128), BF16),
            pltpu.VMEM((TOK, 128), BF16),
            pltpu.VMEM((TOK, 128), BF16),
            pltpu.VMEM((TOK, 64), BF16),
            pltpu.VMEM((TOK, 64), BF16),
            pltpu.VMEM((4, 4, TOK, 128), BF16),
            pltpu.VMEM((3, 128, 128), BF16),
            pltpu.VMEM((STATE_ROWS, REC_KEY), F32),
            pltpu.VMEM((4, STATE_ROWS, REC_KEY), F32),
            pltpu.VMEM((4, STATE_ROWS, REC_KEY), F32),
            pltpu.VMEM((STATE_ROWS, REC_KEY), F32),
            pltpu.VMEM((3, STATE_ROWS, REC_KEY), F32),
            pltpu.VMEM((TOK, REC_VAL), F32),
            pltpu.VMEM((TOK, REC_KEY), BF16),
            pltpu.VMEM((4 * TOK, 128), BF16),
            pltpu.VMEM((TOK, TOK), BF16),
            pltpu.VMEM((4, 4 * TOK, 128), F32),
            pltpu.VMEM((4, 4 * TOK, 128), F32),
            pltpu.VMEM((3, 128, 128), BF16),
            pltpu.VMEM((3, 1, TOK), F32),
            pltpu.VMEM((3, 128, 128), BF16),
            pltpu.VMEM((3, 1, TOK), F32),
            pltpu.VMEM((REC_VAL, REC_KEY), F32),
            pltpu.VMEM((128, 128), BF16),
            pltpu.VMEM((8, 128, 256), BF16),
            pltpu.VMEM((8, 128, 128), BF16),
            pltpu.VMEM((128, 128), BF16),
            pltpu.VMEM((8, 128, 128), BF16),
            dma((12,)), *both(7), *both(13), *both(13),
            *both(3), *both(4, 2), *both(4, 2), *both(2, 3),
            *both(3), *both(2, 7), *both(3, 3), dma((2,)), pltpu.SemaphoreType.REGULAR((3,)),
        ],
        compiler_params=pltpu.CompilerParams(collective_id=0, has_side_effects=True),
        name="layer",
    )(*operands)


def shards(
    tokens,
    input_norm_gain,
    attention_query_weight,
    attention_key_weight,
    attention_value_weight,
    attention_score_bias,
    recurrence_query_weight,
    forget_weight,
    input_weight,
    output_gate_weight,
    forget_minimum,
    decay_spikes,
    head_norm_gain,
    attention_output_weight,
    recurrence_output_weight,
):
    narrow = (
        attention_key_weight, attention_value_weight, input_weight, output_gate_weight, attention_query_weight
    )
    return layer(
        attention_score_bias, tokens, input_norm_gain[None, :], forget_minimum,
        decay_spikes.reshape(1, TOK), head_norm_gain[None, :],
        *(w.T for w in narrow), recurrence_query_weight, forget_weight,
        recurrence_output_weight, attention_output_weight,
    ).astype(BF16)


def solution(mesh):
    placed = (
        P("sp", "tp"),
        P(),
        P(None, "tp"),
        P(None, "tp"),
        P(None, "tp"),
        P("tp"),
        P(None, "tp"),
        P(None, "tp"),
        P(None, "tp"),
        P(None, "tp"),
        P("tp", None),
        P("sp", "tp"),
        P(),
        P("tp", None),
        P("tp", None),
    )
    return jax.shard_map(
        shards, mesh=mesh, in_specs=placed, out_specs=P("sp", "tp"), check_vma=False
    )
```

```python
import functools

import jax
import jax.numpy as jnp
from jax import lax
from jax.experimental import pallas as pl
from jax.experimental.pallas import tpu as pltpu
from jax.sharding import PartitionSpec as P

D = 2048
HEAD = 64
REC_KEY = 128
REC_VAL = 64
REC_SPAN = 64
TOK = 256
LOG2E = 1.4426950408889634
STATE_ROWS = REC_VAL + 8
epsilon = 1e-06
F32, BF16 = jnp.float32, jnp.bfloat16
VMEM = pl.BlockSpec(memory_space=pltpu.VMEM)
SMEM = pl.BlockSpec(memory_space=pltpu.SMEM)
HBM = pl.BlockSpec(memory_space=pltpu.HBM)
MESH = pl.DeviceIdType.MESH


def dot(a, b, ta=False, tb=False):
    dims = (((0 if ta else 1,), (1 if tb else 0,)), ((), ()))
    return lax.dot_general(a, b, dims, preferred_element_type=F32)


def to(src, dst, send, recv, sp):
    return pltpu.make_async_remote_copy(
        src_ref=src, dst_ref=dst, send_sem=send, recv_sem=recv,
        device_id={"sp": sp}, device_id_type=MESH,
    )


def place():
    sp = lax.axis_index("sp")
    return sp, sp // 16, (sp // 4) % 4, sp % 4


def lanes():
    tp = lax.axis_index("tp")
    x, core = tp // 2, tp % 2
    return tp, tp + 1 - 2 * core, (tp + 2) % 8, (tp + 6) % 8, (tp + 4) % 8, 1 - 2 * core


def ring_gather(chunk_ref, slots_ref, send, recv, meanwhile, use, small=False):
    tp, partner, right, left, across, twist = lanes()
    half = chunk_ref.shape[0] // 2
    top, low = slice(0, half), slice(half, 2 * half)

    def copy(n, src, dst, target):
        return pltpu.make_async_remote_copy(
            src_ref=src, dst_ref=dst, send_sem=send.at[n], recv_sem=recv.at[n],
            device_id={"tp": target}, device_id_type=MESH,
        )

    def relay(n, source, part, target):
        return copy(n, slots_ref.at[source, part], slots_ref.at[source, part], target)

    copies = [
        copy(0, chunk_ref, slots_ref.at[tp], partner),
        copy(1, chunk_ref.at[top], slots_ref.at[tp, top], right),
        copy(2, chunk_ref.at[low], slots_ref.at[tp, low], left),
        copy(3, chunk_ref.at[low], slots_ref.at[tp, low], right),
        copy(4, chunk_ref.at[top], slots_ref.at[tp, top], left),
        relay(5, left, top, right),
        relay(6, right, low, left),
        relay(7, left, top, partner),
        relay(8, right, low, partner),
        relay(9, left, low, partner),
        relay(10, right, top, partner),
    ]
    if small:
        copies += [relay(11, left, top, right + twist), relay(12, right, low, left + twist)]
    else:
        copies += [relay(11, across, top, partner), relay(12, across, low, partner)]
    for n in range(5):
        copies[n].start()
    meanwhile()
    use(tp, chunk_ref)
    copies[1].wait_recv()
    copies[5].start()
    if small:
        copies[11].start()
    copies[7].start()
    copies[2].wait_recv()
    copies[6].start()
    if small:
        copies[12].start()
    copies[8].start()
    copies[0].wait_recv()
    use(partner, slots_ref.at[partner])
    copies[3].wait_recv()
    copies[9].start()
    copies[4].wait_recv()
    copies[10].start()
    use(left, slots_ref.at[left])
    use(right, slots_ref.at[right])
    copies[7].wait_recv()
    copies[9].wait_recv()
    use(left + twist, slots_ref.at[left + twist])
    copies[8].wait_recv()
    copies[10].wait_recv()
    use(right + twist, slots_ref.at[right + twist])
    copies[5].wait_recv()
    if not small:
        copies[11].start()
    copies[6].wait_recv()
    if not small:
        copies[12].start()
    use(across, slots_ref.at[across])
    copies[11].wait_recv()
    copies[12].wait_recv()
    use(across + twist, slots_ref.at[across + twist])
    for one in copies:
        one.wait_send()


def column(row):
    return jnp.transpose(jnp.broadcast_to(row, (128, 128)))


def local_scan(query_ref, forget_ref, input_ref, low_ref, spike_ref, out_ref, lift_ref, state_ref):
    span = REC_SPAN
    rows = lax.broadcasted_iota(jnp.int32, (span, span), 0)
    cols = lax.broadcasted_iota(jnp.int32, (span, span), 1)
    causal = cols <= rows
    ones = jnp.where(causal, 1.0, 0.0)
    spikes = jnp.concatenate([column(spike_ref[:, n : n + 128]) for n in (0, 128)], axis=0)
    state = jnp.zeros((REC_VAL, REC_KEY), F32)
    offset = jnp.zeros((1, REC_KEY), F32)
    for n in range(query_ref.shape[0] // span):
        at = slice(n * span, (n + 1) * span)
        query = query_ref[at, :].astype(F32)
        lifted = query * jax.nn.sigmoid(query)
        intake = (1.0 - low_ref[...]) * jax.nn.sigmoid(-forget_ref[at, :].astype(F32))
        log_forget = jnp.log1p(-intake) + spikes[at, :]
        running = lax.dot_general(
            ones, log_forget, (((1,), (0,)), ((), ())),
            precision=lax.Precision.HIGHEST, preferred_element_type=F32,
        )
        total = running[span - 1 : span, :]
        middle = running[span // 2 - 1 : span // 2, :]
        value = input_ref[at, :]
        grown = (lifted * jnp.exp(running - middle)).astype(BF16)
        shrunk = (intake * jnp.exp(middle - running)).astype(BF16)
        inner = jnp.where(causal, dot(grown, shrunk, tb=True), 0.0)
        faded = (lifted * jnp.exp(running)).astype(BF16)
        out_ref[at, :] = dot(inner.astype(BF16), value) + dot(faded, state.astype(BF16), tb=True)
        lift_ref[at, :] = (lifted * jnp.exp(running + offset)).astype(BF16)
        kept = (intake * jnp.exp(total - running)).astype(BF16)
        state = state * jnp.exp(total) + dot(value, kept, ta=True)
        offset = offset + total
    state_ref[0:REC_VAL, :] = state
    state_ref[REC_VAL:STATE_ROWS, :] = jnp.broadcast_to(offset, (8, REC_KEY))


def attend(first, here, plane, bias2, q_ref, kvs_ref, tri_ref, acc_ref, left_ref):
    at = slice(first, first + 2 * TOK)
    ahead = lax.broadcasted_iota(jnp.int32, (TOK, TOK), 1) - lax.broadcasted_iota(jnp.int32, (TOK, TOK), 0)
    q, tri = q_ref[at, :], tri_ref[...]
    acc = jnp.zeros((2 * TOK, 128), F32)
    left = jnp.zeros((2 * TOK, 1), F32)
    for n in (3, 2, 1, 0):

        def masked(x):
            if first > 0:
                return x
            keep = ahead < (here - plane * 4 - n) * TOK
            return jnp.concatenate([jnp.where(keep, x[0:TOK], 0.0), x[TOK:]], axis=0)

        kv = kvs_ref[plane, n]
        z = dot(q, kv, tb=True) * (LOG2E / 8.0) + bias2
        soft = masked(jnp.maximum(z, jnp.log(1.0 + jnp.exp2(jnp.minimum(z, 30.0))) * LOG2E))
        later = dot(soft.astype(BF16), tri)
        weight = masked(jnp.exp2((z - soft) + (later + left)))
        acc = acc + dot(weight.astype(BF16), kv)
        left = left + (later[:, 0:1] - soft[:, 0:1])
    acc_ref[at, :] = acc
    left_ref[at, :] = jnp.broadcast_to(left, (2 * TOK, 128))


def pack(top, low, natural):
    lane = lax.broadcasted_iota(jnp.int32, (128, 128), 1)
    return jnp.where((lane < HEAD) == (natural == 0), top, pltpu.roll(low, 64, 1)).astype(BF16)


def unpack(packed, natural):
    lane = lax.broadcasted_iota(jnp.int32, (128, 128), 1)
    keep = (lane < HEAD) == (natural == 0)
    packed = packed.astype(F32)
    low = pltpu.roll(packed, 64, 1)
    return jnp.concatenate([jnp.where(keep, packed, 0.0), jnp.where(keep, low, 0.0)], axis=0).astype(BF16)


def chain(states_ref, here):
    state = states_ref[0, 0:REC_VAL, :]
    total = states_ref[0, REC_VAL : REC_VAL + 1, :]
    ahead, ahead_total = jnp.zeros_like(state), jnp.zeros_like(total)
    for n in range(1, 4):
        ahead = jnp.where(n <= here, state, ahead)
        ahead_total = jnp.where(n <= here, total, ahead_total)
        more = states_ref[n, REC_VAL : REC_VAL + 1, :]
        state = state * jnp.exp(more) + states_ref[n, 0:REC_VAL, :]
        total = total + more
    return state, total, ahead, ahead_total


def layer_kernel(
    bias_ref, token_hbm, feature_gain_hbm, low_hbm, spike_hbm, gain_hbm,
    key_w, value_w, input_w, gate_w, query_w, rec_w, forget_w, rec_out_w, att_out_w,
    out_ref,
    token_ref, feature_gain_ref, low_ref, spike_ref, gain_ref,
    slots_ref, narrow_ref, wide_ref, first_ref, second_ref, square_ref,
    kv_ref, query_ref, rec_ref, forget_ref, input_ref, gate_ref,
    kvs_ref, queries_ref, state_ref, rows_ref, planes_ref, group_ref, groups_ref,
    local_ref, faded_ref, q_ref, tri_ref, acc_ref, left_ref,
    far_ref, far_left_ref, part_ref, part_left_ref, in_ref,
    heads_ref, columns_ref, head_slots_ref, early_ref, early_slots_ref,
    load, early_send, early_recv, token_send, token_recv, head_send, head_recv,
    line_send, line_recv, row_send, row_recv, half_send, half_recv, state_send, state_recv,
    query_send, query_recv, column_send, column_recv, back_send, back_recv, own_sem, near_sem,
):
    sp, c, zl, y = place()
    tp = lax.axis_index("tp")
    base = c * 16
    row = [base + zl * 4 + (y + d) % 4 for d in range(4)]
    line = [base + ((zl + d) % 4) * 4 + y for d in range(4)]
    far = [(sp + 16 * d) % 64 for d in range(4)]
    lane_peers = [(tp + d) % 8 for d in range(1, 8)]

    narrow = (key_w, value_w, input_w, gate_w, query_w)
    loads = [
        pltpu.make_async_copy(w, narrow_ref.at[n * 64 : n * 64 + 64], load.at[n])
        for n, w in enumerate(narrow)
    ]
    loads += [
        pltpu.make_async_copy(w, wide_ref.at[:, n * 128 : n * 128 + 128], load.at[5 + n])
        for n, w in enumerate((rec_w, forget_w))
    ]
    small = (
        (token_hbm, token_ref), (feature_gain_hbm, feature_gain_ref), (low_hbm, low_ref),
        (spike_hbm, spike_ref), (gain_hbm, gain_ref),
    )
    first_loads = [pltpu.make_async_copy(src, dst, load.at[7 + n]) for n, (src, dst) in enumerate(small)]

    def columns(w, there):
        return w.at[:, pl.ds(pl.multiple_of(there * 256, 256), 256)]

    out_w = ((0, rec_out_w), (1, att_out_w))
    own_columns = [
        pltpu.make_async_copy(columns(w, tp), columns_ref.at[tp, n * 64 : n * 64 + 64], own_sem.at[n])
        for n, w in out_w
    ]
    column_copies = [
        pltpu.make_async_remote_copy(
            src_ref=columns(w, there), dst_ref=columns_ref.at[tp, n * 64 : n * 64 + 64],
            send_sem=column_send.at[n, d], recv_sem=column_recv.at[n, d],
            device_id={"tp": there}, device_id_type=MESH,
        )
        for n, w in out_w
        for d, there in enumerate(lane_peers)
    ]

    barrier = pltpu.get_barrier_semaphore()
    planes = [[(sp + 4 * d) % 64, (sp + 64 - 4 * d) % 64] for d in (1, 2, 4)]
    near = row[1:] + planes[0]
    for peer in lane_peers:
        pl.semaphore_signal(barrier, inc=1, device_id={"tp": peer}, device_id_type=MESH)
    for peer in near:
        pl.semaphore_signal(barrier, inc=1, device_id={"sp": peer}, device_id_type=MESH)
    for copy in first_loads + loads + own_columns:
        copy.start()
    first_ref[...] = jnp.zeros_like(first_ref)
    second_ref[...] = jnp.zeros_like(second_ref)
    square_ref[...] = jnp.zeros_like(square_ref)
    rows = lax.broadcasted_iota(jnp.int32, (TOK, TOK), 0)
    cols = lax.broadcasted_iota(jnp.int32, (TOK, TOK), 1)
    tri_ref[...] = jnp.where(rows > cols, -1.0, 0.0).astype(BF16)
    pl.semaphore_wait(barrier, len(lane_peers) + len(near))

    def vouch(n):
        for peer in planes[n]:
            pl.semaphore_signal(near_sem.at[n], inc=1, device_id={"sp": peer}, device_id_type=MESH)

    vouch(0)
    for copy in first_loads:
        copy.wait()

    def meanwhile():
        pl.semaphore_wait(near_sem.at[0], 2)
        vouch(1)
        for one in loads:
            one.wait()
        pl.semaphore_wait(near_sem.at[1], 2)
        vouch(2)

    def use(source, ref):
        at = pl.ds(pl.multiple_of(source * 256, 256), 256)
        values = ref[...].astype(F32)
        squares = values * values
        square_ref[...] += squares[:, 0:128] + squares[:, 128:256]
        scaled = (values * feature_gain_ref[:, at]).astype(BF16)
        first_ref[...] += dot(scaled, narrow_ref[:, at], tb=True)
        second_ref[...] += dot(scaled, wide_ref[at, :])

    ring_gather(token_ref, slots_ref, token_send, token_recv, meanwhile, use)
    inverse = lax.rsqrt(jnp.sum(square_ref[...], axis=1, keepdims=True) / D + epsilon)
    query = (first_ref[:, 256:320] * inverse).astype(BF16)
    query_ref[...] = jnp.concatenate([query[0:128], query[128:256]], axis=1)
    kv = (first_ref[:, 0:128] * inverse).astype(BF16)
    kv_ref[...] = kv
    kvs_ref[zl, y] = kv
    for n in (1, 2, 3):

        @pl.when(c >= n)
        def _():
            queries_ref[n - 1] = jnp.zeros((128, 128), BF16)


    def query_copy(d):
        slot = (c + 3) % 4
        return to(query_ref, queries_ref.at[slot], query_send.at[d - 1], query_recv.at[slot], far[4 - d])

    pl.semaphore_wait(near_sem.at[2], 2)
    along_line = [
        to(kv_ref, kvs_ref.at[zl, y], line_send.at[d - 1], line_recv.at[d - 1], line[d]) for d in (1, 2, 3)
    ]
    along_row = [
        [
            to(
                kv_ref if d == 0 else kvs_ref.at[(zl - d + 4) % 4, y],
                kvs_ref.at[(zl - d + 4) % 4, y], row_send.at[d, k], row_recv.at[d, k], row[1 if k == 0 else 3],
            )
            for k in range(2)
        ]
        for d in range(4)
    ]

    def onward(d, k):
        block = kvs_ref.at[(zl - d + 4) % 4, (y + 3) % 4 if k == 0 else (y + 1) % 4, k * 128 : k * 128 + 128]
        return to(block, block, half_send.at[d, k], half_recv.at[d, k], row[1 if k == 0 else 3])

    halves = [[onward(d, k) for k in range(2)] for d in range(4)]
    for copy in along_row[0]:
        copy.start()
    for d, n in ((2, 1), (1, 2), (3, 3)):

        @pl.when(c >= d)
        def _():
            query_copy(d).start()

        along_line[n - 1].start()
    input_ref[...] = (first_ref[:, 128:192] * inverse).astype(BF16)
    gate_ref[...] = (first_ref[:, 192:256] * inverse).astype(BF16)
    rec_ref[...] = (second_ref[:, 0:128] * inverse).astype(BF16)
    forget_ref[...] = (second_ref[:, 128:256] * inverse).astype(BF16)
    local_scan(rec_ref, forget_ref, input_ref, low_ref, spike_ref, local_ref, faded_ref, state_ref)
    rows_ref[y] = state_ref[...]
    row_states = [
        to(state_ref, rows_ref.at[y], state_send.at[0, d - 1], state_recv.at[0, d - 1], row[d])
        for d in (1, 2, 3)
    ]
    for copy in row_states:
        copy.start()

    def pass_on(d):
        for k in range(2):
            along_row[d][k].wait_recv()
            halves[d][k].start()

    def from_line(d):
        along_line[d - 1].wait_recv()
        for copy in along_row[d]:
            copy.start()

    def take(n):
        if n > 0:

            @pl.when(c < n)
            def _():
                to(
                    query_ref, queries_ref.at[n - 1], query_send.at[0], query_recv.at[n - 1], far[1]
                ).wait_recv()

        packed = query_ref[...] if n == 0 else queries_ref[n - 1]
        q_ref[n * TOK : (n + 1) * TOK, :] = unpack(packed, 0)

    def attend_plane(d, first):
        if first == (0 if d == 0 else 2 * TOK):
            for k in range(2):
                halves[d][k].wait_recv()
        attend(
            first, zl * 4 + y, (zl - d + 4) % 4, bias_ref[0] * LOG2E, q_ref, kvs_ref, tri_ref,
            acc_ref.at[d], left_ref.at[d],
        )

    pass_on(0)
    from_line(1)
    take(0)
    take(1)
    attend_plane(0, 0)
    from_line(2)
    pass_on(1)
    from_line(3)
    for copy in column_copies:
        copy.start()
    for copy in row_states:
        copy.wait_recv()
    state, total, ahead, ahead_total = chain(rows_ref, y)
    planes_ref[zl, 0:REC_VAL, :] = state
    planes_ref[zl, REC_VAL:STATE_ROWS, :] = jnp.broadcast_to(total, (8, REC_KEY))
    line_states = [
        to(planes_ref.at[zl], planes_ref.at[zl], state_send.at[1, n - 1], state_recv.at[1, n - 1], line[n])
        for n in (1, 2, 3)
    ]
    for copy in line_states:
        copy.start()
    pass_on(2)
    take(2)
    take(3)
    attend_plane(0, 2 * TOK)
    attend_plane(1, 2 * TOK)
    pass_on(3)
    for copy in line_states:
        copy.wait_recv()
    state, total, low, low_total = chain(planes_ref, zl)
    group_ref[0:REC_VAL, :] = state
    group_ref[REC_VAL:STATE_ROWS, :] = jnp.broadcast_to(total, (8, REC_KEY))
    before = low * jnp.exp(ahead_total) + ahead
    before_total = low_total + ahead_total

    def back(k, d):
        slot = (c + d + 3) % 4
        src, dst = ((group_ref, groups_ref), (far_ref, part_ref), (far_left_ref, part_left_ref))[k]
        src = src if k == 0 else src.at[slot % 3]
        return to(src, dst.at[c % 3], back_send.at[k, d - 1], back_recv.at[k, c % 3], far[d])

    def arrival(k, g):
        src, dst = ((group_ref, groups_ref), (far_ref.at[0], part_ref), (far_left_ref.at[0], part_left_ref))[k]
        return to(src, dst.at[g], back_send.at[k, 0], back_recv.at[k, g], far[1])

    for d in (1, 2, 3):

        @pl.when(c + d < 4)
        def _():
            back(0, d).start()

    attend_plane(2, 2 * TOK)
    attend_plane(3, 2 * TOK)

    def joined(at):
        n = (zl + 1) % 4
        acc, left = acc_ref[n, at, :], left_ref[n, at, :]
        for p in (2, 1, 0):
            n = (zl - p + 4) % 4
            acc = acc + acc_ref[n, at, :] * jnp.exp2(left)
            left = left + left_ref[n, at, :]
        return acc, left

    def ready(n):
        at = (n + 1) * TOK
        top, top_left = joined(slice(at, at + 128))
        low, low_left = joined(slice(at + 128, at + 256))
        far_ref[n] = pack(top, low, 1)
        far_left_ref[n, :, 0:128] = jnp.transpose(top_left)[0:1, :]
        far_left_ref[n, :, 128:256] = jnp.transpose(low_left)[0:1, :]

    ready(1)
    ready(2)
    for d in (2, 3, 1):

        @pl.when((c + d < 4) & (c + d > 1))
        def _():
            back(1, d).start()
            back(2, d).start()

    attend_plane(1, 0)

    in_ref[...] = jnp.zeros_like(in_ref)
    for g in (0, 1, 2):

        @pl.when(g < c)
        def _():
            arrival(0, g).wait_recv()
            in_ref[...] = in_ref[...] * jnp.exp(groups_ref[g, REC_VAL : REC_VAL + 1, :]) + groups_ref[
                g, 0:REC_VAL, :
            ]

    entering = in_ref[...] * jnp.exp(before_total) + before
    raw = local_ref[...] + dot(faded_ref[...], entering.astype(BF16), tb=True)
    normed = raw * lax.rsqrt(jnp.mean(raw * raw, axis=1, keepdims=True) + epsilon) * gain_ref[...]
    gate = gate_ref[...].astype(F32)
    state_heads = normed * (gate * jax.nn.sigmoid(gate))
    state_heads = jnp.concatenate([state_heads, jnp.zeros_like(state_heads)], axis=1)
    early_ref[...] = pack(state_heads[0:128], state_heads[128:256], 0)
    early_copies = [
        pltpu.make_async_remote_copy(
            src_ref=early_ref, dst_ref=early_slots_ref.at[tp], send_sem=early_send.at[d],
            recv_sem=early_recv.at[d], device_id={"tp": there}, device_id_type=MESH,
        )
        for d, there in enumerate(lane_peers)
    ]
    for copy in early_copies:
        copy.start()
    early_slots_ref[tp] = early_ref[...]

    attend_plane(2, 0)
    attend_plane(3, 0)
    ready(0)

    @pl.when(c == 0)
    def _():
        back(1, 1).start()
        back(2, 1).start()

    own_acc, own_left = joined(slice(0, TOK))
    acc_ref[0, 0:TOK, :] = own_acc
    left_ref[0, 0:TOK, :] = own_left

    def add(source, ref, natural=1):
        out_ref[...] += dot(unpack(ref[...], natural), columns_ref[source])

    for copy in own_columns:
        copy.wait()
    for copy in column_copies + early_copies:
        copy.wait_recv()
    out_ref[...] = jnp.zeros_like(out_ref)
    for n in range(8):
        add(n, early_slots_ref.at[n], 0)

    for g in (2, 1, 0):

        @pl.when(g < c)
        def _():
            arrival(1, g).wait_recv()
            arrival(2, g).wait_recv()
            packed = part_ref[g].astype(F32)
            scale = jnp.exp2(left_ref[0, 0:TOK, :])
            acc_ref[0, 0:128, :] += packed * scale[0:128, :]
            acc_ref[0, 128:256, :] += pltpu.roll(packed, 64, 1) * scale[128:256, :]
            for at in (0, 128):
                left_ref[0, at : at + 128, :] += column(part_left_ref[g, 0:1, at : at + 128])

    heads_ref[...] = pack(acc_ref[0, 0:128, :], acc_ref[0, 128:256, :], 1)

    ring_gather(heads_ref, head_slots_ref, head_send, head_recv, lambda: None, add, small=True)
    sent = early_copies + along_line + row_states + line_states + column_copies
    for d in range(4):
        sent = sent + along_row[d] + halves[d]
    for copy in sent:
        copy.wait_send()
    for d in (1, 2, 3):

        @pl.when(c >= d)
        def _():
            query_copy(d).wait_send()

        @pl.when(c + d < 4)
        def _():
            for k in range(3):
                back(k, d).wait_send()


def layer(*operands):
    dma = pltpu.SemaphoreType.DMA

    def both(*shape):
        return [dma(shape), dma(shape)]

    return pl.pallas_call(
        layer_kernel,
        out_shape=jax.ShapeDtypeStruct((TOK, 256), F32),
        in_specs=[SMEM] + [HBM] * 14,
        out_specs=VMEM,
        scratch_shapes=[
            pltpu.VMEM((TOK, 256), BF16),
            pltpu.VMEM((1, D), F32),
            pltpu.VMEM((1, REC_KEY), F32),
            pltpu.VMEM((1, TOK), F32),
            pltpu.VMEM((1, REC_VAL), F32),
            pltpu.VMEM((8, TOK, 256), BF16),
            pltpu.VMEM((320, D), BF16),
            pltpu.VMEM((D, 256), BF16),
            pltpu.VMEM((TOK, 320), F32),
            pltpu.VMEM((TOK, 256), F32),
            pltpu.VMEM((TOK, 128), F32),
            pltpu.VMEM((TOK, 128), BF16),
            pltpu.VMEM((128, 128), BF16),
            pltpu.VMEM((TOK, 128), BF16),
            pltpu.VMEM((TOK, 128), BF16),
            pltpu.VMEM((TOK, 64), BF16),
            pltpu.VMEM((TOK, 64), BF16),
            pltpu.VMEM((4, 4, TOK, 128), BF16),
            pltpu.VMEM((3, 128, 128), BF16),
            pltpu.VMEM((STATE_ROWS, REC_KEY), F32),
            pltpu.VMEM((4, STATE_ROWS, REC_KEY), F32),
            pltpu.VMEM((4, STATE_ROWS, REC_KEY), F32),
            pltpu.VMEM((STATE_ROWS, REC_KEY), F32),
            pltpu.VMEM((3, STATE_ROWS, REC_KEY), F32),
            pltpu.VMEM((TOK, REC_VAL), F32),
            pltpu.VMEM((TOK, REC_KEY), BF16),
            pltpu.VMEM((4 * TOK, 128), BF16),
            pltpu.VMEM((TOK, TOK), BF16),
            pltpu.VMEM((4, 4 * TOK, 128), F32),
            pltpu.VMEM((4, 4 * TOK, 128), F32),
            pltpu.VMEM((3, 128, 128), BF16),
            pltpu.VMEM((3, 1, TOK), F32),
            pltpu.VMEM((3, 128, 128), BF16),
            pltpu.VMEM((3, 1, TOK), F32),
            pltpu.VMEM((REC_VAL, REC_KEY), F32),
            pltpu.VMEM((128, 128), BF16),
            pltpu.VMEM((8, 128, 256), BF16),
            pltpu.VMEM((8, 128, 128), BF16),
            pltpu.VMEM((128, 128), BF16),
            pltpu.VMEM((8, 128, 128), BF16),
            dma((12,)), *both(7), *both(13), *both(13),
            *both(3), *both(4, 2), *both(4, 2), *both(2, 3),
            *both(3), *both(2, 7), *both(3, 3), dma((2,)), pltpu.SemaphoreType.REGULAR((3,)),
        ],
        compiler_params=pltpu.CompilerParams(collective_id=0, has_side_effects=True),
        name="layer",
    )(*operands)


def shards(
    tokens,
    input_norm_gain,
    attention_query_weight,
    attention_key_weight,
    attention_value_weight,
    attention_score_bias,
    recurrence_query_weight,
    forget_weight,
    input_weight,
    output_gate_weight,
    forget_minimum,
    decay_spikes,
    head_norm_gain,
    attention_output_weight,
    recurrence_output_weight,
):
    narrow = (
        attention_key_weight, attention_value_weight, input_weight, output_gate_weight, attention_query_weight
    )
    return layer(
        attention_score_bias, tokens, input_norm_gain[None, :], forget_minimum,
        decay_spikes.reshape(1, TOK), head_norm_gain[None, :],
        *(w.T for w in narrow), recurrence_query_weight, forget_weight,
        recurrence_output_weight, attention_output_weight,
    ).astype(BF16)


def solution(mesh):
    placed = (
        P("sp", "tp"),
        P(),
        P(None, "tp"),
        P(None, "tp"),
        P(None, "tp"),
        P("tp"),
        P(None, "tp"),
        P(None, "tp"),
        P(None, "tp"),
        P(None, "tp"),
        P("tp", None),
        P("sp", "tp"),
        P(),
        P("tp", None),
        P("tp", None),
    )
    return jax.shard_map(
        shards, mesh=mesh, in_specs=placed, out_specs=P("sp", "tp"), check_vma=False
    )
```

```python
import functools

import jax
import jax.numpy as jnp
from jax import lax
from jax.experimental import pallas as pl
from jax.experimental.pallas import tpu as pltpu
from jax.sharding import PartitionSpec as P

D = 2048
HEAD = 64
REC_KEY = 128
REC_VAL = 64
REC_SPAN = 64
TOK = 256
LOG2E = 1.4426950408889634
STATE_ROWS = REC_VAL + 8
epsilon = 1e-06
F32, BF16 = jnp.float32, jnp.bfloat16
VMEM = pl.BlockSpec(memory_space=pltpu.VMEM)
SMEM = pl.BlockSpec(memory_space=pltpu.SMEM)
HBM = pl.BlockSpec(memory_space=pltpu.HBM)
MESH = pl.DeviceIdType.MESH


def dot(a, b, ta=False, tb=False):
    dims = (((0 if ta else 1,), (1 if tb else 0,)), ((), ()))
    return lax.dot_general(a, b, dims, preferred_element_type=F32)


def to(src, dst, send, recv, sp):
    return pltpu.make_async_remote_copy(
        src_ref=src, dst_ref=dst, send_sem=send, recv_sem=recv,
        device_id={"sp": sp}, device_id_type=MESH,
    )


def place():
    sp = lax.axis_index("sp")
    return sp, sp // 16, (sp // 4) % 4, sp % 4


def lanes():
    tp = lax.axis_index("tp")
    x, core = tp // 2, tp % 2
    return tp, tp + 1 - 2 * core, (tp + 2) % 8, (tp + 6) % 8, (tp + 4) % 8, 1 - 2 * core


def ring_gather(chunk_ref, slots_ref, send, recv, meanwhile, use, small=False):
    tp, partner, right, left, across, twist = lanes()
    half = chunk_ref.shape[0] // 2
    top, low = slice(0, half), slice(half, 2 * half)

    def copy(n, src, dst, target):
        return pltpu.make_async_remote_copy(
            src_ref=src, dst_ref=dst, send_sem=send.at[n], recv_sem=recv.at[n],
            device_id={"tp": target}, device_id_type=MESH,
        )

    def relay(n, source, part, target):
        return copy(n, slots_ref.at[source, part], slots_ref.at[source, part], target)

    copies = [
        copy(0, chunk_ref, slots_ref.at[tp], partner),
        copy(1, chunk_ref.at[top], slots_ref.at[tp, top], right),
        copy(2, chunk_ref.at[low], slots_ref.at[tp, low], left),
        copy(3, chunk_ref.at[low], slots_ref.at[tp, low], right),
        copy(4, chunk_ref.at[top], slots_ref.at[tp, top], left),
        relay(5, left, top, right),
        relay(6, right, low, left),
        relay(7, left, top, partner),
        relay(8, right, low, partner),
        relay(9, left, low, partner),
        relay(10, right, top, partner),
    ]
    if small:
        copies += [relay(11, left, top, right + twist), relay(12, right, low, left + twist)]
    else:
        copies += [relay(11, across, top, partner), relay(12, across, low, partner)]
    for n in range(5):
        copies[n].start()
    if not small:
        meanwhile()
        use(tp, chunk_ref)
    copies[1].wait_recv()
    copies[5].start()
    if small:
        copies[11].start()
    copies[7].start()
    copies[2].wait_recv()
    copies[6].start()
    if small:
        copies[12].start()
    copies[8].start()
    copies[0].wait_recv()
    if not small:
        use(partner, slots_ref.at[partner])
    copies[3].wait_recv()
    copies[9].start()
    copies[4].wait_recv()
    copies[10].start()
    if small:
        meanwhile()
        use(tp, chunk_ref)
        use(partner, slots_ref.at[partner])
    use(left, slots_ref.at[left])
    use(right, slots_ref.at[right])
    copies[7].wait_recv()
    copies[9].wait_recv()
    use(left + twist, slots_ref.at[left + twist])
    copies[8].wait_recv()
    copies[10].wait_recv()
    use(right + twist, slots_ref.at[right + twist])
    copies[5].wait_recv()
    if not small:
        copies[11].start()
    copies[6].wait_recv()
    if not small:
        copies[12].start()
    use(across, slots_ref.at[across])
    copies[11].wait_recv()
    copies[12].wait_recv()
    use(across + twist, slots_ref.at[across + twist])
    for one in copies:
        one.wait_send()


def column(row):
    return jnp.transpose(jnp.broadcast_to(row, (128, 128)))


def local_scan(query_ref, forget_ref, input_ref, low_ref, spike_ref, out_ref, lift_ref, state_ref):
    span = REC_SPAN
    rows = lax.broadcasted_iota(jnp.int32, (span, span), 0)
    cols = lax.broadcasted_iota(jnp.int32, (span, span), 1)
    causal = cols <= rows
    ones = jnp.where(causal, 1.0, 0.0)
    spikes = jnp.concatenate([column(spike_ref[:, n : n + 128]) for n in (0, 128)], axis=0)
    state = jnp.zeros((REC_VAL, REC_KEY), F32)
    offset = jnp.zeros((1, REC_KEY), F32)
    for n in range(query_ref.shape[0] // span):
        at = slice(n * span, (n + 1) * span)
        query = query_ref[at, :].astype(F32)
        lifted = query * jax.nn.sigmoid(query)
        intake = (1.0 - low_ref[...]) * jax.nn.sigmoid(-forget_ref[at, :].astype(F32))
        log_forget = jnp.log1p(-intake) + spikes[at, :]
        running = lax.dot_general(
            ones, log_forget, (((1,), (0,)), ((), ())),
            precision=lax.Precision.HIGHEST, preferred_element_type=F32,
        )
        total = running[span - 1 : span, :]
        middle = running[span // 2 - 1 : span // 2, :]
        value = input_ref[at, :]
        grown = (lifted * jnp.exp(running - middle)).astype(BF16)
        shrunk = (intake * jnp.exp(middle - running)).astype(BF16)
        inner = jnp.where(causal, dot(grown, shrunk, tb=True), 0.0)
        faded = (lifted * jnp.exp(running)).astype(BF16)
        out_ref[at, :] = dot(inner.astype(BF16), value) + dot(faded, state.astype(BF16), tb=True)
        lift_ref[at, :] = (lifted * jnp.exp(running + offset)).astype(BF16)
        kept = (intake * jnp.exp(total - running)).astype(BF16)
        state = state * jnp.exp(total) + dot(value, kept, ta=True)
        offset = offset + total
    state_ref[0:REC_VAL, :] = state
    state_ref[REC_VAL:STATE_ROWS, :] = jnp.broadcast_to(offset, (8, REC_KEY))


def attend(first, here, plane, bias2, q_ref, kvs_ref, tri_ref, acc_ref, left_ref):
    at = slice(first, first + 2 * TOK)
    ahead = lax.broadcasted_iota(jnp.int32, (TOK, TOK), 1) - lax.broadcasted_iota(jnp.int32, (TOK, TOK), 0)
    q, tri = q_ref[at, :], tri_ref[...]
    acc = jnp.zeros((2 * TOK, 128), F32)
    left = jnp.zeros((2 * TOK, 1), F32)
    for n in (3, 2, 1, 0):

        def masked(x):
            if first > 0:
                return x
            keep = ahead < (here - plane * 4 - n) * TOK
            return jnp.concatenate([jnp.where(keep, x[0:TOK], 0.0), x[TOK:]], axis=0)

        kv = kvs_ref[plane, n]
        z = dot(q, kv, tb=True) * (LOG2E / 8.0) + bias2
        soft = masked(jnp.maximum(z, jnp.log(1.0 + jnp.exp2(jnp.minimum(z, 30.0))) * LOG2E))
        later = dot(soft.astype(BF16), tri)
        weight = masked(jnp.exp2((z - soft) + (later + left)))
        acc = acc + dot(weight.astype(BF16), kv)
        left = left + (later[:, 0:1] - soft[:, 0:1])
    acc_ref[at, :] = acc
    left_ref[at, :] = jnp.broadcast_to(left, (2 * TOK, 128))


def pack(top, low, natural):
    lane = lax.broadcasted_iota(jnp.int32, (128, 128), 1)
    return jnp.where((lane < HEAD) == (natural == 0), top, pltpu.roll(low, 64, 1)).astype(BF16)


def unpack(packed, natural):
    lane = lax.broadcasted_iota(jnp.int32, (128, 128), 1)
    keep = (lane < HEAD) == (natural == 0)
    packed = packed.astype(F32)
    low = pltpu.roll(packed, 64, 1)
    return jnp.concatenate([jnp.where(keep, packed, 0.0), jnp.where(keep, low, 0.0)], axis=0).astype(BF16)


def chain(states_ref, here):
    state = states_ref[0, 0:REC_VAL, :]
    total = states_ref[0, REC_VAL : REC_VAL + 1, :]
    ahead, ahead_total = jnp.zeros_like(state), jnp.zeros_like(total)
    for n in range(1, 4):
        ahead = jnp.where(n <= here, state, ahead)
        ahead_total = jnp.where(n <= here, total, ahead_total)
        more = states_ref[n, REC_VAL : REC_VAL + 1, :]
        state = state * jnp.exp(more) + states_ref[n, 0:REC_VAL, :]
        total = total + more
    return state, total, ahead, ahead_total


def layer_kernel(
    bias_ref, token_hbm, feature_gain_hbm, low_hbm, spike_hbm, gain_hbm,
    key_w, value_w, input_w, gate_w, query_w, rec_w, forget_w, rec_out_w, att_out_w,
    out_ref,
    token_ref, feature_gain_ref, low_ref, spike_ref, gain_ref,
    slots_ref, narrow_ref, wide_ref, first_ref, second_ref, square_ref,
    kv_ref, query_ref, rec_ref, forget_ref, input_ref, gate_ref,
    kvs_ref, queries_ref, state_ref, rows_ref, planes_ref, group_ref, groups_ref,
    local_ref, faded_ref, q_ref, tri_ref, acc_ref, left_ref,
    far_ref, far_left_ref, part_ref, part_left_ref, in_ref,
    heads_ref, columns_ref, head_slots_ref, early_ref, early_slots_ref,
    load, early_send, early_recv, token_send, token_recv, head_send, head_recv,
    line_send, line_recv, row_send, row_recv, half_send, half_recv, state_send, state_recv,
    query_send, query_recv, column_send, column_recv, back_send, back_recv, own_sem, near_sem,
):
    sp, c, zl, y = place()
    tp = lax.axis_index("tp")
    base = c * 16
    row = [base + zl * 4 + (y + d) % 4 for d in range(4)]
    line = [base + ((zl + d) % 4) * 4 + y for d in range(4)]
    far = [(sp + 16 * d) % 64 for d in range(4)]
    lane_peers = [(tp + d) % 8 for d in range(1, 8)]

    narrow = (key_w, value_w, input_w, gate_w, query_w)
    loads = [
        pltpu.make_async_copy(w, narrow_ref.at[n * 64 : n * 64 + 64], load.at[n])
        for n, w in enumerate(narrow)
    ]
    loads += [
        pltpu.make_async_copy(w, wide_ref.at[:, n * 128 : n * 128 + 128], load.at[5 + n])
        for n, w in enumerate((rec_w, forget_w))
    ]
    small = (
        (token_hbm, token_ref), (feature_gain_hbm, feature_gain_ref), (low_hbm, low_ref),
        (spike_hbm, spike_ref), (gain_hbm, gain_ref),
    )
    first_loads = [pltpu.make_async_copy(src, dst, load.at[7 + n]) for n, (src, dst) in enumerate(small)]

    def columns(w, there):
        return w.at[:, pl.ds(pl.multiple_of(there * 256, 256), 256)]

    out_w = ((0, rec_out_w), (1, att_out_w))
    own_columns = [
        pltpu.make_async_copy(columns(w, tp), columns_ref.at[tp, n * 64 : n * 64 + 64], own_sem.at[n])
        for n, w in out_w
    ]
    column_copies = [
        pltpu.make_async_remote_copy(
            src_ref=columns(w, there), dst_ref=columns_ref.at[tp, n * 64 : n * 64 + 64],
            send_sem=column_send.at[n, d], recv_sem=column_recv.at[n, d],
            device_id={"tp": there}, device_id_type=MESH,
        )
        for n, w in out_w
        for d, there in enumerate(lane_peers)
    ]

    barrier = pltpu.get_barrier_semaphore()
    planes = [[(sp + 4 * d) % 64, (sp + 64 - 4 * d) % 64] for d in (1, 2, 4)]
    near = row[1:] + planes[0]
    for peer in lane_peers:
        pl.semaphore_signal(barrier, inc=1, device_id={"tp": peer}, device_id_type=MESH)
    for peer in near:
        pl.semaphore_signal(barrier, inc=1, device_id={"sp": peer}, device_id_type=MESH)
    for copy in first_loads + loads + own_columns:
        copy.start()
    first_ref[...] = jnp.zeros_like(first_ref)
    second_ref[...] = jnp.zeros_like(second_ref)
    square_ref[...] = jnp.zeros_like(square_ref)
    rows = lax.broadcasted_iota(jnp.int32, (TOK, TOK), 0)
    cols = lax.broadcasted_iota(jnp.int32, (TOK, TOK), 1)
    tri_ref[...] = jnp.where(rows > cols, -1.0, 0.0).astype(BF16)
    pl.semaphore_wait(barrier, len(lane_peers) + len(near))

    def vouch(n):
        for peer in planes[n]:
            pl.semaphore_signal(near_sem.at[n], inc=1, device_id={"sp": peer}, device_id_type=MESH)

    vouch(0)
    for copy in first_loads:
        copy.wait()

    def meanwhile():
        pl.semaphore_wait(near_sem.at[0], 2)
        vouch(1)
        for one in loads:
            one.wait()
        pl.semaphore_wait(near_sem.at[1], 2)
        vouch(2)

    def use(source, ref):
        at = pl.ds(pl.multiple_of(source * 256, 256), 256)
        values = ref[...].astype(F32)
        squares = values * values
        square_ref[...] += squares[:, 0:128] + squares[:, 128:256]
        scaled = (values * feature_gain_ref[:, at]).astype(BF16)
        first_ref[...] += dot(scaled, narrow_ref[:, at], tb=True)
        second_ref[...] += dot(scaled, wide_ref[at, :])

    ring_gather(token_ref, slots_ref, token_send, token_recv, meanwhile, use)
    inverse = lax.rsqrt(jnp.sum(square_ref[...], axis=1, keepdims=True) / D + epsilon)
    query = (first_ref[:, 256:320] * inverse).astype(BF16)
    query_ref[...] = jnp.concatenate([query[0:128], query[128:256]], axis=1)
    kv = (first_ref[:, 0:128] * inverse).astype(BF16)
    kv_ref[...] = kv
    kvs_ref[zl, y] = kv
    for n in (1, 2, 3):

        @pl.when(c >= n)
        def _():
            queries_ref[n - 1] = jnp.zeros((128, 128), BF16)


    def query_copy(d):
        slot = (c + 2) % 3
        return to(query_ref, queries_ref.at[slot], query_send.at[d - 1], query_recv.at[slot], far[4 - d])

    pl.semaphore_wait(near_sem.at[2], 2)
    along_line = [
        to(kv_ref, kvs_ref.at[zl, y], line_send.at[d - 1], line_recv.at[d - 1], line[d]) for d in (1, 2, 3)
    ]
    along_row = [
        [
            to(
                kv_ref if d == 0 else kvs_ref.at[(zl - d + 4) % 4, y],
                kvs_ref.at[(zl - d + 4) % 4, y], row_send.at[d, k], row_recv.at[d, k], row[1 if k == 0 else 3],
            )
            for k in range(2)
        ]
        for d in range(4)
    ]

    def onward(d, k):
        block = kvs_ref.at[(zl - d + 4) % 4, (y + 3) % 4 if k == 0 else (y + 1) % 4, k * 128 : k * 128 + 128]
        return to(block, block, half_send.at[d, k], half_recv.at[d, k], row[1 if k == 0 else 3])

    halves = [[onward(d, k) for k in range(2)] for d in range(4)]
    for copy in along_row[0]:
        copy.start()
    for d, n in ((2, 1), (1, 2), (3, 3)):

        @pl.when(c >= d)
        def _():
            query_copy(d).start()

        along_line[n - 1].start()
    input_ref[...] = (first_ref[:, 128:192] * inverse).astype(BF16)
    gate_ref[...] = (first_ref[:, 192:256] * inverse).astype(BF16)
    rec_ref[...] = (second_ref[:, 0:128] * inverse).astype(BF16)
    forget_ref[...] = (second_ref[:, 128:256] * inverse).astype(BF16)
    local_scan(rec_ref, forget_ref, input_ref, low_ref, spike_ref, local_ref, faded_ref, state_ref)
    rows_ref[y] = state_ref[...]
    row_states = [
        to(state_ref, rows_ref.at[y], state_send.at[0, d - 1], state_recv.at[0, d - 1], row[d])
        for d in (1, 2, 3)
    ]
    for copy in row_states:
        copy.start()

    def pass_on(d):
        for k in range(2):
            along_row[d][k].wait_recv()
            halves[d][k].start()

    def from_line(d):
        along_line[d - 1].wait_recv()
        for copy in along_row[d]:
            copy.start()

    def take(n):
        if n > 0:

            @pl.when(c < n)
            def _():
                to(
                    query_ref, queries_ref.at[n - 1], query_send.at[0], query_recv.at[n - 1], far[1]
                ).wait_recv()

        packed = query_ref[...] if n == 0 else queries_ref[n - 1]
        q_ref[n * TOK : (n + 1) * TOK, :] = unpack(packed, 0)

    def attend_plane(d, first):
        if first == (0 if d == 0 else 2 * TOK):
            for k in range(2):
                halves[d][k].wait_recv()
        attend(
            first, zl * 4 + y, (zl - d + 4) % 4, bias_ref[0] * LOG2E, q_ref, kvs_ref, tri_ref,
            acc_ref.at[d], left_ref.at[d],
        )

    pass_on(0)
    from_line(1)
    take(0)
    take(1)
    attend_plane(0, 0)
    from_line(2)
    pass_on(1)
    from_line(3)
    for copy in column_copies:
        copy.start()
    for copy in row_states:
        copy.wait_recv()
    state, total, ahead, ahead_total = chain(rows_ref, y)
    planes_ref[zl, 0:REC_VAL, :] = state
    planes_ref[zl, REC_VAL:STATE_ROWS, :] = jnp.broadcast_to(total, (8, REC_KEY))
    line_states = [
        to(planes_ref.at[zl], planes_ref.at[zl], state_send.at[1, n - 1], state_recv.at[1, n - 1], line[n])
        for n in (1, 2, 3)
    ]
    for copy in line_states:
        copy.start()
    take(2)
    take(3)
    attend_plane(0, 2 * TOK)
    pass_on(2)
    attend_plane(1, 2 * TOK)
    pass_on(3)
    for copy in line_states:
        copy.wait_recv()
    state, total, low, low_total = chain(planes_ref, zl)
    group_ref[0:REC_VAL, :] = state
    group_ref[REC_VAL:STATE_ROWS, :] = jnp.broadcast_to(total, (8, REC_KEY))
    before = low * jnp.exp(ahead_total) + ahead
    before_total = low_total + ahead_total

    def back(k, d):
        slot = (c + d + 3) % 4
        src, dst = ((group_ref, groups_ref), (far_ref, part_ref), (far_left_ref, part_left_ref))[k]
        src = src if k == 0 else src.at[slot % 3]
        return to(src, dst.at[c % 3], back_send.at[k, d - 1], back_recv.at[k, c % 3], far[d])

    def arrival(k, g):
        src, dst = ((group_ref, groups_ref), (far_ref.at[0], part_ref), (far_left_ref.at[0], part_left_ref))[k]
        return to(src, dst.at[g], back_send.at[k, 0], back_recv.at[k, g], far[1])

    for d in (1, 2, 3):

        @pl.when(c + d < 4)
        def _():
            back(0, d).start()

    attend_plane(2, 2 * TOK)
    attend_plane(3, 2 * TOK)

    def joined(at):
        n = (zl + 1) % 4
        acc, left = acc_ref[n, at, :], left_ref[n, at, :]
        for p in (2, 1, 0):
            n = (zl - p + 4) % 4
            acc = acc + acc_ref[n, at, :] * jnp.exp2(left)
            left = left + left_ref[n, at, :]
        return acc, left

    def ready(n):
        at = (n + 1) * TOK
        top, top_left = joined(slice(at, at + 128))
        low, low_left = joined(slice(at + 128, at + 256))
        far_ref[n] = pack(top, low, 1)
        far_left_ref[n, :, 0:128] = jnp.transpose(top_left)[0:1, :]
        far_left_ref[n, :, 128:256] = jnp.transpose(low_left)[0:1, :]

    ready(1)
    ready(2)
    for d in (2, 3, 1):

        @pl.when((c + d < 4) & (c + d > 1))
        def _():
            back(1, d).start()
            back(2, d).start()

    attend_plane(1, 0)

    in_ref[...] = jnp.zeros_like(in_ref)
    for g in (0, 1, 2):

        @pl.when(g < c)
        def _():
            arrival(0, g).wait_recv()
            in_ref[...] = in_ref[...] * jnp.exp(groups_ref[g, REC_VAL : REC_VAL + 1, :]) + groups_ref[
                g, 0:REC_VAL, :
            ]

    entering = in_ref[...] * jnp.exp(before_total) + before
    raw = local_ref[...] + dot(faded_ref[...], entering.astype(BF16), tb=True)
    normed = raw * lax.rsqrt(jnp.mean(raw * raw, axis=1, keepdims=True) + epsilon) * gain_ref[...]
    gate = gate_ref[...].astype(F32)
    state_heads = normed * (gate * jax.nn.sigmoid(gate))
    state_heads = jnp.concatenate([state_heads, jnp.zeros_like(state_heads)], axis=1)
    early_ref[...] = pack(state_heads[0:128], state_heads[128:256], 0)
    early_copies = [
        pltpu.make_async_remote_copy(
            src_ref=early_ref, dst_ref=early_slots_ref.at[tp], send_sem=early_send.at[d],
            recv_sem=early_recv.at[d], device_id={"tp": there}, device_id_type=MESH,
        )
        for d, there in enumerate(lane_peers)
    ]
    for copy in early_copies:
        copy.start()
    early_slots_ref[tp] = early_ref[...]

    attend_plane(2, 0)
    attend_plane(3, 0)
    ready(0)

    @pl.when(c == 0)
    def _():
        back(1, 1).start()
        back(2, 1).start()

    own_acc, own_left = joined(slice(0, TOK))
    acc_ref[0, 0:TOK, :] = own_acc
    left_ref[0, 0:TOK, :] = own_left

    for g in (2, 1, 0):

        @pl.when(g < c)
        def _():
            arrival(1, g).wait_recv()
            arrival(2, g).wait_recv()
            packed = part_ref[g].astype(F32)
            scale = jnp.exp2(left_ref[0, 0:TOK, :])
            acc_ref[0, 0:128, :] += packed * scale[0:128, :]
            acc_ref[0, 128:256, :] += pltpu.roll(packed, 64, 1) * scale[128:256, :]
            for at in (0, 128):
                left_ref[0, at : at + 128, :] += column(part_left_ref[g, 0:1, at : at + 128])

    heads_ref[...] = pack(acc_ref[0, 0:128, :], acc_ref[0, 128:256, :], 1)

    def columns_here():
        for copy in own_columns:
            copy.wait()
        for copy in column_copies + early_copies:
            copy.wait_recv()
        out_ref[...] = jnp.zeros_like(out_ref)
        for n in range(8):
            add(n, early_slots_ref.at[n], 0)

    def add(source, ref, natural=1):
        out_ref[...] += dot(unpack(ref[...], natural), columns_ref[source])

    ring_gather(heads_ref, head_slots_ref, head_send, head_recv, columns_here, add, small=True)
    sent = early_copies + along_line + row_states + line_states + column_copies
    for d in range(4):
        sent = sent + along_row[d] + halves[d]
    for copy in sent:
        copy.wait_send()
    for d in (1, 2, 3):

        @pl.when(c >= d)
        def _():
            query_copy(d).wait_send()

        @pl.when(c + d < 4)
        def _():
            for k in range(3):
                back(k, d).wait_send()


def layer(*operands):
    dma = pltpu.SemaphoreType.DMA

    def both(*shape):
        return [dma(shape), dma(shape)]

    return pl.pallas_call(
        layer_kernel,
        out_shape=jax.ShapeDtypeStruct((TOK, 256), F32),
        in_specs=[SMEM] + [HBM] * 14,
        out_specs=VMEM,
        scratch_shapes=[
            pltpu.VMEM((TOK, 256), BF16),
            pltpu.VMEM((1, D), F32),
            pltpu.VMEM((1, REC_KEY), F32),
            pltpu.VMEM((1, TOK), F32),
            pltpu.VMEM((1, REC_VAL), F32),
            pltpu.VMEM((8, TOK, 256), BF16),
            pltpu.VMEM((320, D), BF16),
            pltpu.VMEM((D, 256), BF16),
            pltpu.VMEM((TOK, 320), F32),
            pltpu.VMEM((TOK, 256), F32),
            pltpu.VMEM((TOK, 128), F32),
            pltpu.VMEM((TOK, 128), BF16),
            pltpu.VMEM((128, 128), BF16),
            pltpu.VMEM((TOK, 128), BF16),
            pltpu.VMEM((TOK, 128), BF16),
            pltpu.VMEM((TOK, 64), BF16),
            pltpu.VMEM((TOK, 64), BF16),
            pltpu.VMEM((4, 4, TOK, 128), BF16),
            pltpu.VMEM((3, 128, 128), BF16),
            pltpu.VMEM((STATE_ROWS, REC_KEY), F32),
            pltpu.VMEM((4, STATE_ROWS, REC_KEY), F32),
            pltpu.VMEM((4, STATE_ROWS, REC_KEY), F32),
            pltpu.VMEM((STATE_ROWS, REC_KEY), F32),
            pltpu.VMEM((3, STATE_ROWS, REC_KEY), F32),
            pltpu.VMEM((TOK, REC_VAL), F32),
            pltpu.VMEM((TOK, REC_KEY), BF16),
            pltpu.VMEM((4 * TOK, 128), BF16),
            pltpu.VMEM((TOK, TOK), BF16),
            pltpu.VMEM((4, 4 * TOK, 128), F32),
            pltpu.VMEM((4, 4 * TOK, 128), F32),
            pltpu.VMEM((3, 128, 128), BF16),
            pltpu.VMEM((3, 1, TOK), F32),
            pltpu.VMEM((3, 128, 128), BF16),
            pltpu.VMEM((3, 1, TOK), F32),
            pltpu.VMEM((REC_VAL, REC_KEY), F32),
            pltpu.VMEM((128, 128), BF16),
            pltpu.VMEM((8, 128, 256), BF16),
            pltpu.VMEM((8, 128, 128), BF16),
            pltpu.VMEM((128, 128), BF16),
            pltpu.VMEM((8, 128, 128), BF16),
            dma((12,)), *both(7), *both(13), *both(13),
            *both(3), *both(4, 2), *both(4, 2), *both(2, 3),
            *both(3), *both(2, 7), *both(3, 3), dma((2,)), pltpu.SemaphoreType.REGULAR((3,)),
        ],
        compiler_params=pltpu.CompilerParams(collective_id=0, has_side_effects=True),
        name="layer",
    )(*operands)


def shards(
    tokens,
    input_norm_gain,
    attention_query_weight,
    attention_key_weight,
    attention_value_weight,
    attention_score_bias,
    recurrence_query_weight,
    forget_weight,
    input_weight,
    output_gate_weight,
    forget_minimum,
    decay_spikes,
    head_norm_gain,
    attention_output_weight,
    recurrence_output_weight,
):
    narrow = (
        attention_key_weight, attention_value_weight, input_weight, output_gate_weight, attention_query_weight
    )
    return layer(
        attention_score_bias, tokens, input_norm_gain[None, :], forget_minimum,
        decay_spikes.reshape(1, TOK), head_norm_gain[None, :],
        *(w.T for w in narrow), recurrence_query_weight, forget_weight,
        recurrence_output_weight, attention_output_weight,
    ).astype(BF16)


def solution(mesh):
    placed = (
        P("sp", "tp"),
        P(),
        P(None, "tp"),
        P(None, "tp"),
        P(None, "tp"),
        P("tp"),
        P(None, "tp"),
        P(None, "tp"),
        P(None, "tp"),
        P(None, "tp"),
        P("tp", None),
        P("sp", "tp"),
        P(),
        P("tp", None),
        P("tp", None),
    )
    return jax.shard_map(
        shards, mesh=mesh, in_specs=placed, out_specs=P("sp", "tp"), check_vma=False
    )
```
